128 devices in a mesh: sp: 16 (over z, x), tp: 8 (over y, core).
Axes of the slice: x: 4, y: 4, z: 4, core: 2. Of those that a mesh axis runs over, the one named last changes fastest.
Arguments:
- token_values: bfloat16 [4096, 2048], P('sp', 'tp'), may hold values from -6 to 6
- write_keys: bfloat16 [4096, 1024], P('sp', 'tp'), may hold values from -0.3125 to 0.3125
- read_keys: bfloat16 [4096, 1024], P('sp', 'tp'), may hold values from -0.3125 to 0.3125
- log_decay: float32 [32, 4096], P('tp', 'sp'), may hold values from -0.7 to 0, as said below
- out_gate: bfloat16 [4096, 2048], P('sp', 'tp'), may hold values from -6 to 6
- out_proj: bfloat16 [4096, 2048], P(None, 'tp'), may hold values from -0.125 to 0.125
- mixed: bfloat16 [4096, 4096], P('sp'), may hold values from -6 to 6
- cotangent: bfloat16 [4096, 4096], P('sp'), may hold values from -8 to 8
- route_ids: int32 [4096, 2], P('sp'), may hold values from 0 to 15, all different within a row; in each aligned block of 256 rows (0 to 255, 256 to 511, ...) at most 48 rows name the same one
- route_weights: float32 [4096, 2], P('sp'), may hold values from 0.25 to 1
- w_gate: bfloat16 [16, 4096, 2048], P('sp', None, 'tp'), may hold values from -0.09375 to 0.09375
- w_up: bfloat16 [16, 4096, 2048], P('sp', None, 'tp'), may hold values from -0.09375 to 0.09375
- w_down: bfloat16 [16, 2048, 4096], P('sp', 'tp'), may hold values from -0.125 to 0.125
Outputs:
- value_grad: bfloat16 [4096, 2048], P('sp', 'tp')
- write_grad: bfloat16 [4096, 1024], P('sp', 'tp')
- read_grad: bfloat16 [4096, 1024], P('sp', 'tp')
- gate_grad: bfloat16 [4096, 2048], P('sp', 'tp')
- proj_grad: float32 [4096, 2048], P('sp', 'tp')
- gate_weight_grad: bfloat16 [16, 4096, 2048], P('sp', None, 'tp')
- up_weight_grad: bfloat16 [16, 4096, 2048], P('sp', None, 'tp')
- down_weight_grad: bfloat16 [16, 2048, 4096], P('sp', 'tp')
The draws below stay inside these ranges and needn't reach their ends.
Inputs may be any that keep to these rules, and one draw needn't show every extreme that they name: `route_ids`: each row names 2 different experts. Within the rows of one device no expert is named more than 48 times, and in every draw some expert is named exactly 48 times by the rows of some device. `log_decay`: every entry is negative.
All inputs are finite; a program needn't handle non-finite values.
Results may differ from the reference program's by a relative error of at most 0.019.
Values may be sent and summed in bfloat16 or wider, within the bound.
A program may use at most 128 MiB of HBM per device.

```python
import math
import jax
import jax.numpy as jnp
import numpy as np
from jax import lax

D = 4096
GROUPS = 8
HEAD_DIM = 64
STATE = 128
HEADS = 32
INNER = 2048
EXPERT_HIDDEN_SIZE = 2048
TOP = 2
BLOCK = 64
TOK_DEV = 256
TOKENS = 4096
EXPERTS = 16
CAP = 48
N_SP = 16
N_TP = 8


def draw_log_decay(key, part):
    keys = jax.random.split(jax.random.fold_in(key, 7), 7)
    fast_share = 0.5
    fast = jax.random.uniform(keys[0], (HEADS, 1), jnp.float32) < fast_share
    fast_rate = jnp.exp(jax.random.uniform(keys[1], (HEADS, 1), jnp.float32, jnp.log(2.3 / 50.0), jnp.log(2.3 / 30.0)))
    keep = jax.random.uniform(keys[2], (HEADS, 1), jnp.float32, 0.55, 0.8)
    slow_rate = -jnp.log(keep) / TOKENS
    segment_factor = jnp.exp(jax.random.uniform(keys[3], (HEADS, TOKENS // TOK_DEV), jnp.float32, -0.45, 0.45))
    segment_factor = jnp.repeat(segment_factor, TOK_DEV, axis=1)
    token_factor = jnp.exp(jax.random.uniform(keys[4], (HEADS, TOKENS), jnp.float32, -0.6, 0.6))
    decay_speed = jnp.where(fast, fast_rate, slow_rate) * segment_factor * token_factor
    positions = jax.random.randint(keys[5], (HEADS, 2), 0, TOKENS)
    gate_intensity = jax.random.uniform(keys[6], (HEADS, 2), jnp.float32, jnp.log(0.5), jnp.log(0.8))
    places = jnp.arange(TOKENS, dtype=jnp.int32)
    dropped_tokens = places[None, None, :] == positions[:, :, None]
    decay_pulse = jnp.sum(jnp.where(dropped_tokens, gate_intensity[:, :, None], 0.0), axis=1)
    return jnp.clip(decay_pulse - decay_speed, -0.7, -1e-06).astype(jnp.float32)


def strengthened(drawn, stream_key, source, target, shards_of, factor):
    def block_of(dim):
        return (jnp.arange(drawn.shape[dim]) // (drawn.shape[dim] // shards_of)).reshape((-1,) + (1,) * (drawn.ndim - 1 - dim))

    first = jax.random.permutation(stream_key, shards_of)[block_of(target)]
    second = (block_of(target) + shards_of // 2) % shards_of
    return jnp.where((block_of(source) == first) | (block_of(source) == second), factor * drawn, drawn)


def shard_levels(own_key, dims, cuts, smallest, high):
    loudness, own = 1.0, jax.random.fold_in(own_key, 6)
    for dim, parts in cuts:
        heights = jnp.exp(jax.random.uniform(jax.random.fold_in(own, dim), (parts,), jnp.float32, smallest / len(cuts), high / len(cuts)))
        loudness = loudness * jnp.repeat(heights, dims[dim] // parts).reshape([-1 if axis == dim else 1 for axis in range(len(dims))])
    return loudness


def deal_out(stream_key, own, number, rows, number_of, top, bound, skew):
    order = jax.random.permutation(stream_key, number_of)
    crowded, usual = shares(number_of, rows * top, bound, skew, True), shares(number_of, rows * top, bound, skew, False)
    places = jnp.arange(number_of)

    def named(sizes, rotation):
        used = int((sizes > 0).sum())
        fixed = max(1, used // 4)
        passed = fixed + (places - fixed + rotation * (used - fixed)) % max(1, number_of - fixed)
        return jnp.zeros((number_of,), jnp.int32).at[order[jnp.where(places < fixed, places, passed)]].set(jnp.asarray(sizes, jnp.int32))

    sizes = jnp.where(number % 4 == 0, named(crowded, number // 4), named(usual, number - number // 4 - 1))
    mixed = jax.random.permutation(jax.random.fold_in(own, 3), number_of)
    source_of, receiver = mixed[0:number_of // 2 * 2:2], mixed[1:number_of // 2 * 2:2]
    margin = jnp.minimum(sizes[source_of] - 1, bound - sizes[receiver]) // 2
    margin = jnp.where((source_of == order[0]) | (receiver == order[0]) | (sizes[receiver] == 0), 0, jnp.maximum(margin, 0))
    passed = jax.random.randint(jax.random.fold_in(own, 4), (number_of // 2,), 0, 1 << 20) % (margin + 1)
    sizes = sizes.at[source_of].add(-passed).at[receiver].add(passed)
    items = jnp.searchsorted(jnp.cumsum(sizes), jnp.arange(rows * top), side="right").astype(jnp.int32)
    table = items.reshape(top, rows).T
    table = table[jax.random.permutation(jax.random.fold_in(own, 1), rows)]
    rotation = jax.random.randint(jax.random.fold_in(own, 2), (rows, 1), 0, top)
    return jnp.take_along_axis(table, (jnp.arange(top)[None, :] + rotation) % top, axis=1)


def shares(count, total, reach, lean, full):
    portions = [(1 << 20) // math.isqrt(rank ** lean) + 1 for rank in range(1, count + 1)]
    largest = reach if full else min(reach, max(-(-total // count), total * portions[0] // sum(portions)))
    least = 1 if total - largest >= count - 1 else 0
    holding, rest = [largest] + [least] * (count - 1), total - largest - least * (count - 1)
    while rest > 0:
        candidates = [i for i in range(1, count) if holding[i] < largest] or [i for i in range(1, count) if holding[i] < reach]
        whole, budget = sum([portions[i] for i in candidates]), rest
        for i in candidates:
            more = min(reach - holding[i], max(1, budget * portions[i] // whole), rest)
            holding[i] = holding[i] + more
            rest = rest - more
    return np.array(holding)


def centred(key, extent, scale, most, cuts=(), held_as=jnp.bfloat16):
    level = shard_levels(key, extent, cuts, -0.22, 0.18) if cuts else 1.0
    array = jax.random.normal(key, extent, jnp.float32) * scale * level
    return jnp.minimum(jnp.maximum(array, -most), most).astype(held_as)


def gaussian_with(stream_key, shape, deviation, most, shards, heavy, held_as=jnp.bfloat16):
    result = deviation * jax.random.normal(stream_key, shape, jnp.float32)
    if shards:
        result = result * shard_levels(stream_key, shape, shards, -0.22, 0.18)
    return jnp.clip(strengthened(result, jax.random.fold_in(stream_key, 3), *heavy), -most, most).astype(held_as)


def setup_inputs(seed: int = 0) -> dict:
    splits = jax.random.split(jax.random.key(seed), 14)
    token_values = centred(splits[0], (TOKENS, INNER), 1.0, 6.0, ((0, 16), (1, 8)))
    write_keys = centred(splits[1], (TOKENS, GROUPS * STATE), ((TOKENS * STATE // 4) ** -0.25), 0.3125, ((0, 16), (1, 8)))
    read_keys = centred(splits[2], (TOKENS, GROUPS * STATE), ((TOKENS * STATE // 4) ** -0.25), 0.3125, ((0, 16), (1, 8)))
    log_decay = draw_log_decay(jax.random.fold_in(splits[13], 71), 0)
    out_gate = centred(splits[4], (TOKENS, INNER), 1.0, 6.0, ((0, 16), (1, 8)))
    out_proj = centred(splits[5], (D, INNER), INNER ** -0.5, 0.125, ((1, 8),))
    mixed = centred(splits[6], (TOKENS, D), 1.0, 6.0, ((0, 16),))
    cotangent = gaussian_with(splits[7], (TOKENS, D), 1.0, 8.0, ((0, 16),), (0, 1, 16, 2.0))
    route_ids_keys = jax.random.split(jax.random.fold_in(splits[8], 1), TOKENS // TOK_DEV)
    route_ids_turns = jax.random.permutation(jax.random.fold_in(splits[8], 3), TOKENS // TOK_DEV)
    route_ids = jax.vmap(lambda own, number: deal_out(jax.random.fold_in(splits[8], 2), own, number, TOK_DEV, EXPERTS, TOP, CAP, 2))(route_ids_keys, route_ids_turns).reshape((TOKENS, TOP))
    route_weights = jnp.clip(0.25 + 0.75 * jax.random.uniform(splits[9], (TOKENS, TOP), jnp.float32) ** shard_levels(splits[9], (TOKENS, TOP), ((0, 16),), -0.2, 0.2), 0.25, 1.0)
    w_gate = centred(splits[10], (EXPERTS, D, EXPERT_HIDDEN_SIZE), D ** -0.5, 0.09375, ((0, 16), (2, 8)))
    w_up = centred(splits[11], (EXPERTS, D, EXPERT_HIDDEN_SIZE), D ** -0.5, 0.09375, ((0, 16), (2, 8)))
    w_down = centred(splits[12], (EXPERTS, EXPERT_HIDDEN_SIZE, D), EXPERT_HIDDEN_SIZE ** -0.5, 0.125, ((0, 16), (1, 8)))
    return {"token_values": token_values, "write_keys": write_keys, "read_keys": read_keys, "log_decay": log_decay, "out_gate": out_gate, "out_proj": out_proj, "mixed": mixed, "cotangent": cotangent, "route_ids": route_ids, "route_weights": route_weights, "w_gate": w_gate, "w_up": w_up, "w_down": w_down}


highest = lax.Precision.HIGHEST

def mix_blocks(token_values, write_keys, read_keys, log_decay, entering):
    length = token_values.shape[0]
    heads = log_decay.shape[0]
    groups = write_keys.shape[1] // STATE
    per_group = heads // groups
    blocks = length // BLOCK
    inputs = token_values.reshape(blocks, BLOCK, groups, per_group, HEAD_DIM)
    writes = write_keys.reshape(blocks, BLOCK, groups, STATE)
    reads = read_keys.reshape(blocks, BLOCK, groups, STATE)
    decay = log_decay.reshape(groups, per_group, blocks, BLOCK).transpose(2, 3, 0, 1)
    cumul = jnp.cumsum(decay, axis=1)
    spans = cumul[:, :, None] - cumul[:, None, :]
    position = jnp.arange(BLOCK, dtype=jnp.int32)
    lower = (position[:, None] >= position[None, :])[None, :, :, None, None]
    weights = jnp.exp(jnp.where(lower, spans, -jnp.inf))
    scores = jnp.einsum('clgn,csgn->clsg', reads, writes, precision=highest)
    inner = jnp.einsum('clsgr,csgrp->clgrp', scores[..., None] * weights, inputs, precision=highest)
    tails = jnp.exp(cumul[:, -1:] - cumul)
    block_states = jnp.einsum('clgn,clgrp->cgrpn', writes, inputs * tails[..., None], precision=highest)
    block_decay = jnp.exp(cumul[:, -1])

    def advance(state, pieces):
        factor, added = pieces
        return (factor[..., None, None] * state + added, state)
    final, before = lax.scan(advance, entering.reshape(groups, per_group, HEAD_DIM, STATE), (block_decay, block_states))
    carried = jnp.einsum('clgn,cgrpn->clgrp', reads, before, precision=highest) * jnp.exp(cumul)[..., None]
    return ((inner + carried).reshape(length, heads * HEAD_DIM), final.reshape(heads, HEAD_DIM, STATE))

def expert_pass(pieces):
    rows, scaled, gate_weight, up_weight, down_weight = pieces
    gate_pre = jnp.dot(rows, gate_weight, preferred_element_type=jnp.float32)
    up_pre = jnp.dot(rows, up_weight, preferred_element_type=jnp.float32)
    sigma = jax.nn.sigmoid(gate_pre)
    hidden = (jax.nn.silu(gate_pre) * up_pre).astype(jnp.bfloat16)
    grad_down = jnp.dot(hidden.T, scaled, preferred_element_type=jnp.float32).astype(jnp.bfloat16)
    d_hidden = jnp.dot(scaled, down_weight.T, preferred_element_type=jnp.float32)
    d_gate = (d_hidden * up_pre * sigma * (1.0 + gate_pre * (1.0 - sigma))).astype(jnp.bfloat16)
    d_up = (d_hidden * jax.nn.silu(gate_pre)).astype(jnp.bfloat16)
    grad_gate = jnp.dot(rows.T, d_gate, preferred_element_type=jnp.float32).astype(jnp.bfloat16)
    grad_up = jnp.dot(rows.T, d_up, preferred_element_type=jnp.float32).astype(jnp.bfloat16)
    number = rows.shape[0]
    width = gate_weight.shape[0]
    value_portion = jnp.einsum('rqf,dqf->qrd', d_gate.astype(jnp.float32).reshape(number, N_TP, -1), gate_weight.astype(jnp.float32).reshape(width, N_TP, -1))
    value_portion = value_portion + jnp.einsum('rqf,dqf->qrd', d_up.astype(jnp.float32).reshape(number, N_TP, -1), up_weight.astype(jnp.float32).reshape(width, N_TP, -1))
    rounded = lax.optimization_barrier(value_portion.astype(jnp.bfloat16)).astype(jnp.float32)
    return (grad_gate, grad_up, grad_down, lax.optimization_barrier(jnp.sum(rounded, axis=0)).astype(jnp.bfloat16))

def reference(token_values, write_keys, read_keys, log_decay, out_gate, out_proj, mixed, cotangent, route_ids, route_weights, w_gate, w_up, w_down):
    width = mixed.shape[1]
    flat_ids = route_ids.reshape(-1).astype(jnp.int32)
    pairs = flat_ids.shape[0]
    source = jnp.arange(pairs, dtype=jnp.int32) // (TOP * TOK_DEV)
    member = (flat_ids[:, None] == jnp.arange(EXPERTS, dtype=jnp.int32)[None, :]).astype(jnp.int32)
    blocked = member.reshape(N_SP, TOP * TOK_DEV, EXPERTS)
    earlier = (jnp.cumsum(blocked, axis=1).astype(jnp.int32) - blocked).reshape(pairs, EXPERTS)
    slot_index = lax.optimization_barrier(jnp.sum(earlier * member, axis=1)).astype(jnp.int32)
    target = ((flat_ids * N_SP + source) * CAP + slot_index).astype(jnp.int32)
    copies = jnp.repeat(mixed, TOP, axis=0)
    scaled = (cotangent.astype(jnp.float32)[:, None, :] * route_weights[:, :, None]).reshape(pairs, width)
    scaled = scaled.astype(jnp.bfloat16)
    places = EXPERTS * N_SP * CAP
    incoming_rows = jnp.zeros((places, width), jnp.bfloat16).at[target].set(copies).reshape(EXPERTS, N_SP * CAP, width)
    scaled_in = jnp.zeros((places, width), jnp.bfloat16).at[target].set(scaled).reshape(EXPERTS, N_SP * CAP, width)
    grad_gate, grad_up, grad_down, row_grads = lax.map(expert_pass, (incoming_rows, scaled_in, w_gate, w_up, w_down))
    picked = jnp.take(row_grads.reshape(places, width), target, axis=0).astype(jnp.float32)
    picked = picked.reshape(-1, TOP, width)
    grad_mixed = (cotangent.astype(jnp.float32) + lax.optimization_barrier(jnp.sum(picked, axis=1))).astype(jnp.bfloat16)
    out_grad = jnp.dot(grad_mixed, out_proj, preferred_element_type=jnp.float32)
    entering = jnp.zeros((log_decay.shape[0], HEAD_DIM, STATE), jnp.float32)

    def whole_mix(values_in, writes_in, reads_in, gate_in):
        mixed_heads, final = mix_blocks(values_in, writes_in, reads_in, log_decay, entering)
        return mixed_heads * jax.nn.silu(gate_in)
    gated, pullback = jax.vjp(whole_mix, token_values.astype(jnp.float32), write_keys.astype(jnp.float32), read_keys.astype(jnp.float32), out_gate.astype(jnp.float32))
    d_values, d_writes, d_reads, d_gate = pullback(out_grad)
    gated_b = gated.astype(jnp.bfloat16)
    proj_grad = jnp.dot(grad_mixed.T, gated_b, preferred_element_type=jnp.float32)
    return (d_values.astype(jnp.bfloat16), d_writes.astype(jnp.bfloat16), d_reads.astype(jnp.bfloat16), d_gate.astype(jnp.bfloat16), proj_grad, grad_gate, grad_up, grad_down)
```

```python
import jax
import jax.numpy as jnp
from jax import lax
from jax.experimental import pallas as pl
from jax.experimental.pallas import tpu as pltpu
from jax.sharding import Mesh
from jax.sharding import PartitionSpec as P

HEAD_DIM = 64
STATE = 128
SP = ("sp_0", "sp_1")
F32 = jnp.float32
BF16 = jnp.bfloat16
highest = lax.Precision.HIGHEST


def nn(a, b):
    return lax.dot_general(a, b, (((1,), (0,)), ((), ())), preferred_element_type=F32)


def nt(a, b):
    return lax.dot_general(a, b, (((1,), (1,)), ((), ())), preferred_element_type=F32)


def tn(a, b):
    return lax.dot_general(a, b, (((0,), (0,)), ((), ())), preferred_element_type=F32)


def iota(shape, dim):
    return lax.broadcasted_iota(jnp.int32, shape, dim)


def slots(ids_t, experts):
    tokens = ids_t.shape[1]
    e = iota((experts, tokens), 0)
    member = (ids_t[0:1, :] == e) | (ids_t[1:2, :] == e)
    before = (iota((tokens, tokens), 0) < iota((tokens, tokens), 1)).astype(BF16)
    slot = nn(member.astype(BF16), before)
    return jnp.where(member, slot.astype(jnp.int32), -1)


def weight_rows(ids_t, w_t, experts):
    e = iota((experts, ids_t.shape[1]), 0)
    return jnp.where(ids_t[0:1, :] == e, w_t[0:1, :], 0.0) + jnp.where(
        ids_t[1:2, :] == e, w_t[1:2, :], 0.0
    )


def decays(ld):
    heads, tokens = ld.shape
    ld8 = jnp.concatenate([ld, jnp.zeros((8 - heads, tokens), F32)], axis=0)
    upto = (iota((tokens, tokens), 0) <= iota((tokens, tokens), 1)).astype(F32)
    row = lax.dot_general(
        ld8, upto, (((1,), (0,)), ((), ())), precision=highest, preferred_element_type=F32
    )
    col = lax.dot_general(
        upto, ld8, (((0,), (1,)), ((), ())), precision=highest, preferred_element_type=F32
    )
    return row, col


def by_lane(col, tokens, heads):
    lane = iota((tokens, 2 * HEAD_DIM), 1)
    return jnp.concatenate(
        [
            jnp.where(lane < HEAD_DIM, col[:, 2 * p : 2 * p + 1], col[:, 2 * p + 1 : 2 * p + 2])
            for p in range(heads // 2)
        ],
        axis=1,
    )


def span_weights(row, col, h, tokens):
    lower = iota((tokens, tokens), 0) >= iota((tokens, tokens), 1)
    return jnp.exp(jnp.where(lower, col[:, h : h + 1] - row[h : h + 1, :], -1e30))


def mix_local(x, b, c, row, col, heads):
    tokens = x.shape[0]
    scores = nt(c, b)
    first = iota((tokens, 2 * HEAD_DIM), 1) < HEAD_DIM
    ys = []
    for p in range(heads // 2):
        xp = x[:, 128 * p : 128 * p + 128]
        pair = [
            nn((scores * span_weights(row, col, 2 * p + i, tokens)).astype(BF16), xp)
            for i in range(2)
        ]
        ys.append(jnp.where(first, pair[0], pair[1]))
    tails = by_lane(jnp.exp(col[tokens - 1 : tokens, :] - col), tokens, heads)
    end = tn((x.astype(F32) * tails).astype(BF16), b)
    return jnp.concatenate(ys, axis=1), end


def mix_backward(x, b, c, gate, out_grad, y, row, col, entering, leaving, heads):
    tokens = x.shape[0]
    sigma = jax.nn.sigmoid(gate)
    g = out_grad * (gate * sigma)
    d_gate = out_grad * y * sigma * (1.0 + gate * (1.0 - sigma))
    gb = g.astype(BF16)
    scores = nt(c, b)
    first = iota((tokens, 2 * HEAD_DIM), 1) < HEAD_DIM
    d_scores = jnp.zeros((tokens, tokens), F32)
    dxs = []
    for p in range(heads // 2):
        xp = x[:, 128 * p : 128 * p + 128]
        gp = gb[:, 128 * p : 128 * p + 128]
        pair = []
        for i in range(2):
            w = span_weights(row, col, 2 * p + i, tokens)
            mine = first if i == 0 else jnp.logical_not(first)
            d_scores = d_scores + w * nt(jnp.where(mine, gp, jnp.zeros_like(gp)), xp)
            pair.append(tn((scores * w).astype(BF16), gp))
        dxs.append(jnp.where(first, pair[0], pair[1]))
    tails = by_lane(jnp.exp(col[tokens - 1 : tokens, :] - col), tokens, heads)
    leads = by_lane(jnp.exp(col), tokens, heads)
    d_x = jnp.concatenate(dxs, axis=1) + tails * nt(b, leaving)
    ds = d_scores.astype(BF16)
    d_c = nn(ds, b) + nn((g * leads).astype(BF16), entering)
    d_b = tn(ds, c) + nn((x.astype(F32) * tails).astype(BF16), leaving)
    return d_x, d_b, d_c, d_gate


def prep_kernel(experts, cap, heads, ids, wts, mixed, cot, ld, x, b, c, send, hot, y, end):
    slot = slots(ids[...], experts)
    weights = weight_rows(ids[...], wts[...], experts)
    tokens = slot.shape[1]
    place = iota((cap, tokens), 0)
    for e in range(experts):
        mine = place == slot[e : e + 1, :]
        one = mine.astype(BF16)
        hot[e * cap : (e + 1) * cap, :] = one
        send[e, 0:cap, :] = nn(one, mixed[...]).astype(BF16)
        w = jnp.sum(jnp.where(mine, weights[e : e + 1, :], 0.0), axis=1, keepdims=True)
        send[e, cap : 2 * cap, :] = (nn(one, cot[...]) * w).astype(BF16)
    row, col = decays(ld[...])
    inner, last = mix_local(x[...], b[...], c[...], row, col, heads)
    y[...] = inner
    end[...] = last


def combine_kernel(hot, came, cot, out):
    out[...] = (cot[...].astype(F32) + tn(hot[...], came[...])).astype(BF16)


def carried_kernel(heads, ld, c, gate, y_inner, entering, out_grad, y, gated, back):
    row, col = decays(ld[...])
    tokens = y_inner.shape[0]
    leads = by_lane(jnp.exp(col), tokens, heads)
    whole = y_inner[...] + leads * nt(c[...], entering[...])
    g = gate[...].astype(F32)
    silu = g * jax.nn.sigmoid(g)
    y[...] = whole
    gated[...] = (whole * silu).astype(BF16)
    back[...] = tn((out_grad[...] * silu * leads).astype(BF16), c[...])


def backward_kernel(heads, ld, x, b, c, gate, og, y, entering, leaving, dx, db, dc, dg):
    row, col = decays(ld[...])
    d_x, d_b, d_c, d_g = mix_backward(
        x[...],
        b[...],
        c[...],
        gate[...].astype(F32),
        og[...],
        y[...],
        row,
        col,
        entering[...],
        leaving[...],
        heads,
    )
    dx[...] = d_x.astype(BF16)
    db[...] = d_b.astype(BF16)
    dc[...] = d_c.astype(BF16)
    dg[...] = d_g.astype(BF16)


def call(kernel, outs, *args, name):
    vmem = pl.BlockSpec(memory_space=pltpu.VMEM)
    return pl.pallas_call(
        kernel,
        out_shape=[jax.ShapeDtypeStruct(s, d) for s, d in outs],
        in_specs=[vmem] * len(args),
        out_specs=[vmem] * len(outs),
        compiler_params=pltpu.CompilerParams(vmem_limit_bytes=24 * 2**20),
        name=name,
    )(*args)


def nothing_yet(array, identity):
    return jax.tree.map(
        lambda a, e: jnp.broadcast_to(jnp.asarray(e, a.dtype), a.shape), array, identity
    )


def prefix_by_axis(array, axes, combine, identity, reverse):
    before = start = nothing_yet(array, identity)
    so_far = array
    for axis in reversed(axes):
        length, position = (lax.axis_size(axis), lax.axis_index(axis))
        pieces = jax.tree.map(
            lambda part, kind: lax.all_gather(part.astype(kind), axis),
            so_far,
            (BF16, BF16),
        )
        inside, so_far = (start, start)
        for k in reversed(range(length)) if reverse else range(length):
            passed = k > position if reverse else k < position
            so_far = combine(
                so_far, jax.tree.map(lambda part, own: part[k].astype(own.dtype), pieces, array)
            )
            inside = jax.tree.map(lambda new, old: jnp.where(passed, new, old), so_far, inside)
        before = combine(inside, before)
    return before


def forward_join(earlier, later):
    return (earlier[0] + later[0], jnp.exp(later[0])[..., None, None] * earlier[1] + later[1])


def backward_join(earlier, later):
    return (earlier[0] + later[0], later[1] + jnp.exp(later[0])[..., None, None] * earlier[1])


def expert_backward(rows, scaled, gate_weight, up_weight, down_weight):
    gate_pre = nn(rows, gate_weight)
    up_pre = nn(rows, up_weight)
    sigma = jax.nn.sigmoid(gate_pre)
    hidden = (gate_pre * sigma * up_pre).astype(BF16)
    d_hidden = nt(scaled, down_weight)
    d_gate = (d_hidden * up_pre * sigma * (1.0 + gate_pre * (1.0 - sigma))).astype(BF16)
    d_up = (d_hidden * (gate_pre * sigma)).astype(BF16)
    portion = nt(d_gate, gate_weight) + nt(d_up, up_weight)
    return (
        tn(rows, d_gate).astype(BF16),
        tn(rows, d_up).astype(BF16),
        tn(hidden, scaled).astype(BF16),
        portion.astype(BF16),
    )


def body(
    token_values,
    write_keys,
    read_keys,
    log_decay,
    out_gate,
    out_proj,
    mixed,
    cotangent,
    route_ids,
    route_weights,
    w_gate,
    w_up,
    w_down,
):
    tokens, width = mixed.shape
    experts = lax.axis_size(SP)
    cap = 3 * tokens // experts
    places = experts * cap
    heads = log_decay.shape[0]
    channels = token_values.shape[1]
    share = width // lax.axis_size("tp")
    offset = lax.axis_index("tp") * share
    mixed_part = lax.dynamic_slice_in_dim(mixed, offset, share, 1)
    cot_part = lax.dynamic_slice_in_dim(cotangent, offset, share, 1)

    def prep(*refs):
        prep_kernel(experts, cap, heads, *refs)

    send, hot, y_inner, local_end = call(
        prep,
        [
            ((experts, 2 * cap, share), BF16),
            ((places, tokens), BF16),
            ((tokens, channels), F32),
            ((channels, STATE), F32),
        ],
        route_ids.T,
        route_weights.T,
        mixed_part,
        cot_part,
        log_decay,
        token_values,
        write_keys,
        read_keys,
        name="prep",
    )
    got = lax.all_to_all(send, SP, split_axis=0, concat_axis=0, tiled=True)
    rows = lax.all_gather(got, "tp", axis=2, tiled=True)
    grads = expert_backward(
        rows[:, :cap].reshape(places, width),
        rows[:, cap:].reshape(places, width),
        w_gate[0],
        w_up[0],
        w_down[0],
    )
    summed = lax.psum_scatter(
        grads[3].reshape(experts, cap, width), "tp", scatter_dimension=2, tiled=True
    )
    came = lax.all_to_all(summed, SP, split_axis=0, concat_axis=0, tiled=True)
    (grad_part,) = call(
        combine_kernel,
        [((tokens, share), BF16)],
        hot,
        came.reshape(places, share),
        cot_part,
        name="combine",
    )
    grad_mixed = lax.all_gather(grad_part, "tp", axis=1, tiled=True)
    out_grad = nn(grad_mixed, out_proj)

    total = jnp.sum(log_decay, axis=1)
    zero_total = jnp.zeros_like(total)
    zero_state = jnp.zeros((heads, HEAD_DIM, STATE), F32)
    shape = (heads, HEAD_DIM, STATE)
    entering = prefix_by_axis(
        (total, local_end.reshape(shape)), SP, forward_join, (zero_total, zero_state), False
    )[1]
    entering = entering.reshape(channels, STATE).astype(BF16)

    def carried(*refs):
        carried_kernel(heads, *refs)

    y, gated, local_back = call(
        carried,
        [((tokens, channels), F32), ((tokens, channels), BF16), ((channels, STATE), F32)],
        log_decay,
        read_keys,
        out_gate,
        y_inner,
        entering,
        out_grad,
        name="carried",
    )
    proj_part = tn(grad_mixed, gated).astype(BF16).reshape(experts, -1, channels)
    proj_came = lax.all_to_all(proj_part, SP, split_axis=0, concat_axis=0, tiled=True)
    proj_grad = proj_came.astype(F32).sum(axis=0)
    leaving = prefix_by_axis(
        (total, local_back.reshape(shape)), SP, backward_join, (zero_total, zero_state), True
    )[1]
    leaving = leaving.reshape(channels, STATE).astype(BF16)

    def backward(*refs):
        backward_kernel(heads, *refs)

    d_values, d_writes, d_reads, d_gate = call(
        backward,
        [(a.shape, BF16) for a in (token_values, write_keys, read_keys, out_gate)],
        log_decay,
        token_values,
        write_keys,
        read_keys,
        out_gate,
        out_grad,
        y,
        entering,
        leaving,
        name="backward",
    )
    return (
        d_values,
        d_writes,
        d_reads,
        d_gate,
        proj_grad,
        grads[0][None],
        grads[1][None],
        grads[2][None],
    )


def solution(mesh):
    finer = Mesh(mesh.devices.reshape(4, 4, mesh.shape["tp"]), ("sp_0", "sp_1", "tp"))
    return jax.shard_map(
        body,
        mesh=finer,
        in_specs=(
            P(SP, "tp"),
            P(SP, "tp"),
            P(SP, "tp"),
            P("tp", SP),
            P(SP, "tp"),
            P(None, "tp"),
            P(SP, None),
            P(SP, None),
            P(SP, None),
            P(SP, None),
            P(SP, None, "tp"),
            P(SP, None, "tp"),
            P(SP, "tp", None),
        ),
        out_specs=(
            P(SP, "tp"),
            P(SP, "tp"),
            P(SP, "tp"),
            P(SP, "tp"),
            P(SP, "tp"),
            P(SP, None, "tp"),
            P(SP, None, "tp"),
            P(SP, "tp", None),
        ),
        check_vma=False,
    )
```

```python
import jax
import jax.numpy as jnp
from jax import lax
from jax.experimental import pallas as pl
from jax.experimental.pallas import tpu as pltpu
from jax.sharding import Mesh
from jax.sharding import PartitionSpec as P

HEAD_DIM = 64
STATE = 128
SP = ("sp_0", "sp_1")
F32 = jnp.float32
BF16 = jnp.bfloat16
highest = lax.Precision.HIGHEST


def nn(a, b):
    return lax.dot_general(a, b, (((1,), (0,)), ((), ())), preferred_element_type=F32)


def nt(a, b):
    return lax.dot_general(a, b, (((1,), (1,)), ((), ())), preferred_element_type=F32)


def tn(a, b):
    return lax.dot_general(a, b, (((0,), (0,)), ((), ())), preferred_element_type=F32)


def iota(shape, dim):
    return lax.broadcasted_iota(jnp.int32, shape, dim)


def slots(ids_t, experts):
    tokens = ids_t.shape[1]
    e = iota((experts, tokens), 0)
    member = (ids_t[0:1, :] == e) | (ids_t[1:2, :] == e)
    before = (iota((tokens, tokens), 0) < iota((tokens, tokens), 1)).astype(BF16)
    slot = nn(member.astype(BF16), before)
    return jnp.where(member, slot.astype(jnp.int32), -1)


def weight_rows(ids_t, w_t, experts):
    e = iota((experts, ids_t.shape[1]), 0)
    return jnp.where(ids_t[0:1, :] == e, w_t[0:1, :], 0.0) + jnp.where(
        ids_t[1:2, :] == e, w_t[1:2, :], 0.0
    )


def decays(ld):
    heads, tokens = ld.shape
    ld8 = jnp.concatenate([ld, jnp.zeros((8 - heads, tokens), F32)], axis=0)
    upto = (iota((tokens, tokens), 0) <= iota((tokens, tokens), 1)).astype(F32)
    row = lax.dot_general(
        ld8, upto, (((1,), (0,)), ((), ())), precision=highest, preferred_element_type=F32
    )
    col = lax.dot_general(
        upto, ld8, (((0,), (1,)), ((), ())), precision=highest, preferred_element_type=F32
    )
    return row, col


def by_lane(col, tokens, heads):
    lane = iota((tokens, 2 * HEAD_DIM), 1)
    return jnp.concatenate(
        [
            jnp.where(lane < HEAD_DIM, col[:, 2 * p : 2 * p + 1], col[:, 2 * p + 1 : 2 * p + 2])
            for p in range(heads // 2)
        ],
        axis=1,
    )


def span_weights(row, col, h, tokens):
    lower = iota((tokens, tokens), 0) >= iota((tokens, tokens), 1)
    return jnp.exp(jnp.where(lower, col[:, h : h + 1] - row[h : h + 1, :], -1e30))


def mix_local(x, b, c, row, col, heads):
    tokens = x.shape[0]
    scores = nt(c, b)
    first = iota((tokens, 2 * HEAD_DIM), 1) < HEAD_DIM
    ys = []
    for p in range(heads // 2):
        xp = x[:, 128 * p : 128 * p + 128]
        pair = [
            nn((scores * span_weights(row, col, 2 * p + i, tokens)).astype(BF16), xp)
            for i in range(2)
        ]
        ys.append(jnp.where(first, pair[0], pair[1]))
    tails = by_lane(jnp.exp(col[tokens - 1 : tokens, :] - col), tokens, heads)
    end = tn((x.astype(F32) * tails).astype(BF16), b)
    return jnp.concatenate(ys, axis=1), end


def mix_backward(x, b, c, gate, out_grad, y, row, col, entering, leaving, heads):
    tokens = x.shape[0]
    sigma = jax.nn.sigmoid(gate)
    g = out_grad * (gate * sigma)
    d_gate = out_grad * y * sigma * (1.0 + gate * (1.0 - sigma))
    gb = g.astype(BF16)
    scores = nt(c, b)
    first = iota((tokens, 2 * HEAD_DIM), 1) < HEAD_DIM
    d_scores = jnp.zeros((tokens, tokens), F32)
    dxs = []
    for p in range(heads // 2):
        xp = x[:, 128 * p : 128 * p + 128]
        gp = gb[:, 128 * p : 128 * p + 128]
        pair = []
        for i in range(2):
            w = span_weights(row, col, 2 * p + i, tokens)
            mine = first if i == 0 else jnp.logical_not(first)
            d_scores = d_scores + w * nt(jnp.where(mine, gp, jnp.zeros_like(gp)), xp)
            pair.append(tn((scores * w).astype(BF16), gp))
        dxs.append(jnp.where(first, pair[0], pair[1]))
    tails = by_lane(jnp.exp(col[tokens - 1 : tokens, :] - col), tokens, heads)
    leads = by_lane(jnp.exp(col), tokens, heads)
    d_x = jnp.concatenate(dxs, axis=1) + tails * nt(b, leaving)
    ds = d_scores.astype(BF16)
    d_c = nn(ds, b) + nn((g * leads).astype(BF16), entering)
    d_b = tn(ds, c) + nn((x.astype(F32) * tails).astype(BF16), leaving)
    return d_x, d_b, d_c, d_gate


def carried_kernel(heads, ld, c, gate, y_inner, entering, out_grad, y, gated, back):
    row, col = decays(ld[...])
    tokens = y_inner.shape[0]
    leads = by_lane(jnp.exp(col), tokens, heads)
    whole = y_inner[...] + leads * nt(c[...], entering[...])
    g = gate[...].astype(F32)
    silu = g * jax.nn.sigmoid(g)
    y[...] = whole
    gated[...] = (whole * silu).astype(BF16)
    back[...] = tn((out_grad[...] * silu * leads).astype(BF16), c[...])


def backward_kernel(heads, ld, x, b, c, gate, og, y, entering, leaving, dx, db, dc, dg):
    row, col = decays(ld[...])
    d_x, d_b, d_c, d_g = mix_backward(
        x[...],
        b[...],
        c[...],
        gate[...].astype(F32),
        og[...],
        y[...],
        row,
        col,
        entering[...],
        leaving[...],
        heads,
    )
    dx[...] = d_x.astype(BF16)
    db[...] = d_b.astype(BF16)
    dc[...] = d_c.astype(BF16)
    dg[...] = d_g.astype(BF16)


MESH = pl.DeviceIdType.MESH
GROUPS_OF = 4


def remote(src, dst, send, recv, device):
    return pltpu.make_async_remote_copy(
        src_ref=src, dst_ref=dst, send_sem=send, recv_sem=recv, device_id=device, device_id_type=MESH
    )


def moe_kernel(
    heads,
    ids,
    wts,
    ld,
    x_in,
    b_in,
    c_in,
    mixed,
    cot,
    wg_hbm,
    wu_hbm,
    wd_hbm,
    gm,
    y_out,
    end_out,
    gg_hbm,
    gu_hbm,
    gd_hbm,
    mixed_q,
    cot_q,
    cot_own,
    wg,
    wu,
    wd,
    slot_ref,
    weight_ref,
    hot,
    sendbuf,
    rows,
    act,
    dgate,
    dup,
    part,
    part_in,
    q1,
    y1,
    q2,
    y2,
    fin,
    ret,
    gg,
    gu,
    gd,
    local,
    a_send,
    a_recv,
    yr_send,
    yr_recv,
    ys_send,
    ys_recv,
    pa_send,
    pa_recv,
    pn_send,
    pn_recv,
    d_send,
    d_recv,
    s1_send,
    s1_recv,
    s2_send,
    s2_recv,
    c_send,
    c_recv,
    g_send,
    g_recv,
):
    z, x, t = lax.axis_index("sp_0"), lax.axis_index("sp_1"), lax.axis_index("tp")
    s = 4 * z + x
    y, core = t // 2, t % 2
    quarter = t % 4
    beside = (quarter + 2) % 4
    partner_q = quarter + 1 - 2 * core
    partner_beside = (partner_q + 2) % 4
    up, down, partner = (z, x, (t + 2) % 8), (z, x, (t + 6) % 8), (z, x, t + 1 - 2 * core)
    tokens, width = mixed.shape
    experts, _, cap, share = sendbuf.shape
    own = width // 8

    loads = [
        pltpu.make_async_copy(mixed.at[:, pl.ds(quarter * share, share)], mixed_q, local.at[0]),
        pltpu.make_async_copy(cot.at[:, pl.ds(quarter * share, share)], cot_q, local.at[1]),
        pltpu.make_async_copy(cot.at[:, pl.ds(t * own, own)], cot_own, local.at[2]),
        pltpu.make_async_copy(wg_hbm, wg, local.at[3]),
        pltpu.make_async_copy(wu_hbm, wu, local.at[4]),
        pltpu.make_async_copy(wd_hbm, wd, local.at[5]),
    ]
    for load in loads:
        load.start()

    barrier = pltpu.get_barrier_semaphore()

    def greet(k, carry):
        j = (s + k) % experts
        pl.semaphore_signal(barrier, inc=1, device_id=(j // 4, j % 4, t), device_id_type=MESH)
        return carry

    lax.fori_loop(1, experts, greet, 0)
    for device in (up, down, partner):
        pl.semaphore_signal(barrier, inc=1, device_id=device, device_id_type=MESH)

    slot_ref[...] = slots(ids[...], experts)
    weight_ref[...] = weight_rows(ids[...], wts[...], experts)
    loads[0].wait()
    loads[1].wait()
    pl.semaphore_wait(barrier, experts - 1 + 3)

    def to_expert(e):
        return remote(
            sendbuf.at[e], rows.at[quarter, s], a_send.at[e], a_recv.at[s], (e // 4, e % 4, t)
        )

    def build(g, carry):
        block = (z + g) % 4
        place = iota((cap, tokens), 0)
        ones, ws = [], []
        for k in range(4):
            e = 4 * block + k
            mine = place == slot_ref[pl.ds(e, 1), :]
            one = mine.astype(BF16)
            hot[e] = one
            ones.append(one)
            w = jnp.where(mine, weight_ref[pl.ds(e, 1), :], 0.0)
            ws.append(jnp.sum(w, axis=1, keepdims=True))
        one = jnp.concatenate(ones, axis=0)
        w = jnp.concatenate(ws, axis=0)
        here = pl.ds(4 * block, 4)
        sendbuf[here, 0] = nn(one, mixed_q[...]).astype(BF16).reshape(4, cap, share)
        sendbuf[here, 1] = (nn(one, cot_q[...]) * w).astype(BF16).reshape(4, cap, share)
        for j in range(4):
            e = 4 * block + (x + j) % 4
            if j > 0:
                to_expert(e).start()
            else:

                @pl.when(g > 0)
                def _():
                    to_expert(e).start()

        return carry

    lax.fori_loop(0, 4, build, 0)
    rows[quarter, s] = sendbuf[s]

    row, col = decays(ld[...])
    inner, last = mix_local(x_in[...], b_in[...], c_in[...], row, col, heads)
    y_out[...] = inner
    end_out[...] = last
    for load in loads[2:]:
        load.wait()

    def source(g, j):
        return 4 * ((z + 4 - g) % 4) + (x + 4 - j) % 4

    def arrived(src):
        return remote(sendbuf.at[src], rows.at[quarter, src], a_send.at[src], a_recv.at[src], up)

    def rows_up(src, q):
        return remote(
            rows.at[q, src, 0], rows.at[q, src, 0], yr_send.at[src], yr_recv.at[src], up
        )

    def scaled_down(src, q):
        return remote(
            rows.at[q, src, 1], rows.at[q, src, 1], ys_send.at[src], ys_recv.at[src], down
        )

    def across(src, q):
        return remote(rows.at[q, src], rows.at[q, src], pa_send.at[src], pa_recv.at[src], partner)

    def across_beside(src, q):
        return remote(rows.at[q, src], rows.at[q, src], pn_send.at[src], pn_recv.at[src], partner)

    def forward_own(g):
        for j in range(4):
            src = source(g, j)
            if j > 0:
                arrived(src).wait_recv()
            else:

                @pl.when(g > 0)
                def _():
                    arrived(src).wait_recv()

            rows_up(src, quarter).start()
            scaled_down(src, quarter).start()
            across(src, quarter).start()

    def forward_beside(g):
        for j in range(4):
            src = source(g, j)
            rows_up(src, beside).wait_recv()
            scaled_down(src, beside).wait_recv()
            across_beside(src, beside).start()

    def halves_across(g):
        return remote(
            part.at[g, 1 - core], part_in.at[g], d_send.at[g], d_recv.at[g], partner
        )

    def compute(g):
        block = (z + 4 - g) % 4
        for j in range(4):
            src = source(g, j)
            across(src, partner_q).wait_recv()
            across_beside(src, partner_beside).wait_recv()
        here = pl.ds(4 * block, 4)
        n = 4 * cap
        gate_pre = up_pre = d_hidden = jnp.zeros((n, wg.shape[1]), F32)
        for q in range(4):
            r = rows[q, here, 0].reshape(n, share)
            sc = rows[q, here, 1].reshape(n, share)
            f = slice(q * share, (q + 1) * share)
            gate_pre = gate_pre + nn(r, wg[f, :])
            up_pre = up_pre + nn(r, wu[f, :])
            d_hidden = d_hidden + nt(sc, wd[:, f])
        sigma = jax.nn.sigmoid(gate_pre)
        silu = gate_pre * sigma
        dg = (d_hidden * up_pre * sigma * (1.0 + gate_pre * (1.0 - sigma))).astype(BF16)
        du = (d_hidden * silu).astype(BF16)
        act[block] = (silu * up_pre).astype(BF16)
        dgate[block] = dg
        dup[block] = du
        for k in range(8):
            f = slice(k * own, (k + 1) * own)
            part[g, k % 2, k // 2] = (nt(dg, wg[f, :]) + nt(du, wu[f, :])).astype(BF16)
        halves_across(g).start()

    def both(g, f):
        return part[g, core, f].astype(F32) + part_in[g, f].astype(F32)

    half = 2 * cap

    def first_step(g, way):
        return remote(
            q1.at[g, way], y1.at[g, way], s1_send.at[g, way], s1_recv.at[g, way], (up, down)[way]
        )

    def second_step(g, way):
        return remote(
            q2.at[g, way], y2.at[g, way], s2_send.at[g, way], s2_recv.at[g, way], (up, down)[way]
        )

    def sum_far(g):
        halves_across(g).wait_recv()
        far = both(g, (y + 2) % 4)
        q1[g, 0] = far[:half].astype(BF16)
        q1[g, 1] = far[half:].astype(BF16)
        first_step(g, 0).start()
        first_step(g, 1).start()

    def sum_near(g):
        first_step(g, 0).wait_recv()
        above = both(g, (y + 1) % 4)
        q2[g, 0, :half] = (above[:half] + y1[g, 0].astype(F32)).astype(BF16)
        q2[g, 0, half:] = above[half:].astype(BF16)
        second_step(g, 0).start()
        first_step(g, 1).wait_recv()
        below = both(g, (y + 3) % 4)
        q2[g, 1, :half] = below[:half].astype(BF16)
        q2[g, 1, half:] = (below[half:] + y1[g, 1].astype(F32)).astype(BF16)
        second_step(g, 1).start()

    def to_owner(g, src):
        return remote(
            fin.at[src], ret.at[s], c_send.at[src], c_recv.at[s], (src // 4, src % 4, t)
        )

    def from_expert(e):
        return remote(fin.at[e], ret.at[e], c_send.at[e], c_recv.at[e], up)

    def sum_own(g):
        second_step(g, 0).wait_recv()
        second_step(g, 1).wait_recv()
        block = (z + 4 - g) % 4
        total = both(g, y) + y2[g, 0].astype(F32) + y2[g, 1].astype(F32)
        fin[pl.ds(4 * block, 4)] = total.astype(BF16).reshape(4, cap, own)
        for j in range(4):
            src = source(g, j)
            if j > 0:
                to_owner(g, src).start()
            else:

                @pl.when(g > 0)
                def _():
                    to_owner(g, src).start()

                @pl.when(g == 0)
                def _():
                    ret[s] = fin[s]

    def grad_rows(target, which):
        for q in range(4):
            r = rows[q, :, 0].reshape(experts * cap, share)
            target[q * share : (q + 1) * share, :] = tn(
                r, which[...].reshape(experts * cap, -1)
            ).astype(BF16)

    def grad_down():
        hidden = act[...].reshape(experts * cap, -1)
        for q in range(4):
            sc = rows[q, :, 1].reshape(experts * cap, share)
            gd[:, q * share : (q + 1) * share] = tn(hidden, sc).astype(BF16)

    stores = [
        pltpu.make_async_copy(gg, gg_hbm, local.at[6]),
        pltpu.make_async_copy(gu, gu_hbm, local.at[7]),
        pltpu.make_async_copy(gd, gd_hbm, local.at[8]),
    ]

    def turn(n, carry):
        for lag, task in enumerate(
            (forward_own, forward_beside, compute, sum_far, sum_near, sum_own)
        ):

            @pl.when((n >= lag) & (n < lag + 4))
            def _():
                task(n - lag)

        @pl.when(n == 5)
        def _():
            grad_rows(gg, dgate)
            stores[0].start()

        @pl.when(n == 6)
        def _():
            grad_rows(gu, dup)
            stores[1].start()

        @pl.when(n == 7)
        def _():
            grad_down()
            stores[2].start()

        return carry

    lax.fori_loop(0, 9, turn, 0)

    def take(k, carry):
        from_expert((s + k) % experts).wait_recv()
        return carry

    lax.fori_loop(1, experts, take, 0)
    places = experts * cap
    picked = tn(hot[...].reshape(places, tokens), ret[...].reshape(places, own))
    gm[t] = (cot_own[...].astype(F32) + picked).astype(BF16)

    low, high = pl.ds(0, tokens // 2), pl.ds(tokens // 2, tokens // 2)
    below, above, far = (t + 6) % 8, (t + 2) % 8, (t + 4) % 8
    mate = t + 1 - 2 * core
    m_below, m_above, m_far = (mate + 6) % 8, (mate + 2) % 8, (mate + 4) % 8

    def gather(k, src, device, part_rows=None):
        ref = gm.at[src] if part_rows is None else gm.at[src, part_rows]
        return remote(ref, ref, g_send.at[k], g_recv.at[k], device)

    gather(1, t, up).start()
    gather(2, t, down).start()
    gather(0, t, partner).start()
    gather(1, below, up).wait_recv()
    gather(3, below, up, low).start()
    gather(5, below, partner).start()
    gather(2, above, down).wait_recv()
    gather(4, above, down, high).start()
    gather(6, above, partner).start()
    gather(3, far, up, low).wait_recv()
    gather(4, far, down, high).wait_recv()
    gather(7, far, partner).start()
    gather(0, mate, partner).wait_recv()
    gather(5, m_below, partner).wait_recv()
    gather(6, m_above, partner).wait_recv()
    gather(7, m_far, partner).wait_recv()

    def sent(k, carry):
        e = (s + k) % experts
        to_expert(e).wait_send()
        to_owner(0, e).wait_send()
        return carry

    lax.fori_loop(1, experts, sent, 0)

    def forwarded(k, carry):
        rows_up(k, quarter).wait_send()
        scaled_down(k, quarter).wait_send()
        across(k, quarter).wait_send()
        across_beside(k, beside).wait_send()
        return carry

    lax.fori_loop(0, experts, forwarded, 0)

    def summed(g, carry):
        halves_across(g).wait_send()
        for way in range(2):
            first_step(g, way).wait_send()
            second_step(g, way).wait_send()
        return carry

    lax.fori_loop(0, 4, summed, 0)
    gather(0, t, partner).wait_send()
    gather(1, t, up).wait_send()
    gather(2, t, down).wait_send()
    gather(3, below, up, low).wait_send()
    gather(4, above, down, high).wait_send()
    gather(5, below, partner).wait_send()
    gather(6, above, partner).wait_send()
    gather(7, far, partner).wait_send()
    for store in stores:
        store.wait()


def moe(ids, wts, ld, x, b, c, mixed, cot, wg, wu, wd, experts, cap, heads):
    tokens, width = mixed.shape
    hidden = wg.shape[1]
    share, own = width // 4, width // 8
    vmem = pl.BlockSpec(memory_space=pltpu.VMEM)
    hbm = pl.BlockSpec(memory_space=pl.ANY)
    dma = pltpu.SemaphoreType.DMA

    def kernel(*refs):
        moe_kernel(heads, *refs)

    def buf(*shape, dtype=BF16):
        return pltpu.VMEM(shape, dtype)

    n = 4 * cap
    return pl.pallas_call(
        kernel,
        out_shape=[
            jax.ShapeDtypeStruct((8, tokens, own), BF16),
            jax.ShapeDtypeStruct(x.shape, F32),
            jax.ShapeDtypeStruct((x.shape[1], STATE), F32),
            jax.ShapeDtypeStruct(wg.shape, BF16),
            jax.ShapeDtypeStruct(wu.shape, BF16),
            jax.ShapeDtypeStruct(wd.shape, BF16),
        ],
        in_specs=[vmem] * 6 + [hbm] * 5,
        out_specs=[vmem] * 3 + [hbm] * 3,
        scratch_shapes=[
            buf(tokens, share),
            buf(tokens, share),
            buf(tokens, own),
            buf(*wg.shape),
            buf(*wu.shape),
            buf(*wd.shape),
            buf(experts, tokens, dtype=jnp.int32),
            buf(experts, tokens, dtype=F32),
            buf(experts, cap, tokens),
            buf(experts, 2, cap, share),
            buf(4, experts, 2, cap, share),
            buf(4, n, hidden),
            buf(4, n, hidden),
            buf(4, n, hidden),
            buf(4, 2, 4, n, own),
            buf(4, 4, n, own),
            buf(4, 2, n // 2, own),
            buf(4, 2, n // 2, own),
            buf(4, 2, n, own),
            buf(4, 2, n, own),
            buf(experts, cap, own),
            buf(experts, cap, own),
            buf(*wg.shape),
            buf(*wu.shape),
            buf(*wd.shape),
            dma((9,)),
        ]
        + [dma((experts,))] * 10
        + [dma((4,))] * 2
        + [dma((4, 2))] * 4
        + [dma((experts,))] * 2
        + [dma((8,))] * 2,
        compiler_params=pltpu.CompilerParams(
            collective_id=0, has_side_effects=True, vmem_limit_bytes=60 * 2**20
        ),
        name="moe",
    )(ids, wts, ld, x, b, c, mixed, cot, wg, wu, wd)


def call(kernel, outs, *args, name):
    vmem = pl.BlockSpec(memory_space=pltpu.VMEM)
    return pl.pallas_call(
        kernel,
        out_shape=[jax.ShapeDtypeStruct(s, d) for s, d in outs],
        in_specs=[vmem] * len(args),
        out_specs=[vmem] * len(outs),
        compiler_params=pltpu.CompilerParams(vmem_limit_bytes=24 * 2**20),
        name=name,
    )(*args)


def nothing_yet(array, identity):
    return jax.tree.map(
        lambda a, e: jnp.broadcast_to(jnp.asarray(e, a.dtype), a.shape), array, identity
    )


def prefix_by_axis(array, axes, combine, identity, reverse):
    before = start = nothing_yet(array, identity)
    so_far = array
    for axis in reversed(axes):
        length, position = (lax.axis_size(axis), lax.axis_index(axis))
        pieces = jax.tree.map(
            lambda part, kind: lax.all_gather(part.astype(kind), axis),
            so_far,
            (BF16, BF16),
        )
        inside, so_far = (start, start)
        for k in reversed(range(length)) if reverse else range(length):
            passed = k > position if reverse else k < position
            so_far = combine(
                so_far, jax.tree.map(lambda part, own: part[k].astype(own.dtype), pieces, array)
            )
            inside = jax.tree.map(lambda new, old: jnp.where(passed, new, old), so_far, inside)
        before = combine(inside, before)
    return before


def forward_join(earlier, later):
    return (earlier[0] + later[0], jnp.exp(later[0])[..., None, None] * earlier[1] + later[1])


def backward_join(earlier, later):
    return (earlier[0] + later[0], later[1] + jnp.exp(later[0])[..., None, None] * earlier[1])


def body(
    token_values,
    write_keys,
    read_keys,
    log_decay,
    out_gate,
    out_proj,
    mixed,
    cotangent,
    route_ids,
    route_weights,
    w_gate,
    w_up,
    w_down,
):
    tokens, width = mixed.shape
    experts = lax.axis_size(SP)
    cap = 3 * tokens // experts
    heads = log_decay.shape[0]
    channels = token_values.shape[1]
    gm, y_inner, local_end, *grads = moe(
        route_ids.T,
        route_weights.T,
        log_decay,
        token_values,
        write_keys,
        read_keys,
        mixed,
        cotangent,
        w_gate[0],
        w_up[0],
        w_down[0],
        experts,
        cap,
        heads,
    )
    grad_mixed = jnp.moveaxis(gm, 0, 1).reshape(tokens, width)
    out_grad = nn(grad_mixed, out_proj)

    total = jnp.sum(log_decay, axis=1)
    zero_total = jnp.zeros_like(total)
    zero_state = jnp.zeros((heads, HEAD_DIM, STATE), F32)
    shape = (heads, HEAD_DIM, STATE)
    entering = prefix_by_axis(
        (total, local_end.reshape(shape)), SP, forward_join, (zero_total, zero_state), False
    )[1]
    entering = entering.reshape(channels, STATE).astype(BF16)

    def carried(*refs):
        carried_kernel(heads, *refs)

    y, gated, local_back = call(
        carried,
        [((tokens, channels), F32), ((tokens, channels), BF16), ((channels, STATE), F32)],
        log_decay,
        read_keys,
        out_gate,
        y_inner,
        entering,
        out_grad,
        name="carried",
    )
    proj_part = tn(grad_mixed, gated).astype(BF16).reshape(experts, -1, channels)
    proj_came = lax.all_to_all(proj_part, SP, split_axis=0, concat_axis=0, tiled=True)
    proj_grad = proj_came.astype(F32).sum(axis=0)
    leaving = prefix_by_axis(
        (total, local_back.reshape(shape)), SP, backward_join, (zero_total, zero_state), True
    )[1]
    leaving = leaving.reshape(channels, STATE).astype(BF16)

    def backward(*refs):
        backward_kernel(heads, *refs)

    d_values, d_writes, d_reads, d_gate = call(
        backward,
        [(a.shape, BF16) for a in (token_values, write_keys, read_keys, out_gate)],
        log_decay,
        token_values,
        write_keys,
        read_keys,
        out_gate,
        out_grad,
        y,
        entering,
        leaving,
        name="backward",
    )
    return (
        d_values,
        d_writes,
        d_reads,
        d_gate,
        proj_grad,
        grads[0][None],
        grads[1][None],
        grads[2][None],
    )


def solution(mesh):
    finer = Mesh(mesh.devices.reshape(4, 4, mesh.shape["tp"]), ("sp_0", "sp_1", "tp"))
    return jax.shard_map(
        body,
        mesh=finer,
        in_specs=(
            P(SP, "tp"),
            P(SP, "tp"),
            P(SP, "tp"),
            P("tp", SP),
            P(SP, "tp"),
            P(None, "tp"),
            P(SP, None),
            P(SP, None),
            P(SP, None),
            P(SP, None),
            P(SP, None, "tp"),
            P(SP, None, "tp"),
            P(SP, "tp", None),
        ),
        out_specs=(
            P(SP, "tp"),
            P(SP, "tp"),
            P(SP, "tp"),
            P(SP, "tp"),
            P(SP, "tp"),
            P(SP, None, "tp"),
            P(SP, None, "tp"),
            P(SP, "tp", None),
        ),
        check_vma=False,
    )
```

```python
import jax
import jax.numpy as jnp
from jax import lax
from jax.experimental import pallas as pl
from jax.experimental.pallas import tpu as pltpu
from jax.sharding import Mesh
from jax.sharding import PartitionSpec as P

HEAD_DIM = 64
STATE = 128
SP = ("sp_0", "sp_1")
F32 = jnp.float32
BF16 = jnp.bfloat16
highest = lax.Precision.HIGHEST


def nn(a, b):
    return lax.dot_general(a, b, (((1,), (0,)), ((), ())), preferred_element_type=F32)


def nt(a, b):
    return lax.dot_general(a, b, (((1,), (1,)), ((), ())), preferred_element_type=F32)


def tn(a, b):
    return lax.dot_general(a, b, (((0,), (0,)), ((), ())), preferred_element_type=F32)


def iota(shape, dim):
    return lax.broadcasted_iota(jnp.int32, shape, dim)


def slots(ids_t, experts):
    tokens = ids_t.shape[1]
    e = iota((experts, tokens), 0)
    member = (ids_t[0:1, :] == e) | (ids_t[1:2, :] == e)
    before = (iota((tokens, tokens), 0) < iota((tokens, tokens), 1)).astype(BF16)
    slot = nn(member.astype(BF16), before)
    return jnp.where(member, slot.astype(jnp.int32), -1)


def weight_rows(ids_t, w_t, experts):
    e = iota((experts, ids_t.shape[1]), 0)
    return jnp.where(ids_t[0:1, :] == e, w_t[0:1, :], 0.0) + jnp.where(
        ids_t[1:2, :] == e, w_t[1:2, :], 0.0
    )


def decays(ld):
    heads, tokens = ld.shape
    ld8 = jnp.concatenate([ld, jnp.zeros((8 - heads, tokens), F32)], axis=0)
    upto = (iota((tokens, tokens), 0) <= iota((tokens, tokens), 1)).astype(F32)
    row = lax.dot_general(
        ld8, upto, (((1,), (0,)), ((), ())), precision=highest, preferred_element_type=F32
    )
    col = lax.dot_general(
        upto, ld8, (((0,), (1,)), ((), ())), precision=highest, preferred_element_type=F32
    )
    return row, col


def by_lane(col, tokens, heads):
    lane = iota((tokens, 2 * HEAD_DIM), 1)
    return jnp.concatenate(
        [
            jnp.where(lane < HEAD_DIM, col[:, 2 * p : 2 * p + 1], col[:, 2 * p + 1 : 2 * p + 2])
            for p in range(heads // 2)
        ],
        axis=1,
    )


def span_weights(row, col, h, tokens):
    lower = iota((tokens, tokens), 0) >= iota((tokens, tokens), 1)
    return jnp.exp(jnp.where(lower, col[:, h : h + 1] - row[h : h + 1, :], -1e30))


def mix_local(x, b, c, row, col, heads):
    tokens = x.shape[0]
    scores = nt(c, b)
    first = iota((tokens, 2 * HEAD_DIM), 1) < HEAD_DIM
    ys = []
    for p in range(heads // 2):
        xp = x[:, 128 * p : 128 * p + 128]
        pair = [
            nn((scores * span_weights(row, col, 2 * p + i, tokens)).astype(BF16), xp)
            for i in range(2)
        ]
        ys.append(jnp.where(first, pair[0], pair[1]))
    tails = by_lane(jnp.exp(col[tokens - 1 : tokens, :] - col), tokens, heads)
    end = tn((x.astype(F32) * tails).astype(BF16), b)
    return jnp.concatenate(ys, axis=1), end


def mix_backward(x, b, c, gate, out_grad, y, lead_grad, entering, row, col, heads):
    tokens = x.shape[0]
    sigma = jax.nn.sigmoid(gate)
    gb = (out_grad * (gate * sigma)).astype(BF16)
    d_gate = out_grad * y * sigma * (1.0 + gate * (1.0 - sigma))
    scores = nt(c, b)
    first = iota((tokens, 2 * HEAD_DIM), 1) < HEAD_DIM
    d_scores = jnp.zeros((tokens, tokens), F32)
    dxs = []
    for p in range(heads // 2):
        xp = x[:, 128 * p : 128 * p + 128]
        gp = gb[:, 128 * p : 128 * p + 128]
        pair = []
        for i in range(2):
            w = span_weights(row, col, 2 * p + i, tokens)
            mine = first if i == 0 else jnp.logical_not(first)
            d_scores = d_scores + w * nt(jnp.where(mine, gp, jnp.zeros_like(gp)), xp)
            pair.append(tn((scores * w).astype(BF16), gp))
        dxs.append(jnp.where(first, pair[0], pair[1]))
    ds = d_scores.astype(BF16)
    return jnp.concatenate(dxs, axis=1), tn(ds, c), nn(ds, b) + nn(lead_grad, entering), d_gate


MESH = pl.DeviceIdType.MESH
STEP = 16


def remote(src, dst, send, recv, device):
    return pltpu.make_async_remote_copy(
        src_ref=src, dst_ref=dst, send_sem=send, recv_sem=recv, device_id=device, device_id_type=MESH
    )


def moe_kernel(
    heads,
    ids,
    wts,
    ld,
    x_in,
    b_in,
    c_in,
    gate_in,
    mixed,
    cot,
    wg_hbm,
    wu_hbm,
    wd_hbm,
    op_hbm,
    dx_out,
    db_out,
    dc_out,
    dgate_out,
    proj_out,
    gg_hbm,
    gu_hbm,
    gd_hbm,
    gm,
    op,
    y_ref,
    gated,
    state_send,
    state_in,
    enter_send,
    enter,
    back_send,
    back_in,
    leave_send,
    leave,
    proj_send,
    proj_in,
    mixed_q,
    cot_q,
    cot_own,
    wg,
    wu,
    wd,
    slot_ref,
    weight_ref,
    hot,
    sendbuf,
    rows,
    act,
    dgate,
    dup,
    part,
    part_in,
    q1,
    y1,
    q2,
    y2,
    fin,
    ret,
    gg,
    gu,
    gd,
    local,
    a_send,
    a_recv,
    yr_send,
    yr_recv,
    ys_send,
    ys_recv,
    pa_send,
    pa_recv,
    pn_send,
    pn_recv,
    d_send,
    d_recv,
    s1_send,
    s1_recv,
    s2_send,
    s2_recv,
    c_send,
    c_recv,
    g_send,
    g_recv,
    e_send,
    e_recv,
    f_send,
    f_recv,
    b_send,
    b_recv,
    l_send,
    l_recv,
    p_send,
    p_recv,
):
    z, x, t = lax.axis_index("sp_0"), lax.axis_index("sp_1"), lax.axis_index("tp")
    s = 4 * z + x
    y, core = t // 2, t % 2
    quarter = t % 4
    beside = (quarter + 2) % 4
    partner_q = quarter + 1 - 2 * core
    partner_beside = (partner_q + 2) % 4
    up, down, partner = (z, x, (t + 2) % 8), (z, x, (t + 6) % 8), (z, x, t + 1 - 2 * core)
    tokens, width = mixed.shape
    experts, _, cap, share = sendbuf.shape
    own = width // 8

    loads = [
        pltpu.make_async_copy(mixed.at[:, pl.ds(quarter * share, share)], mixed_q, local.at[0]),
        pltpu.make_async_copy(cot.at[:, pl.ds(quarter * share, share)], cot_q, local.at[1]),
        pltpu.make_async_copy(cot.at[:, pl.ds(t * own, own)], cot_own, local.at[2]),
        pltpu.make_async_copy(wg_hbm, wg, local.at[3]),
        pltpu.make_async_copy(wu_hbm, wu, local.at[4]),
        pltpu.make_async_copy(wd_hbm, wd, local.at[5]),
        pltpu.make_async_copy(op_hbm, op, local.at[9]),
    ]
    for load in loads:
        load.start()

    barrier = pltpu.get_barrier_semaphore()

    def greet(k, carry):
        j = (s + k) % experts
        pl.semaphore_signal(barrier, inc=1, device_id=(j // 4, j % 4, t), device_id_type=MESH)
        return carry

    lax.fori_loop(1, experts, greet, 0)
    for device in (up, down, partner):
        pl.semaphore_signal(barrier, inc=1, device_id=device, device_id_type=MESH)

    slot_ref[...] = slots(ids[...], experts)
    weight_ref[...] = weight_rows(ids[...], wts[...], experts)
    loads[0].wait()
    loads[1].wait()
    pl.semaphore_wait(barrier, experts - 1 + 3)

    def to_expert(e):
        return remote(
            sendbuf.at[e], rows.at[quarter, s], a_send.at[e], a_recv.at[s], (e // 4, e % 4, t)
        )

    def build(g, carry):
        block = (z + g) % 4
        place = iota((cap, tokens), 0)
        ones, ws = [], []
        for k in range(4):
            e = 4 * block + k
            mine = place == slot_ref[pl.ds(e, 1), :]
            one = mine.astype(BF16)
            hot[e] = one
            ones.append(one)
            w = jnp.where(mine, weight_ref[pl.ds(e, 1), :], 0.0)
            ws.append(jnp.sum(w, axis=1, keepdims=True))
        one = jnp.concatenate(ones, axis=0)
        w = jnp.concatenate(ws, axis=0)
        here = pl.ds(4 * block, 4)
        sendbuf[here, 0] = nn(one, mixed_q[...]).astype(BF16).reshape(4, cap, share)
        sendbuf[here, 1] = (nn(one, cot_q[...]) * w).astype(BF16).reshape(4, cap, share)
        for j in range(4):
            e = 4 * block + (x + j) % 4
            if j > 0:
                to_expert(e).start()
            else:

                @pl.when(g > 0)
                def _():
                    to_expert(e).start()

        return carry

    lax.fori_loop(0, 4, build, 0)
    rows[quarter, s] = sendbuf[s]

    row, col = decays(ld[...])
    inner, last = mix_local(x_in[...], b_in[...], c_in[...], row, col, heads)
    y_ref[...] = inner
    totals = jnp.broadcast_to(row[:, tokens - 1 : tokens], (8, STATE))
    state_send[:, :STEP, :] = last.reshape(experts, STEP, STATE)
    state_send[:, STEP:, :] = jnp.broadcast_to(totals[None], (experts, 8, STATE))
    state_in[s] = state_send[s]

    def peer(k):
        j = (s + k) % experts
        return j, (j // 4, j % 4, t)

    def over_sp(source_ref, target_ref, send, recv):
        def copy(k):
            j, device = peer(k)
            return remote(source_ref.at[j], target_ref.at[s], send.at[j], recv.at[s], device)

        def wait(k):
            j, device = peer(k)
            remote(source_ref.at[j], target_ref.at[j], send.at[j], recv.at[j], device).wait_recv()

        def each(action):
            def step(k, carry):
                action(k)
                return carry

            lax.fori_loop(1, experts, step, 0)

        return (
            lambda: each(lambda k: copy(k).start()),
            lambda: each(wait),
            lambda: each(lambda k: copy(k).wait_send()),
        )

    states = over_sp(state_send, state_in, e_send, e_recv)
    enters = over_sp(enter_send, enter, f_send, f_recv)
    backs = over_sp(back_send, back_in, b_send, b_recv)
    leaves = over_sp(leave_send, leave, l_send, l_recv)
    states[0]()
    for load in loads[2:]:
        load.wait()

    def factor(src):
        return jnp.exp(state_in[src, pl.ds(STEP + s // 4, 1), :])

    def scan_forward():
        states[1]()
        held = jnp.zeros((STEP, STATE), F32)
        for src in range(experts):
            enter_send[src] = held.astype(BF16)
            held = factor(src) * held + state_in[src, :STEP, :]
        enter[s] = enter_send[s]
        enters[0]()

    def scan_back():
        backs[1]()
        held = jnp.zeros((STEP, STATE), F32)
        for src in reversed(range(experts)):
            leave_send[src] = held.astype(BF16)
            held = factor(src) * held + back_in[src].astype(F32)
        leave[s] = leave_send[s]
        leaves[0]()

    def finish_forward():
        enters[1]()
        _, col = decays(ld[...])
        leads = by_lane(jnp.exp(col), tokens, heads)
        entering = enter[...].reshape(x_in.shape[1], STATE)
        whole = y_ref[...] + leads * nt(c_in[...], entering)
        g = gate_in[...].astype(F32)
        y_ref[...] = whole
        gated[...] = (whole * (g * jax.nn.sigmoid(g))).astype(BF16)

    def source(g, j):
        return 4 * ((z + 4 - g) % 4) + (x + 4 - j) % 4

    def arrived(src):
        return remote(sendbuf.at[src], rows.at[quarter, src], a_send.at[src], a_recv.at[src], up)

    def rows_up(src, q):
        return remote(
            rows.at[q, src, 0], rows.at[q, src, 0], yr_send.at[src], yr_recv.at[src], up
        )

    def scaled_down(src, q):
        return remote(
            rows.at[q, src, 1], rows.at[q, src, 1], ys_send.at[src], ys_recv.at[src], down
        )

    def across(src, q):
        return remote(rows.at[q, src], rows.at[q, src], pa_send.at[src], pa_recv.at[src], partner)

    def across_beside(src, q):
        return remote(rows.at[q, src], rows.at[q, src], pn_send.at[src], pn_recv.at[src], partner)

    def forward_own(g):
        for j in range(4):
            src = source(g, j)
            if j > 0:
                arrived(src).wait_recv()
            else:

                @pl.when(g > 0)
                def _():
                    arrived(src).wait_recv()

            rows_up(src, quarter).start()
            scaled_down(src, quarter).start()
            across(src, quarter).start()

    def forward_beside(g):
        for j in range(4):
            src = source(g, j)
            rows_up(src, beside).wait_recv()
            scaled_down(src, beside).wait_recv()
            across_beside(src, beside).start()

    def halves_across(g):
        return remote(
            part.at[g, 1 - core], part_in.at[g], d_send.at[g], d_recv.at[g], partner
        )

    def compute(g):
        block = (z + 4 - g) % 4
        for j in range(4):
            src = source(g, j)
            across(src, partner_q).wait_recv()
            across_beside(src, partner_beside).wait_recv()
        here = pl.ds(4 * block, 4)
        n = 4 * cap
        gate_pre = up_pre = d_hidden = jnp.zeros((n, wg.shape[1]), F32)
        for q in range(4):
            r = rows[q, here, 0].reshape(n, share)
            sc = rows[q, here, 1].reshape(n, share)
            f = slice(q * share, (q + 1) * share)
            gate_pre = gate_pre + nn(r, wg[f, :])
            up_pre = up_pre + nn(r, wu[f, :])
            d_hidden = d_hidden + nt(sc, wd[:, f])
        sigma = jax.nn.sigmoid(gate_pre)
        silu = gate_pre * sigma
        dg = (d_hidden * up_pre * sigma * (1.0 + gate_pre * (1.0 - sigma))).astype(BF16)
        du = (d_hidden * silu).astype(BF16)
        act[block] = (silu * up_pre).astype(BF16)
        dgate[block] = dg
        dup[block] = du
        for k in range(8):
            f = slice(k * own, (k + 1) * own)
            part[g, k % 2, k // 2] = (nt(dg, wg[f, :]) + nt(du, wu[f, :])).astype(BF16)
        halves_across(g).start()

    def both(g, f):
        return part[g, core, f].astype(F32) + part_in[g, f].astype(F32)

    half = 2 * cap

    def first_step(g, way):
        return remote(
            q1.at[g, way], y1.at[g, way], s1_send.at[g, way], s1_recv.at[g, way], (up, down)[way]
        )

    def second_step(g, way):
        return remote(
            q2.at[g, way], y2.at[g, way], s2_send.at[g, way], s2_recv.at[g, way], (up, down)[way]
        )

    def sum_far(g):
        halves_across(g).wait_recv()
        far = both(g, (y + 2) % 4)
        q1[g, 0] = far[:half].astype(BF16)
        q1[g, 1] = far[half:].astype(BF16)
        first_step(g, 0).start()
        first_step(g, 1).start()

    def sum_near(g):
        first_step(g, 0).wait_recv()
        above = both(g, (y + 1) % 4)
        q2[g, 0, :half] = (above[:half] + y1[g, 0].astype(F32)).astype(BF16)
        q2[g, 0, half:] = above[half:].astype(BF16)
        second_step(g, 0).start()
        first_step(g, 1).wait_recv()
        below = both(g, (y + 3) % 4)
        q2[g, 1, :half] = below[:half].astype(BF16)
        q2[g, 1, half:] = (below[half:] + y1[g, 1].astype(F32)).astype(BF16)
        second_step(g, 1).start()

    def to_owner(g, src):
        return remote(
            fin.at[src], ret.at[s], c_send.at[src], c_recv.at[s], (src // 4, src % 4, t)
        )

    def from_expert(e):
        return remote(fin.at[e], ret.at[e], c_send.at[e], c_recv.at[e], up)

    def sum_own(g):
        second_step(g, 0).wait_recv()
        second_step(g, 1).wait_recv()
        block = (z + 4 - g) % 4
        total = both(g, y) + y2[g, 0].astype(F32) + y2[g, 1].astype(F32)
        fin[pl.ds(4 * block, 4)] = total.astype(BF16).reshape(4, cap, own)
        for j in range(4):
            src = source(g, j)
            if j > 0:
                to_owner(g, src).start()
            else:

                @pl.when(g > 0)
                def _():
                    to_owner(g, src).start()

                @pl.when(g == 0)
                def _():
                    ret[s] = fin[s]

    def grad_rows(target, which):
        for q in range(4):
            r = rows[q, :, 0].reshape(experts * cap, share)
            target[q * share : (q + 1) * share, :] = tn(
                r, which[...].reshape(experts * cap, -1)
            ).astype(BF16)

    def grad_down():
        hidden = act[...].reshape(experts * cap, -1)
        for q in range(4):
            sc = rows[q, :, 1].reshape(experts * cap, share)
            gd[:, q * share : (q + 1) * share] = tn(hidden, sc).astype(BF16)

    stores = [
        pltpu.make_async_copy(gg, gg_hbm, local.at[6]),
        pltpu.make_async_copy(gu, gu_hbm, local.at[7]),
        pltpu.make_async_copy(gd, gd_hbm, local.at[8]),
    ]

    def turn(n, carry):
        for lag, task in enumerate(
            (forward_own, forward_beside, compute, sum_far, sum_near, sum_own)
        ):

            @pl.when((n >= lag) & (n < lag + 4))
            def _():
                task(n - lag)

        @pl.when(n == 2)
        def _():
            scan_forward()

        @pl.when(n == 4)
        def _():
            finish_forward()

        @pl.when(n == 5)
        def _():
            grad_rows(gg, dgate)
            stores[0].start()

        @pl.when(n == 6)
        def _():
            grad_rows(gu, dup)
            stores[1].start()

        @pl.when(n == 7)
        def _():
            grad_down()
            stores[2].start()

        return carry

    lax.fori_loop(0, 9, turn, 0)

    def take(k, carry):
        from_expert((s + k) % experts).wait_recv()
        return carry

    lax.fori_loop(1, experts, take, 0)
    places = experts * cap
    picked = tn(hot[...].reshape(places, tokens), ret[...].reshape(places, own))
    gm[t] = (cot_own[...].astype(F32) + picked).astype(BF16)

    low, high = pl.ds(0, tokens // 2), pl.ds(tokens // 2, tokens // 2)
    below, above, far = (t + 6) % 8, (t + 2) % 8, (t + 4) % 8
    mate = t + 1 - 2 * core
    m_below, m_above, m_far = (mate + 6) % 8, (mate + 2) % 8, (mate + 4) % 8

    def gather(k, src, device, part_rows=None):
        ref = gm.at[src] if part_rows is None else gm.at[src, part_rows]
        return remote(ref, ref, g_send.at[k], g_recv.at[k], device)

    def to_column(i):
        return remote(
            proj_send.at[i], proj_in.at[s], p_send.at[i], p_recv.at[s], (i // 4, i % 4, t)
        )

    columns = gated.shape[1]
    gated_b = gated[...]

    def project(j):
        for k in range(own // columns):
            i = j * (own // columns) + k
            block = gm[j, :, k * columns : (k + 1) * columns]
            proj_send[i] = tn(block, gated_b).astype(BF16)

            @pl.when(i != s)
            def _():
                to_column(i).start()

            @pl.when(i == s)
            def _():
                proj_in[s] = proj_send[s]

        return nn(gm[j], op[pl.ds(j * own, own), :])

    gather(1, t, up).start()
    gather(2, t, down).start()
    gather(0, t, partner).start()
    out_grad = project(t)
    gather(0, mate, partner).wait_recv()
    out_grad = out_grad + project(mate)
    gather(1, below, up).wait_recv()
    gather(3, below, up, low).start()
    gather(5, below, partner).start()
    gather(2, above, down).wait_recv()
    gather(4, above, down, high).start()
    gather(6, above, partner).start()
    out_grad = out_grad + project(below) + project(above)
    gather(5, m_below, partner).wait_recv()
    out_grad = out_grad + project(m_below)
    gather(6, m_above, partner).wait_recv()
    out_grad = out_grad + project(m_above)
    gather(3, far, up, low).wait_recv()
    gather(4, far, down, high).wait_recv()
    gather(7, far, partner).start()
    out_grad = out_grad + project(far)
    gather(7, m_far, partner).wait_recv()
    out_grad = out_grad + project(m_far)

    row, col = decays(ld[...])
    leads = by_lane(jnp.exp(col), tokens, heads)
    gate = gate_in[...].astype(F32)
    lead_grad = (out_grad * (gate * jax.nn.sigmoid(gate)) * leads).astype(BF16)
    back_send[...] = tn(lead_grad, c_in[...]).astype(BF16).reshape(experts, STEP, STATE)
    back_in[s] = back_send[s]
    backs[0]()
    backward = mix_backward(
        x_in[...], b_in[...], c_in[...], gate, out_grad, y_ref[...], lead_grad,
        enter[...].reshape(x_in.shape[1], STATE), row, col, heads
    )
    dgate_out[...] = backward[3].astype(BF16)
    dc_out[...] = backward[2].astype(BF16)
    scan_back()
    tails = by_lane(jnp.exp(col[tokens - 1 : tokens, :] - col), tokens, heads)
    tail_values = (x_in[...].astype(F32) * tails).astype(BF16)
    leaves[1]()
    leaving = leave[...].reshape(x_in.shape[1], STATE)
    dx_out[...] = (backward[0] + tails * nt(b_in[...], leaving)).astype(BF16)
    db_out[...] = (backward[1] + nn(tail_values, leaving)).astype(BF16)

    def column(k, total):
        i = (s + k) % experts
        remote(
            proj_send.at[i], proj_in.at[i], p_send.at[i], p_recv.at[i], up
        ).wait_recv()
        return total + proj_in[i].astype(F32)

    proj_out[...] = lax.fori_loop(1, experts, column, proj_in[s].astype(F32))
    for exchange in (states, enters, backs, leaves):
        exchange[2]()

    def sent(k, carry):
        e = (s + k) % experts
        to_expert(e).wait_send()
        to_owner(0, e).wait_send()
        to_column(e).wait_send()
        return carry

    lax.fori_loop(1, experts, sent, 0)

    def forwarded(k, carry):
        rows_up(k, quarter).wait_send()
        scaled_down(k, quarter).wait_send()
        across(k, quarter).wait_send()
        across_beside(k, beside).wait_send()
        return carry

    lax.fori_loop(0, experts, forwarded, 0)

    def summed(g, carry):
        halves_across(g).wait_send()
        for way in range(2):
            first_step(g, way).wait_send()
            second_step(g, way).wait_send()
        return carry

    lax.fori_loop(0, 4, summed, 0)
    gather(0, t, partner).wait_send()
    gather(1, t, up).wait_send()
    gather(2, t, down).wait_send()
    gather(3, below, up, low).wait_send()
    gather(4, above, down, high).wait_send()
    gather(5, below, partner).wait_send()
    gather(6, above, partner).wait_send()
    gather(7, far, partner).wait_send()
    for store in stores:
        store.wait()


def whole(ids, wts, ld, x, b, c, gate, mixed, cot, wg, wu, wd, op, experts, cap, heads):
    tokens, width = mixed.shape
    hidden = wg.shape[1]
    channels = x.shape[1]
    share, own = width // 4, width // 8
    vmem = pl.BlockSpec(memory_space=pltpu.VMEM)
    hbm = pl.BlockSpec(memory_space=pl.ANY)
    dma = pltpu.SemaphoreType.DMA

    def kernel(*refs):
        moe_kernel(heads, *refs)

    def buf(*shape, dtype=BF16):
        return pltpu.VMEM(shape, dtype)

    n = 4 * cap
    return pl.pallas_call(
        kernel,
        out_shape=[
            jax.ShapeDtypeStruct(x.shape, BF16),
            jax.ShapeDtypeStruct(b.shape, BF16),
            jax.ShapeDtypeStruct(c.shape, BF16),
            jax.ShapeDtypeStruct(gate.shape, BF16),
            jax.ShapeDtypeStruct((width // experts, channels), F32),
            jax.ShapeDtypeStruct(wg.shape, BF16),
            jax.ShapeDtypeStruct(wu.shape, BF16),
            jax.ShapeDtypeStruct(wd.shape, BF16),
        ],
        in_specs=[vmem] * 7 + [hbm] * 6,
        out_specs=[vmem] * 5 + [hbm] * 3,
        scratch_shapes=[
            buf(8, tokens, own),
            buf(*op.shape),
            buf(tokens, channels, dtype=F32),
            buf(tokens, channels),
            buf(experts, STEP + 8, STATE, dtype=F32),
            buf(experts, STEP + 8, STATE, dtype=F32),
            buf(experts, STEP, STATE),
            buf(experts, STEP, STATE),
            buf(experts, STEP, STATE),
            buf(experts, STEP, STATE),
            buf(experts, STEP, STATE),
            buf(experts, STEP, STATE),
            buf(experts, width // experts, channels),
            buf(experts, width // experts, channels),
            buf(tokens, share),
            buf(tokens, share),
            buf(tokens, own),
            buf(*wg.shape),
            buf(*wu.shape),
            buf(*wd.shape),
            buf(experts, tokens, dtype=jnp.int32),
            buf(experts, tokens, dtype=F32),
            buf(experts, cap, tokens),
            buf(experts, 2, cap, share),
            buf(4, experts, 2, cap, share),
            buf(4, n, hidden),
            buf(4, n, hidden),
            buf(4, n, hidden),
            buf(4, 2, 4, n, own),
            buf(4, 4, n, own),
            buf(4, 2, n // 2, own),
            buf(4, 2, n // 2, own),
            buf(4, 2, n, own),
            buf(4, 2, n, own),
            buf(experts, cap, own),
            buf(experts, cap, own),
            buf(*wg.shape),
            buf(*wu.shape),
            buf(*wd.shape),
            dma((10,)),
        ]
        + [dma((experts,))] * 10
        + [dma((4,))] * 2
        + [dma((4, 2))] * 4
        + [dma((experts,))] * 2
        + [dma((8,))] * 2
        + [dma((experts,))] * 10,
        compiler_params=pltpu.CompilerParams(
            collective_id=0, has_side_effects=True, vmem_limit_bytes=60 * 2**20
        ),
        name="whole",
    )(ids, wts, ld, x, b, c, gate, mixed, cot, wg, wu, wd, op)


def body(
    token_values,
    write_keys,
    read_keys,
    log_decay,
    out_gate,
    out_proj,
    mixed,
    cotangent,
    route_ids,
    route_weights,
    w_gate,
    w_up,
    w_down,
):
    experts = lax.axis_size(SP)
    outs = whole(
        route_ids.T,
        route_weights.T,
        log_decay,
        token_values,
        write_keys,
        read_keys,
        out_gate,
        mixed,
        cotangent,
        w_gate[0],
        w_up[0],
        w_down[0],
        out_proj,
        experts,
        3 * mixed.shape[0] // experts,
        log_decay.shape[0],
    )
    return (*outs[:5], *(g[None] for g in outs[5:]))


def solution(mesh):
    finer = Mesh(mesh.devices.reshape(4, 4, mesh.shape["tp"]), ("sp_0", "sp_1", "tp"))
    return jax.shard_map(
        body,
        mesh=finer,
        in_specs=(
            P(SP, "tp"),
            P(SP, "tp"),
            P(SP, "tp"),
            P("tp", SP),
            P(SP, "tp"),
            P(None, "tp"),
            P(SP, None),
            P(SP, None),
            P(SP, None),
            P(SP, None),
            P(SP, None, "tp"),
            P(SP, None, "tp"),
            P(SP, "tp", None),
        ),
        out_specs=(
            P(SP, "tp"),
            P(SP, "tp"),
            P(SP, "tp"),
            P(SP, "tp"),
            P(SP, "tp"),
            P(SP, None, "tp"),
            P(SP, None, "tp"),
            P(SP, "tp", None),
        ),
        check_vma=False,
    )
```

```python
import jax
import jax.numpy as jnp
from jax import lax
from jax.experimental import pallas as pl
from jax.experimental.pallas import tpu as pltpu
from jax.sharding import Mesh
from jax.sharding import PartitionSpec as P

HEAD_DIM = 64
STATE = 128
SP = ("sp_0", "sp_1")
F32 = jnp.float32
BF16 = jnp.bfloat16
highest = lax.Precision.HIGHEST


def nn(a, b):
    return lax.dot_general(a, b, (((1,), (0,)), ((), ())), preferred_element_type=F32)


def nt(a, b):
    return lax.dot_general(a, b, (((1,), (1,)), ((), ())), preferred_element_type=F32)


def tn(a, b):
    return lax.dot_general(a, b, (((0,), (0,)), ((), ())), preferred_element_type=F32)


def iota(shape, dim):
    return lax.broadcasted_iota(jnp.int32, shape, dim)


def slots(ids_t, experts):
    tokens = ids_t.shape[1]
    e = iota((experts, tokens), 0)
    member = (ids_t[0:1, :] == e) | (ids_t[1:2, :] == e)
    before = (iota((tokens, tokens), 0) < iota((tokens, tokens), 1)).astype(BF16)
    slot = nn(member.astype(BF16), before)
    return jnp.where(member, slot.astype(jnp.int32), -1)


def weight_rows(ids_t, w_t, experts):
    e = iota((experts, ids_t.shape[1]), 0)
    return jnp.where(ids_t[0:1, :] == e, w_t[0:1, :], 0.0) + jnp.where(
        ids_t[1:2, :] == e, w_t[1:2, :], 0.0
    )


def decays(ld):
    heads, tokens = ld.shape
    ld8 = jnp.concatenate([ld, jnp.zeros((8 - heads, tokens), F32)], axis=0)
    upto = (iota((tokens, tokens), 0) <= iota((tokens, tokens), 1)).astype(F32)
    row = lax.dot_general(
        ld8, upto, (((1,), (0,)), ((), ())), precision=highest, preferred_element_type=F32
    )
    col = lax.dot_general(
        upto, ld8, (((0,), (1,)), ((), ())), precision=highest, preferred_element_type=F32
    )
    return row, col


def by_lane(col, tokens, heads):
    lane = iota((tokens, 2 * HEAD_DIM), 1)
    return jnp.concatenate(
        [
            jnp.where(lane < HEAD_DIM, col[:, 2 * p : 2 * p + 1], col[:, 2 * p + 1 : 2 * p + 2])
            for p in range(heads // 2)
        ],
        axis=1,
    )


def span_weights(row, col, h, tokens):
    lower = iota((tokens, tokens), 0) >= iota((tokens, tokens), 1)
    return jnp.exp(jnp.where(lower, col[:, h : h + 1] - row[h : h + 1, :], -1e30))


def mix_local(x, b, c, row, col, heads):
    tokens = x.shape[0]
    scores = nt(c, b)
    first = iota((tokens, 2 * HEAD_DIM), 1) < HEAD_DIM
    ys = []
    for p in range(heads // 2):
        xp = x[:, 128 * p : 128 * p + 128]
        pair = [
            nn((scores * span_weights(row, col, 2 * p + i, tokens)).astype(BF16), xp)
            for i in range(2)
        ]
        ys.append(jnp.where(first, pair[0], pair[1]))
    tails = by_lane(jnp.exp(col[tokens - 1 : tokens, :] - col), tokens, heads)
    end = tn((x.astype(F32) * tails).astype(BF16), b)
    return jnp.concatenate(ys, axis=1), end


def mix_backward(x, b, c, gate, out_grad, y, lead_grad, entering, row, col, heads):
    tokens = x.shape[0]
    sigma = jax.nn.sigmoid(gate)
    gb = (out_grad * (gate * sigma)).astype(BF16)
    d_gate = out_grad * y * sigma * (1.0 + gate * (1.0 - sigma))
    scores = nt(c, b)
    first = iota((tokens, 2 * HEAD_DIM), 1) < HEAD_DIM
    d_scores = jnp.zeros((tokens, tokens), F32)
    dxs = []
    for p in range(heads // 2):
        xp = x[:, 128 * p : 128 * p + 128]
        gp = gb[:, 128 * p : 128 * p + 128]
        pair = []
        for i in range(2):
            w = span_weights(row, col, 2 * p + i, tokens)
            mine = first if i == 0 else jnp.logical_not(first)
            d_scores = d_scores + w * nt(jnp.where(mine, gp, jnp.zeros_like(gp)), xp)
            pair.append(tn((scores * w).astype(BF16), gp))
        dxs.append(jnp.where(first, pair[0], pair[1]))
    ds = d_scores.astype(BF16)
    return jnp.concatenate(dxs, axis=1), tn(ds, c), nn(ds, b) + nn(lead_grad, entering), d_gate


MESH = pl.DeviceIdType.MESH
STEP = 16


def remote(src, dst, send, recv, device):
    return pltpu.make_async_remote_copy(
        src_ref=src, dst_ref=dst, send_sem=send, recv_sem=recv, device_id=device, device_id_type=MESH
    )


def moe_kernel(
    heads,
    ids,
    wts,
    ld,
    x_in,
    b_in,
    c_in,
    gate_in,
    mixed,
    cot,
    wg_hbm,
    wu_hbm,
    wd_hbm,
    op_hbm,
    dx_out,
    db_out,
    dc_out,
    dgate_out,
    proj_out,
    gg_hbm,
    gu_hbm,
    gd_hbm,
    gm,
    op,
    y_ref,
    gated,
    state_send,
    state_in,
    enter_send,
    enter,
    back_send,
    back_in,
    leave_send,
    leave,
    proj_send,
    proj_in,
    mixed_q,
    cot_q,
    cot_own,
    wg,
    wu,
    wd,
    slot_ref,
    weight_ref,
    hot,
    sendbuf,
    rows,
    act,
    dgate,
    dup,
    part,
    part_in,
    q1,
    y1,
    q2,
    y2,
    fin,
    ret,
    gg,
    gu,
    gd,
    local,
    a_send,
    a_recv,
    yr_send,
    yr_recv,
    ys_send,
    ys_recv,
    pa_send,
    pa_recv,
    pn_send,
    pn_recv,
    d_send,
    d_recv,
    s1_send,
    s1_recv,
    s2_send,
    s2_recv,
    c_send,
    c_recv,
    g_send,
    g_recv,
    e_send,
    e_recv,
    f_send,
    f_recv,
    b_send,
    b_recv,
    l_send,
    l_recv,
    p_send,
    p_recv,
):
    z, x, t = lax.axis_index("sp_0"), lax.axis_index("sp_1"), lax.axis_index("tp")
    s = 4 * z + x
    y, core = t // 2, t % 2
    quarter = t % 4
    beside = (quarter + 2) % 4
    partner_q = quarter + 1 - 2 * core
    partner_beside = (partner_q + 2) % 4
    up, down, partner = (z, x, (t + 2) % 8), (z, x, (t + 6) % 8), (z, x, t + 1 - 2 * core)
    tokens, width = mixed.shape
    experts, _, cap, share = sendbuf.shape
    own = width // 8

    loads = [
        pltpu.make_async_copy(mixed.at[:, pl.ds(quarter * share, share)], mixed_q, local.at[0]),
        pltpu.make_async_copy(cot.at[:, pl.ds(quarter * share, share)], cot_q, local.at[1]),
        pltpu.make_async_copy(cot.at[:, pl.ds(t * own, own)], cot_own, local.at[2]),
        pltpu.make_async_copy(wg_hbm, wg, local.at[3]),
        pltpu.make_async_copy(wu_hbm, wu, local.at[4]),
        pltpu.make_async_copy(wd_hbm, wd, local.at[5]),
        pltpu.make_async_copy(op_hbm, op, local.at[9]),
    ]
    for load in loads:
        load.start()

    barrier = pltpu.get_barrier_semaphore()

    def peer(k):
        to_z, to_x = (z + k % 4) % 4, (x + k % 4 + k // 4) % 4
        return 4 * to_z + to_x, (to_z, to_x, t)

    def greet(k, carry):
        pl.semaphore_signal(barrier, inc=1, device_id=peer(k)[1], device_id_type=MESH)
        return carry

    lax.fori_loop(1, experts, greet, 0)
    for device in (up, down, partner):
        pl.semaphore_signal(barrier, inc=1, device_id=device, device_id_type=MESH)

    slot_ref[...] = slots(ids[...], experts)
    weight_ref[...] = weight_rows(ids[...], wts[...], experts)
    loads[0].wait()
    loads[1].wait()
    pl.semaphore_wait(barrier, experts - 1 + 3)

    def to_expert(e):
        return remote(
            sendbuf.at[e], rows.at[quarter, s], a_send.at[e], a_recv.at[s], (e // 4, e % 4, t)
        )

    def build(g, carry):
        place = iota((cap, tokens), 0)
        ones, ws = [], []
        for j in range(4):
            e = peer(4 * g + j)[0]
            mine = place == slot_ref[pl.ds(e, 1), :]
            one = mine.astype(BF16)
            hot[e] = one
            ones.append(one)
            w = jnp.where(mine, weight_ref[pl.ds(e, 1), :], 0.0)
            ws.append(jnp.sum(w, axis=1, keepdims=True))
        one = jnp.concatenate(ones, axis=0)
        w = jnp.concatenate(ws, axis=0)
        plain = nn(one, mixed_q[...]).astype(BF16)
        scaled = (nn(one, cot_q[...]) * w).astype(BF16)
        for j in range(4):
            e = peer(4 * g + j)[0]
            sendbuf[e, 0] = plain[j * cap : (j + 1) * cap]
            sendbuf[e, 1] = scaled[j * cap : (j + 1) * cap]
        for j in range(4):
            e = peer(4 * g + j)[0]
            if j > 0:
                to_expert(e).start()
            else:

                @pl.when(g > 0)
                def _():
                    to_expert(e).start()

        return carry

    lax.fori_loop(0, 4, build, 0)
    rows[quarter, s] = sendbuf[s]

    row, col = decays(ld[...])
    inner, last = mix_local(x_in[...], b_in[...], c_in[...], row, col, heads)
    y_ref[...] = inner
    totals = jnp.broadcast_to(row[:, tokens - 1 : tokens], (8, STATE))
    state_send[:, :STEP, :] = last.reshape(experts, STEP, STATE)
    state_send[:, STEP:, :] = jnp.broadcast_to(totals[None], (experts, 8, STATE))
    state_in[s] = state_send[s]

    def over_sp(source_ref, target_ref, send, recv):
        def copy(k):
            j, device = peer(k)
            return remote(source_ref.at[j], target_ref.at[s], send.at[j], recv.at[s], device)

        def wait(k):
            j, device = peer(k)
            remote(source_ref.at[j], target_ref.at[j], send.at[j], recv.at[j], device).wait_recv()

        def each(action):
            def step(k, carry):
                action(k)
                return carry

            lax.fori_loop(1, experts, step, 0)

        return (
            lambda: each(lambda k: copy(k).start()),
            lambda: each(wait),
            lambda: each(lambda k: copy(k).wait_send()),
        )

    states = over_sp(state_send, state_in, e_send, e_recv)
    enters = over_sp(enter_send, enter, f_send, f_recv)
    backs = over_sp(back_send, back_in, b_send, b_recv)
    leaves = over_sp(leave_send, leave, l_send, l_recv)
    states[0]()
    for load in loads[2:]:
        load.wait()

    def factor(src):
        return jnp.exp(state_in[src, pl.ds(STEP + s // 4, 1), :])

    def scan_forward():
        states[1]()
        held = jnp.zeros((STEP, STATE), F32)
        for src in range(experts):
            enter_send[src] = held.astype(BF16)
            held = factor(src) * held + state_in[src, :STEP, :]
        enter[s] = enter_send[s]
        enters[0]()

    def scan_back():
        backs[1]()
        held = jnp.zeros((STEP, STATE), F32)
        for src in reversed(range(experts)):
            leave_send[src] = held.astype(BF16)
            held = factor(src) * held + back_in[src].astype(F32)
        leave[s] = leave_send[s]
        leaves[0]()

    def finish_forward():
        enters[1]()
        _, col = decays(ld[...])
        leads = by_lane(jnp.exp(col), tokens, heads)
        entering = enter[...].reshape(x_in.shape[1], STATE)
        whole = y_ref[...] + leads * nt(c_in[...], entering)
        g = gate_in[...].astype(F32)
        y_ref[...] = whole
        gated[...] = (whole * (g * jax.nn.sigmoid(g))).astype(BF16)

    def source(g, j):
        return 4 * ((z + 4 - j) % 4) + (x + 8 - j - g) % 4

    def arrived(src):
        return remote(sendbuf.at[src], rows.at[quarter, src], a_send.at[src], a_recv.at[src], up)

    def rows_up(src, q):
        return remote(
            rows.at[q, src, 0], rows.at[q, src, 0], yr_send.at[src], yr_recv.at[src], up
        )

    def scaled_down(src, q):
        return remote(
            rows.at[q, src, 1], rows.at[q, src, 1], ys_send.at[src], ys_recv.at[src], down
        )

    def across(src, q):
        return remote(rows.at[q, src], rows.at[q, src], pa_send.at[src], pa_recv.at[src], partner)

    def across_beside(src, q):
        return remote(rows.at[q, src], rows.at[q, src], pn_send.at[src], pn_recv.at[src], partner)

    def forward_own(g):
        for j in range(4):
            src = source(g, j)
            if j > 0:
                arrived(src).wait_recv()
            else:

                @pl.when(g > 0)
                def _():
                    arrived(src).wait_recv()

            rows_up(src, quarter).start()
            scaled_down(src, quarter).start()
            across(src, quarter).start()

    def forward_beside(g):
        for j in range(4):
            src = source(g, j)
            rows_up(src, beside).wait_recv()
            scaled_down(src, beside).wait_recv()
            across_beside(src, beside).start()

    def halves_across(g):
        return remote(
            part.at[g, 1 - core], part_in.at[g], d_send.at[g], d_recv.at[g], partner
        )

    def compute(g):
        sources = [source(g, j) for j in range(4)]
        for src in sources:
            across(src, partner_q).wait_recv()
            across_beside(src, partner_beside).wait_recv()
        n = 4 * cap
        gate_pre = up_pre = d_hidden = jnp.zeros((n, wg.shape[1]), F32)
        for q in range(4):
            r = jnp.concatenate([rows[q, src, 0] for src in sources], axis=0)
            sc = jnp.concatenate([rows[q, src, 1] for src in sources], axis=0)
            f = slice(q * share, (q + 1) * share)
            gate_pre = gate_pre + nn(r, wg[f, :])
            up_pre = up_pre + nn(r, wu[f, :])
            d_hidden = d_hidden + nt(sc, wd[:, f])
        sigma = jax.nn.sigmoid(gate_pre)
        silu = gate_pre * sigma
        dg = (d_hidden * up_pre * sigma * (1.0 + gate_pre * (1.0 - sigma))).astype(BF16)
        du = (d_hidden * silu).astype(BF16)
        hidden = (silu * up_pre).astype(BF16)
        for j, src in enumerate(sources):
            part_rows = slice(j * cap, (j + 1) * cap)
            act[src] = hidden[part_rows]
            dgate[src] = dg[part_rows]
            dup[src] = du[part_rows]
        for k in range(8):
            f = slice(k * own, (k + 1) * own)
            part[g, k % 2, k // 2] = (nt(dg, wg[f, :]) + nt(du, wu[f, :])).astype(BF16)
        halves_across(g).start()

    def both(g, f):
        return part[g, core, f].astype(F32) + part_in[g, f].astype(F32)

    half = 2 * cap

    def first_step(g, way):
        return remote(
            q1.at[g, way], y1.at[g, way], s1_send.at[g, way], s1_recv.at[g, way], (up, down)[way]
        )

    def second_step(g, way):
        return remote(
            q2.at[g, way], y2.at[g, way], s2_send.at[g, way], s2_recv.at[g, way], (up, down)[way]
        )

    def sum_far(g):
        halves_across(g).wait_recv()
        far = both(g, (y + 2) % 4)
        q1[g, 0] = far[:half].astype(BF16)
        q1[g, 1] = far[half:].astype(BF16)
        first_step(g, 0).start()
        first_step(g, 1).start()

    def sum_near(g):
        first_step(g, 0).wait_recv()
        above = both(g, (y + 1) % 4)
        q2[g, 0, :half] = (above[:half] + y1[g, 0].astype(F32)).astype(BF16)
        q2[g, 0, half:] = above[half:].astype(BF16)
        second_step(g, 0).start()
        first_step(g, 1).wait_recv()
        below = both(g, (y + 3) % 4)
        q2[g, 1, :half] = below[:half].astype(BF16)
        q2[g, 1, half:] = (below[half:] + y1[g, 1].astype(F32)).astype(BF16)
        second_step(g, 1).start()

    def to_owner(g, src):
        return remote(
            fin.at[src], ret.at[s], c_send.at[src], c_recv.at[s], (src // 4, src % 4, t)
        )

    def from_expert(e):
        return remote(fin.at[e], ret.at[e], c_send.at[e], c_recv.at[e], up)

    def sum_own(g):
        second_step(g, 0).wait_recv()
        second_step(g, 1).wait_recv()
        total = (both(g, y) + y2[g, 0].astype(F32) + y2[g, 1].astype(F32)).astype(BF16)
        for j in range(4):
            fin[source(g, j)] = total[j * cap : (j + 1) * cap]
        for j in range(4):
            src = source(g, j)
            if j > 0:
                to_owner(g, src).start()
            else:

                @pl.when(g > 0)
                def _():
                    to_owner(g, src).start()

                @pl.when(g == 0)
                def _():
                    ret[s] = fin[s]

    def grad_rows(target, which):
        for q in range(4):
            r = rows[q, :, 0].reshape(experts * cap, share)
            target[q * share : (q + 1) * share, :] = tn(
                r, which[...].reshape(experts * cap, -1)
            ).astype(BF16)

    def grad_down():
        hidden = act[...].reshape(experts * cap, -1)
        for q in range(4):
            sc = rows[q, :, 1].reshape(experts * cap, share)
            gd[:, q * share : (q + 1) * share] = tn(hidden, sc).astype(BF16)

    stores = [
        pltpu.make_async_copy(gg, gg_hbm, local.at[6]),
        pltpu.make_async_copy(gu, gu_hbm, local.at[7]),
        pltpu.make_async_copy(gd, gd_hbm, local.at[8]),
    ]

    def turn(n, carry):
        for lag, task in enumerate(
            (forward_own, forward_beside, compute, sum_far, sum_near, sum_own)
        ):

            @pl.when((n >= lag) & (n < lag + 4))
            def _():
                task(n - lag)

        @pl.when(n == 4)
        def _():
            scan_forward()

        @pl.when(n == 7)
        def _():
            finish_forward()

        @pl.when(n == 5)
        def _():
            grad_rows(gg, dgate)
            stores[0].start()

        @pl.when(n == 6)
        def _():
            grad_rows(gu, dup)
            stores[1].start()

        @pl.when(n == 7)
        def _():
            grad_down()
            stores[2].start()

        return carry

    lax.fori_loop(0, 9, turn, 0)

    def take(k, carry):
        from_expert(peer(k)[0]).wait_recv()
        return carry

    lax.fori_loop(1, experts, take, 0)
    places = experts * cap
    picked = tn(hot[...].reshape(places, tokens), ret[...].reshape(places, own))
    gm[t] = (cot_own[...].astype(F32) + picked).astype(BF16)

    low, high = pl.ds(0, tokens // 2), pl.ds(tokens // 2, tokens // 2)
    below, above, far = (t + 6) % 8, (t + 2) % 8, (t + 4) % 8
    mate = t + 1 - 2 * core
    m_below, m_above, m_far = (mate + 6) % 8, (mate + 2) % 8, (mate + 4) % 8

    def gather(k, src, device, part_rows=None):
        ref = gm.at[src] if part_rows is None else gm.at[src, part_rows]
        return remote(ref, ref, g_send.at[k], g_recv.at[k], device)

    def to_column(i):
        return remote(
            proj_send.at[i], proj_in.at[s], p_send.at[i], p_recv.at[s], (i // 4, i % 4, t)
        )

    columns = gated.shape[1]
    gated_b = gated[...]

    def project(j, send=False):
        for k in range(own // columns):
            i = j * (own // columns) + k
            block = gm[j, :, k * columns : (k + 1) * columns]
            proj_send[i] = tn(block, gated_b).astype(BF16)

            if send:

                @pl.when(i != s)
                def _():
                    to_column(i).start()

            @pl.when(i == s)
            def _():
                proj_in[s] = proj_send[s]

        return nn(gm[j], op[pl.ds(j * own, own), :])

    gather(1, t, up).start()
    gather(2, t, down).start()
    gather(0, t, partner).start()
    out_grad = project(t, True)
    gather(0, mate, partner).wait_recv()
    out_grad = out_grad + project(mate, True)
    gather(1, below, up).wait_recv()
    gather(3, below, up, low).start()
    gather(5, below, partner).start()
    gather(2, above, down).wait_recv()
    gather(4, above, down, high).start()
    gather(6, above, partner).start()
    out_grad = out_grad + project(below) + project(above)
    gather(5, m_below, partner).wait_recv()
    out_grad = out_grad + project(m_below)
    gather(6, m_above, partner).wait_recv()
    out_grad = out_grad + project(m_above)
    gather(3, far, up, low).wait_recv()
    gather(4, far, down, high).wait_recv()
    gather(7, far, partner).start()
    out_grad = out_grad + project(far)
    gather(7, m_far, partner).wait_recv()
    out_grad = out_grad + project(m_far)

    def send_column(k, carry):
        i, device = peer(k)

        @pl.when(device[0] != y)
        def _():
            to_column(i).start()

        return carry

    lax.fori_loop(1, experts, send_column, 0)
    row, col = decays(ld[...])
    leads = by_lane(jnp.exp(col), tokens, heads)
    gate = gate_in[...].astype(F32)
    lead_grad = (out_grad * (gate * jax.nn.sigmoid(gate)) * leads).astype(BF16)
    back_send[...] = tn(lead_grad, c_in[...]).astype(BF16).reshape(experts, STEP, STATE)
    back_in[s] = back_send[s]
    backs[0]()
    backward = mix_backward(
        x_in[...], b_in[...], c_in[...], gate, out_grad, y_ref[...], lead_grad,
        enter[...].reshape(x_in.shape[1], STATE), row, col, heads
    )
    dgate_out[...] = backward[3].astype(BF16)
    dc_out[...] = backward[2].astype(BF16)
    scan_back()
    tails = by_lane(jnp.exp(col[tokens - 1 : tokens, :] - col), tokens, heads)
    tail_values = (x_in[...].astype(F32) * tails).astype(BF16)
    leaves[1]()
    leaving = leave[...].reshape(x_in.shape[1], STATE)
    dx_out[...] = (backward[0] + tails * nt(b_in[...], leaving)).astype(BF16)
    db_out[...] = (backward[1] + nn(tail_values, leaving)).astype(BF16)

    def column(k, total):
        i = peer(k)[0]
        remote(
            proj_send.at[i], proj_in.at[i], p_send.at[i], p_recv.at[i], up
        ).wait_recv()
        return total + proj_in[i].astype(F32)

    proj_out[...] = lax.fori_loop(1, experts, column, proj_in[s].astype(F32))
    for exchange in (states, enters, backs, leaves):
        exchange[2]()

    def sent(k, carry):
        e = peer(k)[0]
        to_expert(e).wait_send()
        to_owner(0, e).wait_send()
        to_column(e).wait_send()
        return carry

    lax.fori_loop(1, experts, sent, 0)

    def forwarded(k, carry):
        rows_up(k, quarter).wait_send()
        scaled_down(k, quarter).wait_send()
        across(k, quarter).wait_send()
        across_beside(k, beside).wait_send()
        return carry

    lax.fori_loop(0, experts, forwarded, 0)

    def summed(g, carry):
        halves_across(g).wait_send()
        for way in range(2):
            first_step(g, way).wait_send()
            second_step(g, way).wait_send()
        return carry

    lax.fori_loop(0, 4, summed, 0)
    gather(0, t, partner).wait_send()
    gather(1, t, up).wait_send()
    gather(2, t, down).wait_send()
    gather(3, below, up, low).wait_send()
    gather(4, above, down, high).wait_send()
    gather(5, below, partner).wait_send()
    gather(6, above, partner).wait_send()
    gather(7, far, partner).wait_send()
    for store in stores:
        store.wait()


def whole(ids, wts, ld, x, b, c, gate, mixed, cot, wg, wu, wd, op, experts, cap, heads):
    tokens, width = mixed.shape
    hidden = wg.shape[1]
    channels = x.shape[1]
    share, own = width // 4, width // 8
    vmem = pl.BlockSpec(memory_space=pltpu.VMEM)
    hbm = pl.BlockSpec(memory_space=pl.ANY)
    dma = pltpu.SemaphoreType.DMA

    def kernel(*refs):
        moe_kernel(heads, *refs)

    def buf(*shape, dtype=BF16):
        return pltpu.VMEM(shape, dtype)

    n = 4 * cap
    return pl.pallas_call(
        kernel,
        out_shape=[
            jax.ShapeDtypeStruct(x.shape, BF16),
            jax.ShapeDtypeStruct(b.shape, BF16),
            jax.ShapeDtypeStruct(c.shape, BF16),
            jax.ShapeDtypeStruct(gate.shape, BF16),
            jax.ShapeDtypeStruct((width // experts, channels), F32),
            jax.ShapeDtypeStruct(wg.shape, BF16),
            jax.ShapeDtypeStruct(wu.shape, BF16),
            jax.ShapeDtypeStruct(wd.shape, BF16),
        ],
        in_specs=[vmem] * 7 + [hbm] * 6,
        out_specs=[vmem] * 5 + [hbm] * 3,
        scratch_shapes=[
            buf(8, tokens, own),
            buf(*op.shape),
            buf(tokens, channels, dtype=F32),
            buf(tokens, channels),
            buf(experts, STEP + 8, STATE, dtype=F32),
            buf(experts, STEP + 8, STATE, dtype=F32),
            buf(experts, STEP, STATE),
            buf(experts, STEP, STATE),
            buf(experts, STEP, STATE),
            buf(experts, STEP, STATE),
            buf(experts, STEP, STATE),
            buf(experts, STEP, STATE),
            buf(experts, width // experts, channels),
            buf(experts, width // experts, channels),
            buf(tokens, share),
            buf(tokens, share),
            buf(tokens, own),
            buf(*wg.shape),
            buf(*wu.shape),
            buf(*wd.shape),
            buf(experts, tokens, dtype=jnp.int32),
            buf(experts, tokens, dtype=F32),
            buf(experts, cap, tokens),
            buf(experts, 2, cap, share),
            buf(4, experts, 2, cap, share),
            buf(experts, cap, hidden),
            buf(experts, cap, hidden),
            buf(experts, cap, hidden),
            buf(4, 2, 4, n, own),
            buf(4, 4, n, own),
            buf(4, 2, n // 2, own),
            buf(4, 2, n // 2, own),
            buf(4, 2, n, own),
            buf(4, 2, n, own),
            buf(experts, cap, own),
            buf(experts, cap, own),
            buf(*wg.shape),
            buf(*wu.shape),
            buf(*wd.shape),
            dma((10,)),
        ]
        + [dma((experts,))] * 10
        + [dma((4,))] * 2
        + [dma((4, 2))] * 4
        + [dma((experts,))] * 2
        + [dma((8,))] * 2
        + [dma((experts,))] * 10,
        compiler_params=pltpu.CompilerParams(
            collective_id=0, has_side_effects=True, vmem_limit_bytes=60 * 2**20
        ),
        name="whole",
    )(ids, wts, ld, x, b, c, gate, mixed, cot, wg, wu, wd, op)


def hand_out(arrays):
    pieces = []
    for k, a in enumerate(arrays):
        count = max(1, a.size * a.dtype.itemsize // 2**19)
        step = a.shape[0] // count
        pieces += [(k, pl.ds(m * step, step)) for m in range(count)]

    def kernel(*refs):
        n = len(arrays)
        ins, outs, held, (come, go) = refs[:n], refs[n : 2 * n], refs[2 * n : 3 * n], refs[3 * n :]
        fetch = [
            pltpu.make_async_copy(ins[k].at[at], held[k].at[at], come.at[m])
            for m, (k, at) in enumerate(pieces)
        ]
        store = [
            pltpu.make_async_copy(held[k].at[at], outs[k].at[at], go.at[m])
            for m, (k, at) in enumerate(pieces)
        ]
        for f in fetch:
            f.start()
        for f, g in zip(fetch, store):
            f.wait()
            g.start()
        for g in store:
            g.wait()

    hbm = pl.BlockSpec(memory_space=pl.ANY)
    return pl.pallas_call(
        kernel,
        out_shape=[jax.ShapeDtypeStruct(a.shape, a.dtype) for a in arrays],
        in_specs=[hbm] * len(arrays),
        out_specs=[hbm] * len(arrays),
        scratch_shapes=[pltpu.VMEM(a.shape, a.dtype) for a in arrays]
        + [pltpu.SemaphoreType.DMA((len(pieces),))] * 2,
        name="hand_out",
    )(*arrays)


def body(
    token_values,
    write_keys,
    read_keys,
    log_decay,
    out_gate,
    out_proj,
    mixed,
    cotangent,
    route_ids,
    route_weights,
    w_gate,
    w_up,
    w_down,
):
    experts = lax.axis_size(SP)
    outs = hand_out(whole(
        route_ids.T,
        route_weights.T,
        log_decay,
        token_values,
        write_keys,
        read_keys,
        out_gate,
        mixed,
        cotangent,
        w_gate[0],
        w_up[0],
        w_down[0],
        out_proj,
        experts,
        3 * mixed.shape[0] // experts,
        log_decay.shape[0],
    ))
    return (*outs[:5], *(g[None] for g in outs[5:]))


def solution(mesh):
    finer = Mesh(mesh.devices.reshape(4, 4, mesh.shape["tp"]), ("sp_0", "sp_1", "tp"))
    return jax.shard_map(
        body,
        mesh=finer,
        in_specs=(
            P(SP, "tp"),
            P(SP, "tp"),
            P(SP, "tp"),
            P("tp", SP),
            P(SP, "tp"),
            P(None, "tp"),
            P(SP, None),
            P(SP, None),
            P(SP, None),
            P(SP, None),
            P(SP, None, "tp"),
            P(SP, None, "tp"),
            P(SP, "tp", None),
        ),
        out_specs=(
            P(SP, "tp"),
            P(SP, "tp"),
            P(SP, "tp"),
            P(SP, "tp"),
            P(SP, "tp"),
            P(SP, None, "tp"),
            P(SP, None, "tp"),
            P(SP, "tp", None),
        ),
        check_vma=False,
    )
```

```python
import jax
import jax.numpy as jnp
from jax import lax
from jax.experimental import pallas as pl
from jax.experimental.pallas import tpu as pltpu
from jax.sharding import Mesh
from jax.sharding import PartitionSpec as P

HEAD_DIM = 64
STATE = 128
SP = ("sp_0", "sp_1")
F32 = jnp.float32
BF16 = jnp.bfloat16
highest = lax.Precision.HIGHEST


def nn(a, b):
    return lax.dot_general(a, b, (((1,), (0,)), ((), ())), preferred_element_type=F32)


def nt(a, b):
    return lax.dot_general(a, b, (((1,), (1,)), ((), ())), preferred_element_type=F32)


def tn(a, b):
    return lax.dot_general(a, b, (((0,), (0,)), ((), ())), preferred_element_type=F32)


def iota(shape, dim):
    return lax.broadcasted_iota(jnp.int32, shape, dim)


def slots(ids_t, experts):
    tokens = ids_t.shape[1]
    e = iota((experts, tokens), 0)
    member = (ids_t[0:1, :] == e) | (ids_t[1:2, :] == e)
    before = (iota((tokens, tokens), 0) < iota((tokens, tokens), 1)).astype(BF16)
    slot = nn(member.astype(BF16), before)
    return jnp.where(member, slot.astype(jnp.int32), -1)


def weight_rows(ids_t, w_t, experts):
    e = iota((experts, ids_t.shape[1]), 0)
    return jnp.where(ids_t[0:1, :] == e, w_t[0:1, :], 0.0) + jnp.where(
        ids_t[1:2, :] == e, w_t[1:2, :], 0.0
    )


def decays(ld):
    heads, tokens = ld.shape
    ld8 = jnp.concatenate([ld, jnp.zeros((8 - heads, tokens), F32)], axis=0)
    upto = (iota((tokens, tokens), 0) <= iota((tokens, tokens), 1)).astype(F32)
    row = lax.dot_general(
        ld8, upto, (((1,), (0,)), ((), ())), precision=highest, preferred_element_type=F32
    )
    col = lax.dot_general(
        upto, ld8, (((0,), (1,)), ((), ())), precision=highest, preferred_element_type=F32
    )
    return row, col


def by_lane(col, tokens, heads):
    lane = iota((tokens, 2 * HEAD_DIM), 1)
    return jnp.concatenate(
        [
            jnp.where(lane < HEAD_DIM, col[:, 2 * p : 2 * p + 1], col[:, 2 * p + 1 : 2 * p + 2])
            for p in range(heads // 2)
        ],
        axis=1,
    )


def span_weights(row, col, h, tokens):
    lower = iota((tokens, tokens), 0) >= iota((tokens, tokens), 1)
    return jnp.exp(jnp.where(lower, col[:, h : h + 1] - row[h : h + 1, :], -1e30))


def mix_local(x, b, c, row, col, heads):
    tokens = x.shape[0]
    scores = nt(c, b)
    first = iota((tokens, 2 * HEAD_DIM), 1) < HEAD_DIM
    ys = []
    for p in range(heads // 2):
        xp = x[:, 128 * p : 128 * p + 128]
        pair = [
            nn((scores * span_weights(row, col, 2 * p + i, tokens)).astype(BF16), xp)
            for i in range(2)
        ]
        ys.append(jnp.where(first, pair[0], pair[1]))
    tails = by_lane(jnp.exp(col[tokens - 1 : tokens, :] - col), tokens, heads)
    end = tn((x.astype(F32) * tails).astype(BF16), b)
    return jnp.concatenate(ys, axis=1), end


def mix_backward(x, b, c, gate, out_grad, y, lead_grad, entering, row, col, heads):
    tokens = x.shape[0]
    sigma = jax.nn.sigmoid(gate)
    gb = (out_grad * (gate * sigma)).astype(BF16)
    d_gate = out_grad * y * sigma * (1.0 + gate * (1.0 - sigma))
    scores = nt(c, b)
    first = iota((tokens, 2 * HEAD_DIM), 1) < HEAD_DIM
    d_scores = jnp.zeros((tokens, tokens), F32)
    dxs = []
    for p in range(heads // 2):
        xp = x[:, 128 * p : 128 * p + 128]
        gp = gb[:, 128 * p : 128 * p + 128]
        pair = []
        for i in range(2):
            w = span_weights(row, col, 2 * p + i, tokens)
            mine = first if i == 0 else jnp.logical_not(first)
            d_scores = d_scores + w * nt(jnp.where(mine, gp, jnp.zeros_like(gp)), xp)
            pair.append(tn((scores * w).astype(BF16), gp))
        dxs.append(jnp.where(first, pair[0], pair[1]))
    ds = d_scores.astype(BF16)
    return jnp.concatenate(dxs, axis=1), tn(ds, c), nn(ds, b) + nn(lead_grad, entering), d_gate


MESH = pl.DeviceIdType.MESH
STEP = 16


def remote(src, dst, send, recv, device):
    return pltpu.make_async_remote_copy(
        src_ref=src, dst_ref=dst, send_sem=send, recv_sem=recv, device_id=device, device_id_type=MESH
    )


def moe_kernel(
    heads,
    ids,
    wts,
    ld,
    x_in,
    b_in,
    c_in,
    gate_in,
    mixed,
    cot,
    wg_hbm,
    wu_hbm,
    wd_hbm,
    op_hbm,
    dx_out,
    db_out,
    dc_out,
    dgate_out,
    proj_out,
    gg_hbm,
    gu_hbm,
    gd_hbm,
    gm,
    op,
    y_ref,
    gated,
    state_send,
    state_in,
    enter_send,
    enter,
    back_send,
    back_in,
    leave_send,
    leave,
    proj_send,
    row_in,
    column_send,
    column_in,
    mixed_q,
    cot_q,
    cot_own,
    wg,
    wu,
    wd,
    slot_ref,
    weight_ref,
    hot,
    sendbuf,
    rows,
    act,
    dgate,
    dup,
    part,
    part_in,
    q1,
    y1,
    q2,
    y2,
    fin,
    ret,
    gg,
    gu,
    gd,
    local,
    a_send,
    a_recv,
    yr_send,
    yr_recv,
    ys_send,
    ys_recv,
    pa_send,
    pa_recv,
    pn_send,
    pn_recv,
    d_send,
    d_recv,
    s1_send,
    s1_recv,
    s2_send,
    s2_recv,
    c_send,
    c_recv,
    g_send,
    g_recv,
    e_send,
    e_recv,
    f_send,
    f_recv,
    b_send,
    b_recv,
    l_send,
    l_recv,
    p_send,
    p_recv,
    q_send,
    q_recv,
):
    z, x, t = lax.axis_index("sp_0"), lax.axis_index("sp_1"), lax.axis_index("tp")
    s = 4 * z + x
    y, core = t // 2, t % 2
    quarter = t % 4
    beside = (quarter + 2) % 4
    partner_q = quarter + 1 - 2 * core
    partner_beside = (partner_q + 2) % 4
    up, down, partner = (z, x, (t + 2) % 8), (z, x, (t + 6) % 8), (z, x, t + 1 - 2 * core)
    tokens, width = mixed.shape
    experts, _, cap, share = sendbuf.shape
    own = width // 8

    loads = [
        pltpu.make_async_copy(mixed.at[:, pl.ds(quarter * share, share)], mixed_q, local.at[0]),
        pltpu.make_async_copy(cot.at[:, pl.ds(quarter * share, share)], cot_q, local.at[1]),
        pltpu.make_async_copy(cot.at[:, pl.ds(t * own, own)], cot_own, local.at[2]),
        pltpu.make_async_copy(wg_hbm, wg, local.at[3]),
        pltpu.make_async_copy(wu_hbm, wu, local.at[4]),
        pltpu.make_async_copy(wd_hbm, wd, local.at[5]),
        pltpu.make_async_copy(op_hbm, op, local.at[9]),
    ]
    for load in loads:
        load.start()

    barrier = pltpu.get_barrier_semaphore()

    def peer(k):
        to_z, to_x = (z + k % 4) % 4, (x + k % 4 + k // 4) % 4
        return 4 * to_z + to_x, (to_z, to_x, t)

    def greet(k, carry):
        pl.semaphore_signal(barrier, inc=1, device_id=peer(k)[1], device_id_type=MESH)
        return carry

    lax.fori_loop(1, experts, greet, 0)
    for device in (up, down, partner):
        pl.semaphore_signal(barrier, inc=1, device_id=device, device_id_type=MESH)

    slot_ref[...] = slots(ids[...], experts)
    weight_ref[...] = weight_rows(ids[...], wts[...], experts)
    loads[0].wait()
    loads[1].wait()
    pl.semaphore_wait(barrier, experts - 1 + 3)

    def to_expert(e):
        return remote(
            sendbuf.at[e], rows.at[quarter, s], a_send.at[e], a_recv.at[s], (e // 4, e % 4, t)
        )

    def build(g, carry):
        place = iota((cap, tokens), 0)
        ones, ws = [], []
        for j in range(4):
            e = peer(4 * g + j)[0]
            mine = place == slot_ref[pl.ds(e, 1), :]
            one = mine.astype(BF16)
            hot[e] = one
            ones.append(one)
            w = jnp.where(mine, weight_ref[pl.ds(e, 1), :], 0.0)
            ws.append(jnp.sum(w, axis=1, keepdims=True))
        one = jnp.concatenate(ones, axis=0)
        w = jnp.concatenate(ws, axis=0)
        plain = nn(one, mixed_q[...]).astype(BF16)
        scaled = (nn(one, cot_q[...]) * w).astype(BF16)
        for j in range(4):
            e = peer(4 * g + j)[0]
            sendbuf[e, 0] = plain[j * cap : (j + 1) * cap]
            sendbuf[e, 1] = scaled[j * cap : (j + 1) * cap]
        for j in range(4):
            e = peer(4 * g + j)[0]
            if j > 0:
                to_expert(e).start()
            else:

                @pl.when(g > 0)
                def _():
                    to_expert(e).start()

        return carry

    lax.fori_loop(0, 4, build, 0)
    rows[quarter, s] = sendbuf[s]

    row, col = decays(ld[...])
    inner, last = mix_local(x_in[...], b_in[...], c_in[...], row, col, heads)
    y_ref[...] = inner
    totals = jnp.broadcast_to(row[:, tokens - 1 : tokens], (8, STATE))
    state_send[:, :STEP, :] = last.reshape(experts, STEP, STATE)
    state_send[:, STEP:, :] = jnp.broadcast_to(totals[None], (experts, 8, STATE))
    state_in[s] = state_send[s]

    def over_sp(source_ref, target_ref, send, recv):
        def copy(k):
            j, device = peer(k)
            return remote(source_ref.at[j], target_ref.at[s], send.at[j], recv.at[s], device)

        def wait(k):
            j, device = peer(k)
            remote(source_ref.at[j], target_ref.at[j], send.at[j], recv.at[j], device).wait_recv()

        def each(action):
            def step(k, carry):
                action(k)
                return carry

            lax.fori_loop(1, experts, step, 0)

        return (
            lambda: each(lambda k: copy(k).start()),
            lambda: each(wait),
            lambda: each(lambda k: copy(k).wait_send()),
        )

    states = over_sp(state_send, state_in, e_send, e_recv)
    enters = over_sp(enter_send, enter, f_send, f_recv)
    backs = over_sp(back_send, back_in, b_send, b_recv)
    leaves = over_sp(leave_send, leave, l_send, l_recv)
    states[0]()
    for load in loads[2:]:
        load.wait()

    def factor(src):
        return jnp.exp(state_in[src, pl.ds(STEP + s // 4, 1), :])

    def scan_forward():
        states[1]()
        held = jnp.zeros((STEP, STATE), F32)
        for src in range(experts):
            enter_send[src] = held.astype(BF16)
            held = factor(src) * held + state_in[src, :STEP, :]
        enter[s] = enter_send[s]
        enters[0]()

    def scan_back():
        backs[1]()
        held = jnp.zeros((STEP, STATE), F32)
        for src in reversed(range(experts)):
            leave_send[src] = held.astype(BF16)
            held = factor(src) * held + back_in[src].astype(F32)
        leave[s] = leave_send[s]
        leaves[0]()

    def finish_forward():
        enters[1]()
        _, col = decays(ld[...])
        leads = by_lane(jnp.exp(col), tokens, heads)
        entering = enter[...].reshape(x_in.shape[1], STATE)
        whole = y_ref[...] + leads * nt(c_in[...], entering)
        g = gate_in[...].astype(F32)
        y_ref[...] = whole
        gated[...] = (whole * (g * jax.nn.sigmoid(g))).astype(BF16)

    def source(g, j):
        return 4 * ((z + 4 - j) % 4) + (x + 8 - j - g) % 4

    def arrived(src):
        return remote(sendbuf.at[src], rows.at[quarter, src], a_send.at[src], a_recv.at[src], up)

    def rows_up(src, q):
        return remote(
            rows.at[q, src, 0], rows.at[q, src, 0], yr_send.at[src], yr_recv.at[src], up
        )

    def scaled_down(src, q):
        return remote(
            rows.at[q, src, 1], rows.at[q, src, 1], ys_send.at[src], ys_recv.at[src], down
        )

    def across(src, q):
        return remote(rows.at[q, src], rows.at[q, src], pa_send.at[src], pa_recv.at[src], partner)

    def across_beside(src, q):
        return remote(rows.at[q, src], rows.at[q, src], pn_send.at[src], pn_recv.at[src], partner)

    def forward_own(g):
        for j in range(4):
            src = source(g, j)
            if j > 0:
                arrived(src).wait_recv()
            else:

                @pl.when(g > 0)
                def _():
                    arrived(src).wait_recv()

            rows_up(src, quarter).start()
            scaled_down(src, quarter).start()
            across(src, quarter).start()

    def forward_beside(g):
        for j in range(4):
            src = source(g, j)
            rows_up(src, beside).wait_recv()
            scaled_down(src, beside).wait_recv()
            across_beside(src, beside).start()

    def halves_across(g, f):
        return remote(
            part.at[g, 1 - core, f], part_in.at[g, f], d_send.at[g, f], d_recv.at[g, f], partner
        )

    def compute(g):
        sources = [source(g, j) for j in range(4)]
        for src in sources:
            across(src, partner_q).wait_recv()
            across_beside(src, partner_beside).wait_recv()
        n = 4 * cap
        gate_pre = up_pre = d_hidden = jnp.zeros((n, wg.shape[1]), F32)
        for q in range(4):
            r = jnp.concatenate([rows[q, src, 0] for src in sources], axis=0)
            sc = jnp.concatenate([rows[q, src, 1] for src in sources], axis=0)
            f = slice(q * share, (q + 1) * share)
            gate_pre = gate_pre + nn(r, wg[f, :])
            up_pre = up_pre + nn(r, wu[f, :])
            d_hidden = d_hidden + nt(sc, wd[:, f])
        sigma = jax.nn.sigmoid(gate_pre)
        silu = gate_pre * sigma
        dg = (d_hidden * up_pre * sigma * (1.0 + gate_pre * (1.0 - sigma))).astype(BF16)
        du = (d_hidden * silu).astype(BF16)
        hidden = (silu * up_pre).astype(BF16)
        for j, src in enumerate(sources):
            part_rows = slice(j * cap, (j + 1) * cap)
            act[src] = hidden[part_rows]
            dgate[src] = dg[part_rows]
            dup[src] = du[part_rows]
        for step in (2, 1, 3, 0):
            f = (y + step) % 4
            for k in range(2):
                cols = pl.ds(f * share + k * own, own)
                part[g, k, f] = (nt(dg, wg[cols, :]) + nt(du, wu[cols, :])).astype(BF16)
            halves_across(g, f).start()
        sum_far(g)

    def both(g, f):
        return part[g, core, f].astype(F32) + part_in[g, f].astype(F32)

    half = 2 * cap

    def first_step(g, way):
        return remote(
            q1.at[g, way], y1.at[g, way], s1_send.at[g, way], s1_recv.at[g, way], (up, down)[way]
        )

    def second_step(g, way):
        return remote(
            q2.at[g, way], y2.at[g, way], s2_send.at[g, way], s2_recv.at[g, way], (up, down)[way]
        )

    def sum_far(g):
        halves_across(g, (y + 2) % 4).wait_recv()
        far = both(g, (y + 2) % 4)
        q1[g, 0] = far[:half].astype(BF16)
        q1[g, 1] = far[half:].astype(BF16)
        first_step(g, 0).start()
        first_step(g, 1).start()

    def sum_near(g):
        first_step(g, 0).wait_recv()
        halves_across(g, (y + 1) % 4).wait_recv()
        above = both(g, (y + 1) % 4)
        q2[g, 0, :half] = (above[:half] + y1[g, 0].astype(F32)).astype(BF16)
        q2[g, 0, half:] = above[half:].astype(BF16)
        second_step(g, 0).start()
        first_step(g, 1).wait_recv()
        halves_across(g, (y + 3) % 4).wait_recv()
        below = both(g, (y + 3) % 4)
        q2[g, 1, :half] = below[:half].astype(BF16)
        q2[g, 1, half:] = (below[half:] + y1[g, 1].astype(F32)).astype(BF16)
        second_step(g, 1).start()

    def to_owner(g, src):
        return remote(
            fin.at[src], ret.at[s], c_send.at[src], c_recv.at[s], (src // 4, src % 4, t)
        )

    def from_expert(e):
        return remote(fin.at[e], ret.at[e], c_send.at[e], c_recv.at[e], up)

    def sum_own(g):
        second_step(g, 0).wait_recv()
        second_step(g, 1).wait_recv()
        halves_across(g, y).wait_recv()
        total = (both(g, y) + y2[g, 0].astype(F32) + y2[g, 1].astype(F32)).astype(BF16)
        for j in range(4):
            fin[source(g, j)] = total[j * cap : (j + 1) * cap]
        for j in range(4):
            src = source(g, j)
            if j > 0:
                to_owner(g, src).start()
            else:

                @pl.when(g > 0)
                def _():
                    to_owner(g, src).start()

                @pl.when(g == 0)
                def _():
                    ret[s] = fin[s]

    def grad_rows(target, which):
        for q in range(4):
            r = rows[q, :, 0].reshape(experts * cap, share)
            target[q * share : (q + 1) * share, :] = tn(
                r, which[...].reshape(experts * cap, -1)
            ).astype(BF16)

    def grad_down():
        hidden = act[...].reshape(experts * cap, -1)
        for q in range(4):
            sc = rows[q, :, 1].reshape(experts * cap, share)
            gd[:, q * share : (q + 1) * share] = tn(hidden, sc).astype(BF16)

    stores = [
        pltpu.make_async_copy(gg, gg_hbm, local.at[6]),
        pltpu.make_async_copy(gu, gu_hbm, local.at[7]),
        pltpu.make_async_copy(gd, gd_hbm, local.at[8]),
    ]

    def turn(n, carry):
        for lag, task in (
            (0, forward_own),
            (2, compute),
            (1, forward_beside),
            (3, sum_near),
            (4, sum_own),
        ):

            @pl.when((n >= lag) & (n < lag + 4))
            def _():
                task(n - lag)

        @pl.when(n == 4)
        def _():
            scan_forward()

        @pl.when(n == 6)
        def _():
            finish_forward()

        @pl.when(n == 5)
        def _():
            grad_rows(gg, dgate)
            stores[0].start()

        @pl.when(n == 6)
        def _():
            grad_rows(gu, dup)
            stores[1].start()

        @pl.when(n == 6)
        def _():
            grad_down()
            stores[2].start()

        return carry

    lax.fori_loop(0, 8, turn, 0)

    def take(k, carry):
        from_expert(peer(k)[0]).wait_recv()
        return carry

    lax.fori_loop(1, experts, take, 0)
    places = experts * cap
    picked = tn(hot[...].reshape(places, tokens), ret[...].reshape(places, own))
    gm[t] = (cot_own[...].astype(F32) + picked).astype(BF16)

    low, high = pl.ds(0, tokens // 2), pl.ds(tokens // 2, tokens // 2)
    below, above, far = (t + 6) % 8, (t + 2) % 8, (t + 4) % 8
    mate = t + 1 - 2 * core
    m_below, m_above, m_far = (mate + 6) % 8, (mate + 2) % 8, (mate + 4) % 8

    def gather(k, src, device, part_rows=None):
        ref = gm.at[src] if part_rows is None else gm.at[src, part_rows]
        return remote(ref, ref, g_send.at[k], g_recv.at[k], device)

    def to_row(i, to_x):
        return remote(
            proj_send.at[i], row_in.at[i // 4, x], p_send.at[i], p_recv.at[i // 4, x], (z, to_x, t)
        )

    columns = gated.shape[1]
    gated_b = gated[...]

    def send_rows(j):
        for k in range(2):
            to_x = 2 * (j % 2) + k

            @pl.when(to_x != x)
            def _():
                to_row(2 * j + k, to_x).start()

    def project(j):
        for k in range(2):
            block = gm[j, :, k * columns : (k + 1) * columns]
            proj_send[2 * j + k] = tn(block, gated_b).astype(BF16)
        return nn(gm[j], op[pl.ds(j * own, own), :])

    def to_column(f):
        return remote(
            column_send.at[f], column_in.at[z], q_send.at[f], q_recv.at[z], (f, x, t)
        )

    def sum_row(f):
        total = proj_send[4 * f + x].astype(F32)
        for k in range(1, 4):
            j = (x + k) % 4
            remote(
                proj_send.at[j], row_in.at[f, j], p_send.at[j], p_recv.at[f, j], up
            ).wait_recv()
            total = total + row_in[f, j].astype(F32)
        column_send[f] = total.astype(BF16)

        @pl.when(f != z)
        def _():
            to_column(f).start()

        @pl.when(f == z)
        def _():
            proj_out[...] = total

    moves = (
        (1, t, up, low),
        (2, t, up, high),
        (3, t, down, high),
        (4, t, down, low),
        (0, t, partner, None),
        (5, below, up, low),
        (6, above, down, high),
        (7, below, partner, None),
        (8, above, partner, None),
        (9, far, partner, None),
    )

    def start(k):
        gather(*[m for m in moves if m[0] == k][0]).start()

    for k in (1, 3, 2, 4, 0):
        start(k)
    out_grad = project(t)
    send_rows(t)
    gather(0, mate, partner).wait_recv()
    out_grad = out_grad + project(mate)
    send_rows(mate)
    gather(1, below, up, low).wait_recv()
    start(5)
    gather(3, above, down, high).wait_recv()
    start(6)
    gather(2, below, up, high).wait_recv()
    start(7)
    gather(4, above, down, low).wait_recv()
    start(8)
    out_grad = out_grad + project(above)
    send_rows(above)
    out_grad = out_grad + project(below)
    gather(8, m_above, partner).wait_recv()
    out_grad = out_grad + project(m_above)
    send_rows(m_above)
    gather(7, m_below, partner).wait_recv()
    out_grad = out_grad + project(m_below)
    gather(5, far, up, low).wait_recv()
    gather(6, far, down, high).wait_recv()
    start(9)
    out_grad = out_grad + project(far)
    gather(9, m_far, partner).wait_recv()
    out_grad = out_grad + project(m_far)

    row, col = decays(ld[...])
    leads = by_lane(jnp.exp(col), tokens, heads)
    gate = gate_in[...].astype(F32)
    lead_grad = (out_grad * (gate * jax.nn.sigmoid(gate)) * leads).astype(BF16)
    back_send[...] = tn(lead_grad, c_in[...]).astype(BF16).reshape(experts, STEP, STATE)
    back_in[s] = back_send[s]
    backs[0]()
    for j in (below, m_below, far, m_far):
        send_rows(j)
    backward = mix_backward(
        x_in[...], b_in[...], c_in[...], gate, out_grad, y_ref[...], lead_grad,
        enter[...].reshape(x_in.shape[1], STATE), row, col, heads
    )
    dgate_out[...] = backward[3].astype(BF16)
    dc_out[...] = backward[2].astype(BF16)
    scan_back()
    tails = by_lane(jnp.exp(col[tokens - 1 : tokens, :] - col), tokens, heads)
    tail_values = (x_in[...].astype(F32) * tails).astype(BF16)
    sum_row(y)
    sum_row((y + 1) % 4)
    leaves[1]()
    leaving = leave[...].reshape(x_in.shape[1], STATE)
    dx_out[...] = (backward[0] + tails * nt(b_in[...], leaving)).astype(BF16)
    db_out[...] = (backward[1] + nn(tail_values, leaving)).astype(BF16)
    sum_row((y + 3) % 4)
    sum_row((y + 2) % 4)
    for k in range(1, 4):
        j = (z + k) % 4
        remote(
            column_send.at[j], column_in.at[j], q_send.at[j], q_recv.at[j], up
        ).wait_recv()
        proj_out[...] += column_in[j].astype(F32)
        to_column(j).wait_send()
        for f in range(4):
            to_row(4 * f + (x + k) % 4, x).wait_send()
    for exchange in (states, enters, backs, leaves):
        exchange[2]()

    def sent(k, carry):
        e = peer(k)[0]
        to_expert(e).wait_send()
        to_owner(0, e).wait_send()
        return carry

    lax.fori_loop(1, experts, sent, 0)

    def forwarded(k, carry):
        rows_up(k, quarter).wait_send()
        scaled_down(k, quarter).wait_send()
        across(k, quarter).wait_send()
        across_beside(k, beside).wait_send()
        return carry

    lax.fori_loop(0, experts, forwarded, 0)

    def summed(g, carry):
        for f in range(4):
            halves_across(g, f).wait_send()
        for way in range(2):
            first_step(g, way).wait_send()
            second_step(g, way).wait_send()
        return carry

    lax.fori_loop(0, 4, summed, 0)
    for move in moves:
        gather(*move).wait_send()
    for store in stores:
        store.wait()


def whole(ids, wts, ld, x, b, c, gate, mixed, cot, wg, wu, wd, op, experts, cap, heads):
    tokens, width = mixed.shape
    hidden = wg.shape[1]
    channels = x.shape[1]
    share, own = width // 4, width // 8
    vmem = pl.BlockSpec(memory_space=pltpu.VMEM)
    hbm = pl.BlockSpec(memory_space=pl.ANY)
    dma = pltpu.SemaphoreType.DMA

    def kernel(*refs):
        moe_kernel(heads, *refs)

    def buf(*shape, dtype=BF16):
        return pltpu.VMEM(shape, dtype)

    n = 4 * cap
    return pl.pallas_call(
        kernel,
        out_shape=[
            jax.ShapeDtypeStruct(x.shape, BF16),
            jax.ShapeDtypeStruct(b.shape, BF16),
            jax.ShapeDtypeStruct(c.shape, BF16),
            jax.ShapeDtypeStruct(gate.shape, BF16),
            jax.ShapeDtypeStruct((width // experts, channels), F32),
            jax.ShapeDtypeStruct(wg.shape, BF16),
            jax.ShapeDtypeStruct(wu.shape, BF16),
            jax.ShapeDtypeStruct(wd.shape, BF16),
        ],
        in_specs=[vmem] * 7 + [hbm] * 6,
        out_specs=[vmem] * 5 + [hbm] * 3,
        scratch_shapes=[
            buf(8, tokens, own),
            buf(*op.shape),
            buf(tokens, channels, dtype=F32),
            buf(tokens, channels),
            buf(experts, STEP + 8, STATE, dtype=F32),
            buf(experts, STEP + 8, STATE, dtype=F32),
            buf(experts, STEP, STATE),
            buf(experts, STEP, STATE),
            buf(experts, STEP, STATE),
            buf(experts, STEP, STATE),
            buf(experts, STEP, STATE),
            buf(experts, STEP, STATE),
            buf(experts, width // experts, channels),
            buf(4, 4, width // experts, channels),
            buf(4, width // experts, channels),
            buf(4, width // experts, channels),
            buf(tokens, share),
            buf(tokens, share),
            buf(tokens, own),
            buf(*wg.shape),
            buf(*wu.shape),
            buf(*wd.shape),
            buf(experts, tokens, dtype=jnp.int32),
            buf(experts, tokens, dtype=F32),
            buf(experts, cap, tokens),
            buf(experts, 2, cap, share),
            buf(4, experts, 2, cap, share),
            buf(experts, cap, hidden),
            buf(experts, cap, hidden),
            buf(experts, cap, hidden),
            buf(4, 2, 4, n, own),
            buf(4, 4, n, own),
            buf(4, 2, n // 2, own),
            buf(4, 2, n // 2, own),
            buf(4, 2, n, own),
            buf(4, 2, n, own),
            buf(experts, cap, own),
            buf(experts, cap, own),
            buf(*wg.shape),
            buf(*wu.shape),
            buf(*wd.shape),
            dma((10,)),
        ]
        + [dma((experts,))] * 10
        + [dma((4, 4))] * 2
        + [dma((4, 2))] * 4
        + [dma((experts,))] * 2
        + [dma((10,))] * 2
        + [dma((experts,))] * 9
        + [dma((4, 4))]
        + [dma((4,))] * 2,
        compiler_params=pltpu.CompilerParams(
            collective_id=0, has_side_effects=True, vmem_limit_bytes=60 * 2**20
        ),
        name="whole",
    )(ids, wts, ld, x, b, c, gate, mixed, cot, wg, wu, wd, op)


def hand_out(arrays):
    pieces = []
    for k, a in enumerate(arrays):
        count = max(1, a.size * a.dtype.itemsize // 2**19)
        step = a.shape[0] // count
        pieces += [(k, pl.ds(m * step, step)) for m in range(count)]

    def kernel(*refs):
        n = len(arrays)
        ins, outs, held, (come, go) = refs[:n], refs[n : 2 * n], refs[2 * n : 3 * n], refs[3 * n :]
        fetch = [
            pltpu.make_async_copy(ins[k].at[at], held[k].at[at], come.at[m])
            for m, (k, at) in enumerate(pieces)
        ]
        store = [
            pltpu.make_async_copy(held[k].at[at], outs[k].at[at], go.at[m])
            for m, (k, at) in enumerate(pieces)
        ]
        for f in fetch:
            f.start()
        for f, g in zip(fetch, store):
            f.wait()
            g.start()
        for g in store:
            g.wait()

    hbm = pl.BlockSpec(memory_space=pl.ANY)
    return pl.pallas_call(
        kernel,
        out_shape=[jax.ShapeDtypeStruct(a.shape, a.dtype) for a in arrays],
        in_specs=[hbm] * len(arrays),
        out_specs=[hbm] * len(arrays),
        scratch_shapes=[pltpu.VMEM(a.shape, a.dtype) for a in arrays]
        + [pltpu.SemaphoreType.DMA((len(pieces),))] * 2,
        name="hand_out",
    )(*arrays)


def body(
    token_values,
    write_keys,
    read_keys,
    log_decay,
    out_gate,
    out_proj,
    mixed,
    cotangent,
    route_ids,
    route_weights,
    w_gate,
    w_up,
    w_down,
):
    experts = lax.axis_size(SP)
    outs = hand_out(whole(
        route_ids.T,
        route_weights.T,
        log_decay,
        token_values,
        write_keys,
        read_keys,
        out_gate,
        mixed,
        cotangent,
        w_gate[0],
        w_up[0],
        w_down[0],
        out_proj,
        experts,
        3 * mixed.shape[0] // experts,
        log_decay.shape[0],
    ))
    return (*outs[:5], *(g[None] for g in outs[5:]))


def solution(mesh):
    finer = Mesh(mesh.devices.reshape(4, 4, mesh.shape["tp"]), ("sp_0", "sp_1", "tp"))
    return jax.shard_map(
        body,
        mesh=finer,
        in_specs=(
            P(SP, "tp"),
            P(SP, "tp"),
            P(SP, "tp"),
            P("tp", SP),
            P(SP, "tp"),
            P(None, "tp"),
            P(SP, None),
            P(SP, None),
            P(SP, None),
            P(SP, None),
            P(SP, None, "tp"),
            P(SP, None, "tp"),
            P(SP, "tp", None),
        ),
        out_specs=(
            P(SP, "tp"),
            P(SP, "tp"),
            P(SP, "tp"),
            P(SP, "tp"),
            P(SP, "tp"),
            P(SP, None, "tp"),
            P(SP, None, "tp"),
            P(SP, "tp", None),
        ),
        check_vma=False,
    )
```

```python
import jax
import jax.numpy as jnp
from jax import lax
from jax.experimental import pallas as pl
from jax.experimental.pallas import tpu as pltpu
from jax.sharding import Mesh
from jax.sharding import PartitionSpec as P

HEAD_DIM = 64
STATE = 128
SP = ("sp_0", "sp_1")
F32 = jnp.float32
BF16 = jnp.bfloat16
highest = lax.Precision.HIGHEST


def nn(a, b):
    return lax.dot_general(a, b, (((1,), (0,)), ((), ())), preferred_element_type=F32)


def nt(a, b):
    return lax.dot_general(a, b, (((1,), (1,)), ((), ())), preferred_element_type=F32)


def tn(a, b):
    return lax.dot_general(a, b, (((0,), (0,)), ((), ())), preferred_element_type=F32)


def iota(shape, dim):
    return lax.broadcasted_iota(jnp.int32, shape, dim)


def slots(ids_t, experts):
    tokens = ids_t.shape[1]
    e = iota((experts, tokens), 0)
    member = (ids_t[0:1, :] == e) | (ids_t[1:2, :] == e)
    before = (iota((tokens, tokens), 0) < iota((tokens, tokens), 1)).astype(BF16)
    slot = nn(member.astype(BF16), before)
    return jnp.where(member, slot.astype(jnp.int32), -1)


def weight_rows(ids_t, w_t, experts):
    e = iota((experts, ids_t.shape[1]), 0)
    return jnp.where(ids_t[0:1, :] == e, w_t[0:1, :], 0.0) + jnp.where(
        ids_t[1:2, :] == e, w_t[1:2, :], 0.0
    )


def decays(ld):
    heads, tokens = ld.shape
    ld8 = jnp.concatenate([ld, jnp.zeros((8 - heads, tokens), F32)], axis=0)
    upto = (iota((tokens, tokens), 0) <= iota((tokens, tokens), 1)).astype(F32)
    row = lax.dot_general(
        ld8, upto, (((1,), (0,)), ((), ())), precision=highest, preferred_element_type=F32
    )
    col = lax.dot_general(
        upto, ld8, (((0,), (1,)), ((), ())), precision=highest, preferred_element_type=F32
    )
    return row, col


def by_lane(col, tokens, heads):
    lane = iota((tokens, 2 * HEAD_DIM), 1)
    return jnp.concatenate(
        [
            jnp.where(lane < HEAD_DIM, col[:, 2 * p : 2 * p + 1], col[:, 2 * p + 1 : 2 * p + 2])
            for p in range(heads // 2)
        ],
        axis=1,
    )


def span_weights(row, col, h, tokens):
    lower = iota((tokens, tokens), 0) >= iota((tokens, tokens), 1)
    return jnp.exp(jnp.where(lower, col[:, h : h + 1] - row[h : h + 1, :], -1e30))


def mix_local(x, b, c, row, col, heads):
    tokens = x.shape[0]
    scores = nt(c, b)
    first = iota((tokens, 2 * HEAD_DIM), 1) < HEAD_DIM
    ys = []
    for p in range(heads // 2):
        xp = x[:, 128 * p : 128 * p + 128]
        pair = [
            nn((scores * span_weights(row, col, 2 * p + i, tokens)).astype(BF16), xp)
            for i in range(2)
        ]
        ys.append(jnp.where(first, pair[0], pair[1]))
    tails = by_lane(jnp.exp(col[tokens - 1 : tokens, :] - col), tokens, heads)
    end = tn((x.astype(F32) * tails).astype(BF16), b)
    return jnp.concatenate(ys, axis=1), end


def mix_backward(x, b, c, gate, out_grad, y, lead_grad, entering, row, col, heads):
    tokens = x.shape[0]
    sigma = jax.nn.sigmoid(gate)
    gb = (out_grad * (gate * sigma)).astype(BF16)
    d_gate = out_grad * y * sigma * (1.0 + gate * (1.0 - sigma))
    scores = nt(c, b)
    first = iota((tokens, 2 * HEAD_DIM), 1) < HEAD_DIM
    d_scores = jnp.zeros((tokens, tokens), F32)
    dxs = []
    for p in range(heads // 2):
        xp = x[:, 128 * p : 128 * p + 128]
        gp = gb[:, 128 * p : 128 * p + 128]
        pair = []
        for i in range(2):
            w = span_weights(row, col, 2 * p + i, tokens)
            mine = first if i == 0 else jnp.logical_not(first)
            d_scores = d_scores + w * nt(jnp.where(mine, gp, jnp.zeros_like(gp)), xp)
            pair.append(tn((scores * w).astype(BF16), gp))
        dxs.append(jnp.where(first, pair[0], pair[1]))
    ds = d_scores.astype(BF16)
    return jnp.concatenate(dxs, axis=1), tn(ds, c), nn(ds, b) + nn(lead_grad, entering), d_gate


MESH = pl.DeviceIdType.MESH
STEP = 16


def remote(src, dst, send, recv, device):
    return pltpu.make_async_remote_copy(
        src_ref=src, dst_ref=dst, send_sem=send, recv_sem=recv, device_id=device, device_id_type=MESH
    )


def moe_kernel(
    heads,
    ids,
    wts,
    ld,
    x_in,
    b_in,
    c_in,
    gate_in,
    mixed,
    cot,
    wg_hbm,
    wu_hbm,
    wd_hbm,
    op_hbm,
    dx_out,
    db_out,
    dc_out,
    dgate_out,
    proj_out,
    gg_hbm,
    gu_hbm,
    gd_hbm,
    gm,
    op,
    y_ref,
    gated,
    state_send,
    state_in,
    enter_send,
    enter,
    back_send,
    back_in,
    leave_send,
    leave,
    features,
    mixed_q,
    cot_q,
    cot_own,
    wg,
    wu,
    wd,
    slot_ref,
    weight_ref,
    hot,
    sendbuf,
    rows,
    act,
    dgate,
    dup,
    part,
    part_in,
    q1,
    y1,
    q2,
    y2,
    fin,
    ret,
    sums,
    gg,
    gu,
    gd,
    local,
    a_send,
    a_recv,
    yr_send,
    yr_recv,
    ys_send,
    ys_recv,
    pa_send,
    pa_recv,
    pn_send,
    pn_recv,
    d_send,
    d_recv,
    s1_send,
    s1_recv,
    s2_send,
    s2_recv,
    c_send,
    c_recv,
    g_send,
    g_recv,
    e_send,
    e_recv,
    f_send,
    f_recv,
    b_send,
    b_recv,
    l_send,
    l_recv,
    p_send,
    p_recv,
    q_send,
    q_recv,
    r_send,
    r_recv,
):
    z, x, t = lax.axis_index("sp_0"), lax.axis_index("sp_1"), lax.axis_index("tp")
    s = 4 * z + x
    y, core = t // 2, t % 2
    quarter = t % 4
    beside = (quarter + 2) % 4
    partner_q = quarter + 1 - 2 * core
    partner_beside = (partner_q + 2) % 4
    up, down, partner = (z, x, (t + 2) % 8), (z, x, (t + 6) % 8), (z, x, t + 1 - 2 * core)
    tokens, width = mixed.shape
    experts, _, _, cap, chunk = sendbuf.shape
    share = 2 * chunk
    own = width // 8

    loads = [
        pltpu.make_async_copy(mixed.at[:, pl.ds(quarter * share, share)], mixed_q, local.at[0]),
        pltpu.make_async_copy(cot.at[:, pl.ds(quarter * share, share)], cot_q, local.at[1]),
        pltpu.make_async_copy(cot.at[:, pl.ds(t * own, own)], cot_own, local.at[2]),
        pltpu.make_async_copy(wg_hbm, wg, local.at[3]),
        pltpu.make_async_copy(wu_hbm, wu, local.at[4]),
        pltpu.make_async_copy(wd_hbm, wd, local.at[5]),
        pltpu.make_async_copy(op_hbm, op, local.at[9]),
    ]
    for load in loads:
        load.start()

    barrier = pltpu.get_barrier_semaphore()

    def peer(k):
        to_z, to_x = (z + k % 4) % 4, (x + k % 4 + k // 4) % 4
        return 4 * to_z + to_x, (to_z, to_x, t)

    def greet(k, carry):
        pl.semaphore_signal(barrier, inc=1, device_id=peer(k)[1], device_id_type=MESH)
        return carry

    lax.fori_loop(1, experts, greet, 0)
    for device in (up, down, partner):
        pl.semaphore_signal(barrier, inc=1, device_id=device, device_id_type=MESH)

    slot_ref[...] = slots(ids[...], experts)
    weight_ref[...] = weight_rows(ids[...], wts[...], experts)
    row, col = decays(ld[...])
    inner, last = mix_local(x_in[...], b_in[...], c_in[...], row, col, heads)
    y_ref[...] = inner
    totals = jnp.broadcast_to(row[:, tokens - 1 : tokens], (8, STATE))
    state_send[:, :STEP, :] = last.reshape(experts, STEP, STATE)
    state_send[:, STEP:, :] = jnp.broadcast_to(totals[None], (experts, 8, STATE))
    state_in[s] = state_send[s]

    def over_sp(source_ref, target_ref, send, recv):
        def copy(k):
            j, device = peer(k)
            return remote(source_ref.at[j], target_ref.at[s], send.at[j], recv.at[s], device)

        def wait(k):
            j, device = peer(k)
            remote(source_ref.at[j], target_ref.at[j], send.at[j], recv.at[j], device).wait_recv()

        def each(action):
            def step(k, carry):
                action(k)
                return carry

            lax.fori_loop(1, experts, step, 0)

        return (
            lambda: each(lambda k: copy(k).start()),
            lambda: each(wait),
            lambda: each(lambda k: copy(k).wait_send()),
        )

    def gated_to(k):
        j, device = peer(k)
        return remote(gated.at[s], gated.at[s], q_send.at[j], q_recv.at[s], device)

    def gated_from(k):
        j, device = peer(k)
        return remote(gated.at[j], gated.at[j], q_send.at[j], q_recv.at[j], device)

    def every(action):
        def step(k, carry):
            action(k)
            return carry

        lax.fori_loop(1, experts, step, 0)

    gates = (
        lambda: every(lambda k: gated_to(k).start()),
        lambda: every(lambda k: gated_from(k).wait_recv()),
        lambda: every(lambda k: gated_to(k).wait_send()),
    )
    states = over_sp(state_send, state_in, e_send, e_recv)
    enters = over_sp(enter_send, enter, f_send, f_recv)
    backs = over_sp(back_send, back_in, b_send, b_recv)
    leaves = over_sp(leave_send, leave, l_send, l_recv)

    loads[0].wait()
    loads[1].wait()
    pl.semaphore_wait(barrier, experts - 1 + 3)
    states[0]()

    def to_expert(e, h):
        return remote(
            sendbuf.at[e, h],
            rows.at[quarter, s, h],
            a_send.at[e, h],
            a_recv.at[s, h],
            (e // 4, e % 4, t),
        )

    def build(g, carry):
        place = iota((cap, tokens), 0)
        ones, ws = [], []
        for j in range(4):
            e = peer(4 * g + j)[0]
            mine = place == slot_ref[pl.ds(e, 1), :]
            one = mine.astype(BF16)
            hot[e] = one
            ones.append(one)
            w = jnp.where(mine, weight_ref[pl.ds(e, 1), :], 0.0)
            ws.append(jnp.sum(w, axis=1, keepdims=True))
        one = jnp.concatenate(ones, axis=0)
        w = jnp.concatenate(ws, axis=0)
        plain = nn(one, mixed_q[...]).astype(BF16)
        scaled = (nn(one, cot_q[...]) * w).astype(BF16)
        for j in range(4):
            e = peer(4 * g + j)[0]
            for h in range(2):
                part_rows, f = slice(j * cap, (j + 1) * cap), slice(h * chunk, (h + 1) * chunk)
                sendbuf[e, h, 0] = plain[part_rows, f]
                sendbuf[e, h, 1] = scaled[part_rows, f]
        for h in range(2):
            for j in range(4):
                e = peer(4 * g + j)[0]
                if j > 0:
                    to_expert(e, h).start()
                else:

                    @pl.when(g > 0)
                    def _():
                        to_expert(e, h).start()

        return carry

    lax.fori_loop(0, 4, build, 0)
    rows[quarter, s] = sendbuf[s]
    for load in loads[2:]:
        load.wait()

    def factor(src):
        return jnp.exp(state_in[src, pl.ds(STEP + s // 4, 1), :])

    def scan_forward():
        states[1]()
        held = jnp.zeros((STEP, STATE), F32)
        for src in range(experts):
            enter_send[src] = held.astype(BF16)
            held = factor(src) * held + state_in[src, :STEP, :]
        enter[s] = enter_send[s]
        enters[0]()

    def scan_back():
        backs[1]()
        held = jnp.zeros((STEP, STATE), F32)
        for src in reversed(range(experts)):
            leave_send[src] = held.astype(BF16)
            held = factor(src) * held + back_in[src].astype(F32)
        leave[s] = leave_send[s]
        leaves[0]()

    def finish_forward():
        enters[1]()
        _, col = decays(ld[...])
        leads = by_lane(jnp.exp(col), tokens, heads)
        entering = enter[...].reshape(x_in.shape[1], STATE)
        whole = y_ref[...] + leads * nt(c_in[...], entering)
        g = gate_in[...].astype(F32)
        y_ref[...] = whole
        gated[s] = (whole * (g * jax.nn.sigmoid(g))).astype(BF16)
        gates[0]()

    def source(g, j):
        return 4 * ((z + 4 - j) % 4) + (x + 8 - j - g) % 4

    def arrived(src, h):
        return remote(
            sendbuf.at[src, h], rows.at[quarter, src, h], a_send.at[src, h], a_recv.at[src, h], up
        )

    def rows_up(src, h, q):
        ref = rows.at[q, src, h, 0]
        return remote(ref, ref, yr_send.at[src, h], yr_recv.at[src, h], up)

    def scaled_down(src, h, q):
        ref = rows.at[q, src, h, 1]
        return remote(ref, ref, ys_send.at[src, h], ys_recv.at[src, h], down)

    def across(src, h, q):
        ref = rows.at[q, src, h]
        return remote(ref, ref, pa_send.at[src, h], pa_recv.at[src, h], partner)

    def across_beside(src, h, q):
        ref = rows.at[q, src, h]
        return remote(ref, ref, pn_send.at[src, h], pn_recv.at[src, h], partner)

    def unit(u):
        g, h, j = u // 8, u // 4 % 2, u % 4
        return source(g, j), h

    def forward_own(u):
        src, h = unit(u)

        @pl.when(src != s)
        def _():
            arrived(src, h).wait_recv()

        rows_up(src, h, quarter).start()
        scaled_down(src, h, quarter).start()
        across(src, h, quarter).start()

    def forward_beside(u):
        src, h = unit(u)
        rows_up(src, h, beside).wait_recv()
        scaled_down(src, h, beside).wait_recv()
        across_beside(src, h, beside).start()

    def halves_across(g, f):
        return remote(
            part.at[g, 1 - core, f], part_in.at[g, f], d_send.at[g, f], d_recv.at[g, f], partner
        )

    def multiply(g, q):
        sources = [source(g, j) for j in range(4)]

        @pl.when(q == 0)
        def _():
            for src in sources:
                for h in range(2):
                    across(src, h, partner_q).wait_recv()
                    across_beside(src, h, partner_beside).wait_recv()
            sums[...] = jnp.zeros_like(sums)

        for h in range(2):
            r = jnp.concatenate([rows[q, src, h, 0] for src in sources], axis=0)
            sc = jnp.concatenate([rows[q, src, h, 1] for src in sources], axis=0)
            f = pl.ds(pl.multiple_of(q * share + h * chunk, chunk), chunk)
            sums[0] += nn(r, wg[f, :])
            sums[1] += nn(r, wu[f, :])
            sums[2] += nt(sc, wd[:, f])

    def activate(g):
        sources = [source(g, j) for j in range(4)]
        gate_pre, up_pre, d_hidden = sums[0], sums[1], sums[2]
        sigma = jax.nn.sigmoid(gate_pre)
        silu = gate_pre * sigma
        dg = (d_hidden * up_pre * sigma * (1.0 + gate_pre * (1.0 - sigma))).astype(BF16)
        du = (d_hidden * silu).astype(BF16)
        hidden = (silu * up_pre).astype(BF16)
        for j, src in enumerate(sources):
            part_rows = slice(j * cap, (j + 1) * cap)
            act[src] = hidden[part_rows]
            dgate[src] = dg[part_rows]
            dup[src] = du[part_rows]

    def back(g, k):
        sources = [source(g, j) for j in range(4)]
        dg = jnp.concatenate([dgate[src] for src in sources], axis=0)
        du = jnp.concatenate([dup[src] for src in sources], axis=0)
        f = (y + 2 + 3 * k) % 4
        for m in range(2):
            cols = pl.ds(pl.multiple_of(f * share + m * own, own), own)
            part[g, m, f] = (nt(dg, wg[cols, :]) + nt(du, wu[cols, :])).astype(BF16)
        halves_across(g, f).start()

    def both(g, f):
        return part[g, core, f].astype(F32) + part_in[g, f].astype(F32)

    half = 2 * cap

    def first_step(g, way):
        return remote(
            q1.at[g, way], y1.at[g, way], s1_send.at[g, way], s1_recv.at[g, way], (up, down)[way]
        )

    def second_step(g, way):
        return remote(
            q2.at[g, way], y2.at[g, way], s2_send.at[g, way], s2_recv.at[g, way], (up, down)[way]
        )

    def sum_far(g):
        halves_across(g, (y + 2) % 4).wait_recv()
        far = both(g, (y + 2) % 4)
        q1[g, 0] = far[:half].astype(BF16)
        q1[g, 1] = far[half:].astype(BF16)
        first_step(g, 0).start()
        first_step(g, 1).start()

    def sum_near(g):
        first_step(g, 0).wait_recv()
        halves_across(g, (y + 1) % 4).wait_recv()
        above = both(g, (y + 1) % 4)
        q2[g, 0, :half] = (above[:half] + y1[g, 0].astype(F32)).astype(BF16)
        q2[g, 0, half:] = above[half:].astype(BF16)
        second_step(g, 0).start()
        first_step(g, 1).wait_recv()
        halves_across(g, (y + 3) % 4).wait_recv()
        below = both(g, (y + 3) % 4)
        q2[g, 1, :half] = below[:half].astype(BF16)
        q2[g, 1, half:] = (below[half:] + y1[g, 1].astype(F32)).astype(BF16)
        second_step(g, 1).start()

    def to_owner(g, src):
        return remote(
            fin.at[src], ret.at[s], c_send.at[src], c_recv.at[s], (src // 4, src % 4, t)
        )

    def from_expert(e):
        return remote(fin.at[e], ret.at[e], c_send.at[e], c_recv.at[e], up)

    def sum_own(g):
        second_step(g, 0).wait_recv()
        second_step(g, 1).wait_recv()
        halves_across(g, y).wait_recv()
        total = (both(g, y) + y2[g, 0].astype(F32) + y2[g, 1].astype(F32)).astype(BF16)
        for j in range(4):
            fin[source(g, j)] = total[j * cap : (j + 1) * cap]
        for j in range(4):
            src = source(g, j)
            if j > 0:
                to_owner(g, src).start()
            else:

                @pl.when(g > 0)
                def _():
                    to_owner(g, src).start()

                @pl.when(g == 0)
                def _():
                    ret[s] = fin[s]

    def grad_rows(target, which):
        for k in range(8):
            r = rows[k // 2, :, k % 2, 0].reshape(experts * cap, chunk)
            target[k * chunk : (k + 1) * chunk, :] = tn(
                r, which[...].reshape(experts * cap, -1)
            ).astype(BF16)

    def grad_down():
        hidden = act[...].reshape(experts * cap, -1)
        for k in range(8):
            sc = rows[k // 2, :, k % 2, 1].reshape(experts * cap, chunk)
            gd[:, k * chunk : (k + 1) * chunk] = tn(hidden, sc).astype(BF16)

    stores = [
        pltpu.make_async_copy(gg, gg_hbm, local.at[6]),
        pltpu.make_async_copy(gu, gu_hbm, local.at[7]),
        pltpu.make_async_copy(gd, gd_hbm, local.at[8]),
    ]

    def turn(u, carry):
        @pl.when(u < 32)
        def _():
            forward_own(u)

        v = u - 5

        @pl.when((v >= 0) & (v < 32))
        def _():
            forward_beside(v)

        m = u - 14
        g, k = (m + 64) // 8 - 8, (m + 64) % 8
        active = (m >= 0) & (m < 32)

        @pl.when(active & (k < 4))
        def _():
            multiply(g, k)

        @pl.when(active & (k == 3))
        def _():
            activate(g)

        @pl.when(active & (k >= 4))
        def _():
            back(g, k - 4)

        @pl.when(active & (k == 5))
        def _():
            sum_far(g)

        for late, task in ((11, sum_near), (17, sum_own)):
            w = m - late

            @pl.when((w >= 0) & (w < 32) & ((w + 64) % 8 == 0))
            def _():
                task((w + 64) // 8 - 8)

        @pl.when(u == 20)
        def _():
            scan_forward()

        @pl.when(u == 33)
        def _():
            finish_forward()

        @pl.when(m == 32)
        def _():
            grad_rows(gg, dgate)
            stores[0].start()

        @pl.when(m == 24 + 11)
        def _():
            grad_rows(gu, dup)
            stores[1].start()
            grad_down()
            stores[2].start()

        return carry

    lax.fori_loop(0, 14 + 24 + 17 + 1, turn, 0)

    def sent(k, carry):
        e = peer(k)[0]
        to_expert(e, 0).wait_send()
        to_expert(e, 1).wait_send()
        to_owner(0, e).wait_send()
        return carry

    lax.fori_loop(1, experts, sent, 0)

    def forwarded(k, carry):
        for h in range(2):
            rows_up(k, h, quarter).wait_send()
            scaled_down(k, h, quarter).wait_send()
            across(k, h, quarter).wait_send()
            across_beside(k, h, beside).wait_send()
        return carry

    lax.fori_loop(0, experts, forwarded, 0)

    def summed(g, carry):
        for f in range(4):
            halves_across(g, f).wait_send()
        for way in range(2):
            first_step(g, way).wait_send()
            second_step(g, way).wait_send()
        return carry

    lax.fori_loop(0, 4, summed, 0)
    for exchange in (states, enters):
        exchange[2]()

    def take(k, carry):
        from_expert(peer(k)[0]).wait_recv()
        return carry

    lax.fori_loop(1, experts, take, 0)
    places = experts * cap
    picked = tn(hot[...].reshape(places, tokens), ret[...].reshape(places, own))
    gm[t] = (cot_own[...].astype(F32) + picked).astype(BF16)

    low, high = pl.ds(0, tokens // 2), pl.ds(tokens // 2, tokens // 2)
    below, above, far = (t + 6) % 8, (t + 2) % 8, (t + 4) % 8
    mate = t + 1 - 2 * core
    m_below, m_above, m_far = (mate + 6) % 8, (mate + 2) % 8, (mate + 4) % 8

    def gather(k, src, device, part_rows=None):
        ref = gm.at[src] if part_rows is None else gm.at[src, part_rows]
        return remote(ref, ref, g_send.at[k], g_recv.at[k], device)

    columns = gated.shape[2]
    my_half = pl.ds(core * (tokens // 2), tokens // 2)
    mate_half = pl.ds((1 - core) * (tokens // 2), tokens // 2)

    def to_features(i, k):
        return remote(
            gm.at[i // 2, my_half, k * columns : (k + 1) * columns],
            features.at[s, my_half],
            p_send.at[i],
            p_recv.at[s],
            (i // 4, i % 4, t),
        )

    def share_half(src, half_rows):
        ref = features.at[src, half_rows]
        return remote(ref, ref, r_send.at[src], r_recv.at[src], partner)

    def send_rows(j):
        for k in range(2):
            i = 2 * j + k

            @pl.when(i != s)
            def _():
                to_features(i, k).start()

            @pl.when(i == s)
            def _():
                features[s] = gm[j, :, k * columns : (k + 1) * columns]

    def project(j):
        return nn(gm[j], op[pl.ds(j * own, own), :])

    def take_features(k):
        src = peer(k)[0]
        remote(
            features.at[src, my_half], features.at[src, my_half], p_send.at[src], p_recv.at[src], up
        ).wait_recv()
        share_half(src, my_half).start()

    def multiply_features(k):
        src = peer(k)[0]
        share_half(src, mate_half).wait_recv()
        proj_out[...] += tn(features[src], gated[src])

    moves = (
        (1, t, up, low),
        (2, t, up, high),
        (3, t, down, high),
        (4, t, down, low),
        (0, t, partner, None),
        (5, below, up, low),
        (6, above, down, high),
        (7, below, partner, None),
        (8, above, partner, None),
        (9, far, partner, None),
    )

    def start(k):
        gather(*[m for m in moves if m[0] == k][0]).start()

    for k in (1, 3, 2, 4, 0):
        start(k)
    out_grad = project(t)
    send_rows(t)
    gather(0, mate, partner).wait_recv()
    out_grad = out_grad + project(mate)
    send_rows(mate)
    gather(1, below, up, low).wait_recv()
    start(5)
    gather(3, above, down, high).wait_recv()
    start(6)
    gather(2, below, up, high).wait_recv()
    start(7)
    gather(4, above, down, low).wait_recv()
    start(8)
    out_grad = out_grad + project(above)
    send_rows(above)
    out_grad = out_grad + project(below)
    send_rows(below)
    gather(8, m_above, partner).wait_recv()
    out_grad = out_grad + project(m_above)
    send_rows(m_above)
    gather(7, m_below, partner).wait_recv()
    out_grad = out_grad + project(m_below)
    send_rows(m_below)
    gather(5, far, up, low).wait_recv()
    gather(6, far, down, high).wait_recv()
    start(9)
    out_grad = out_grad + project(far)
    gather(9, m_far, partner).wait_recv()
    out_grad = out_grad + project(m_far)

    row, col = decays(ld[...])
    leads = by_lane(jnp.exp(col), tokens, heads)
    gate = gate_in[...].astype(F32)
    lead_grad = (out_grad * (gate * jax.nn.sigmoid(gate)) * leads).astype(BF16)
    back_send[...] = tn(lead_grad, c_in[...]).astype(BF16).reshape(experts, STEP, STATE)
    back_in[s] = back_send[s]
    backs[0]()
    for j in (far, m_far):
        send_rows(j)
    backward = mix_backward(
        x_in[...], b_in[...], c_in[...], gate, out_grad, y_ref[...], lead_grad,
        enter[...].reshape(x_in.shape[1], STATE), row, col, heads
    )
    dgate_out[...] = backward[3].astype(BF16)
    dc_out[...] = backward[2].astype(BF16)
    scan_back()
    tails = by_lane(jnp.exp(col[tokens - 1 : tokens, :] - col), tokens, heads)
    tail_values = (x_in[...].astype(F32) * tails).astype(BF16)
    every(take_features)
    gates[1]()
    proj_out[...] = tn(features[s], gated[s])
    every(multiply_features)
    def features_sent(k):
        i = peer(k)[0]
        to_features(i, 0).wait_send()
        share_half(i, my_half).wait_send()

    every(features_sent)
    gates[2]()
    backs[2]()
    for move in moves:
        gather(*move).wait_send()
    for store in stores:
        store.wait()

    leaves[1]()
    leaving = leave[...].reshape(x_in.shape[1], STATE)
    dx_out[...] = (backward[0] + tails * nt(b_in[...], leaving)).astype(BF16)
    db_out[...] = (backward[1] + nn(tail_values, leaving)).astype(BF16)

    leaves[2]()


def whole(ids, wts, ld, x, b, c, gate, mixed, cot, wg, wu, wd, op, experts, cap, heads):
    tokens, width = mixed.shape
    hidden = wg.shape[1]
    channels = x.shape[1]
    share, own = width // 4, width // 8
    vmem = pl.BlockSpec(memory_space=pltpu.VMEM)
    hbm = pl.BlockSpec(memory_space=pl.ANY)
    dma = pltpu.SemaphoreType.DMA

    def kernel(*refs):
        moe_kernel(heads, *refs)

    def buf(*shape, dtype=BF16):
        return pltpu.VMEM(shape, dtype)

    n = 4 * cap
    return pl.pallas_call(
        kernel,
        out_shape=[
            jax.ShapeDtypeStruct(x.shape, BF16),
            jax.ShapeDtypeStruct(b.shape, BF16),
            jax.ShapeDtypeStruct(c.shape, BF16),
            jax.ShapeDtypeStruct(gate.shape, BF16),
            jax.ShapeDtypeStruct((width // experts, channels), F32),
            jax.ShapeDtypeStruct(wg.shape, BF16),
            jax.ShapeDtypeStruct(wu.shape, BF16),
            jax.ShapeDtypeStruct(wd.shape, BF16),
        ],
        in_specs=[vmem] * 7 + [hbm] * 6,
        out_specs=[vmem] * 5 + [hbm] * 3,
        scratch_shapes=[
            buf(8, tokens, own),
            buf(*op.shape),
            buf(tokens, channels, dtype=F32),
            buf(experts, tokens, channels),
            buf(experts, STEP + 8, STATE, dtype=F32),
            buf(experts, STEP + 8, STATE, dtype=F32),
            buf(experts, STEP, STATE),
            buf(experts, STEP, STATE),
            buf(experts, STEP, STATE),
            buf(experts, STEP, STATE),
            buf(experts, STEP, STATE),
            buf(experts, STEP, STATE),
            buf(experts, tokens, width // experts),
            buf(tokens, share),
            buf(tokens, share),
            buf(tokens, own),
            buf(*wg.shape),
            buf(*wu.shape),
            buf(*wd.shape),
            buf(experts, tokens, dtype=jnp.int32),
            buf(experts, tokens, dtype=F32),
            buf(experts, cap, tokens),
            buf(experts, 2, 2, cap, own),
            buf(4, experts, 2, 2, cap, own),
            buf(experts, cap, hidden),
            buf(experts, cap, hidden),
            buf(experts, cap, hidden),
            buf(4, 2, 4, n, own),
            buf(4, 4, n, own),
            buf(4, 2, n // 2, own),
            buf(4, 2, n // 2, own),
            buf(4, 2, n, own),
            buf(4, 2, n, own),
            buf(experts, cap, own),
            buf(experts, cap, own),
            buf(3, n, hidden, dtype=F32),
            buf(*wg.shape),
            buf(*wu.shape),
            buf(*wd.shape),
            dma((10,)),
        ]
        + [dma((experts, 2))] * 10
        + [dma((4, 4))] * 2
        + [dma((4, 2))] * 4
        + [dma((experts,))] * 2
        + [dma((10,))] * 2
        + [dma((experts,))] * 14,
        compiler_params=pltpu.CompilerParams(
            collective_id=0, has_side_effects=True, vmem_limit_bytes=60 * 2**20
        ),
        name="whole",
    )(ids, wts, ld, x, b, c, gate, mixed, cot, wg, wu, wd, op)


def hand_out(arrays):
    pieces = []
    for k, a in enumerate(arrays):
        count = max(1, a.size * a.dtype.itemsize // 2**19)
        step = a.shape[0] // count
        pieces += [(k, pl.ds(m * step, step)) for m in range(count)]

    def kernel(*refs):
        n = len(arrays)
        ins, outs, held, (come, go) = refs[:n], refs[n : 2 * n], refs[2 * n : 3 * n], refs[3 * n :]
        fetch = [
            pltpu.make_async_copy(ins[k].at[at], held[k].at[at], come.at[m])
            for m, (k, at) in enumerate(pieces)
        ]
        store = [
            pltpu.make_async_copy(held[k].at[at], outs[k].at[at], go.at[m])
            for m, (k, at) in enumerate(pieces)
        ]
        for f in fetch:
            f.start()
        for f, g in zip(fetch, store):
            f.wait()
            g.start()
        for g in store:
            g.wait()

    hbm = pl.BlockSpec(memory_space=pl.ANY)
    return pl.pallas_call(
        kernel,
        out_shape=[jax.ShapeDtypeStruct(a.shape, a.dtype) for a in arrays],
        in_specs=[hbm] * len(arrays),
        out_specs=[hbm] * len(arrays),
        scratch_shapes=[pltpu.VMEM(a.shape, a.dtype) for a in arrays]
        + [pltpu.SemaphoreType.DMA((len(pieces),))] * 2,
        name="hand_out",
    )(*arrays)


def body(
    token_values,
    write_keys,
    read_keys,
    log_decay,
    out_gate,
    out_proj,
    mixed,
    cotangent,
    route_ids,
    route_weights,
    w_gate,
    w_up,
    w_down,
):
    experts = lax.axis_size(SP)
    outs = hand_out(whole(
        route_ids.T,
        route_weights.T,
        log_decay,
        token_values,
        write_keys,
        read_keys,
        out_gate,
        mixed,
        cotangent,
        w_gate[0],
        w_up[0],
        w_down[0],
        out_proj,
        experts,
        3 * mixed.shape[0] // experts,
        log_decay.shape[0],
    ))
    return (*outs[:5], *(g[None] for g in outs[5:]))


def solution(mesh):
    finer = Mesh(mesh.devices.reshape(4, 4, mesh.shape["tp"]), ("sp_0", "sp_1", "tp"))
    return jax.shard_map(
        body,
        mesh=finer,
        in_specs=(
            P(SP, "tp"),
            P(SP, "tp"),
            P(SP, "tp"),
            P("tp", SP),
            P(SP, "tp"),
            P(None, "tp"),
            P(SP, None),
            P(SP, None),
            P(SP, None),
            P(SP, None),
            P(SP, None, "tp"),
            P(SP, None, "tp"),
            P(SP, "tp", None),
        ),
        out_specs=(
            P(SP, "tp"),
            P(SP, "tp"),
            P(SP, "tp"),
            P(SP, "tp"),
            P(SP, "tp"),
            P(SP, None, "tp"),
            P(SP, None, "tp"),
            P(SP, "tp", None),
        ),
        check_vma=False,
    )
```

```python
import jax
import jax.numpy as jnp
from jax import lax
from jax.experimental import pallas as pl
from jax.experimental.pallas import tpu as pltpu
from jax.sharding import Mesh
from jax.sharding import PartitionSpec as P

HEAD_DIM = 64
STATE = 128
SP = ("sp_0", "sp_1")
F32 = jnp.float32
BF16 = jnp.bfloat16
highest = lax.Precision.HIGHEST


def nn(a, b):
    return lax.dot_general(a, b, (((1,), (0,)), ((), ())), preferred_element_type=F32)


def nt(a, b):
    return lax.dot_general(a, b, (((1,), (1,)), ((), ())), preferred_element_type=F32)


def tn(a, b):
    return lax.dot_general(a, b, (((0,), (0,)), ((), ())), preferred_element_type=F32)


def iota(shape, dim):
    return lax.broadcasted_iota(jnp.int32, shape, dim)


def slots(ids_t, experts):
    tokens = ids_t.shape[1]
    e = iota((experts, tokens), 0)
    member = (ids_t[0:1, :] == e) | (ids_t[1:2, :] == e)
    before = (iota((tokens, tokens), 0) < iota((tokens, tokens), 1)).astype(BF16)
    slot = nn(member.astype(BF16), before)
    return jnp.where(member, slot.astype(jnp.int32), -1)


def weight_rows(ids_t, w_t, experts):
    e = iota((experts, ids_t.shape[1]), 0)
    return jnp.where(ids_t[0:1, :] == e, w_t[0:1, :], 0.0) + jnp.where(
        ids_t[1:2, :] == e, w_t[1:2, :], 0.0
    )


def decays(ld):
    heads, tokens = ld.shape
    ld8 = jnp.concatenate([ld, jnp.zeros((8 - heads, tokens), F32)], axis=0)
    upto = (iota((tokens, tokens), 0) <= iota((tokens, tokens), 1)).astype(F32)
    row = lax.dot_general(
        ld8, upto, (((1,), (0,)), ((), ())), precision=highest, preferred_element_type=F32
    )
    col = lax.dot_general(
        upto, ld8, (((0,), (1,)), ((), ())), precision=highest, preferred_element_type=F32
    )
    return row, col


def by_lane(col, tokens, heads):
    lane = iota((tokens, 2 * HEAD_DIM), 1)
    return jnp.concatenate(
        [
            jnp.where(lane < HEAD_DIM, col[:, 2 * p : 2 * p + 1], col[:, 2 * p + 1 : 2 * p + 2])
            for p in range(heads // 2)
        ],
        axis=1,
    )


def span_weights(row, col, h, tokens):
    lower = iota((tokens, tokens), 0) >= iota((tokens, tokens), 1)
    return jnp.exp(jnp.where(lower, col[:, h : h + 1] - row[h : h + 1, :], -1e30))


def mix_local(x, b, c, row, col, heads):
    tokens = x.shape[0]
    scores = nt(c, b)
    first = iota((tokens, 2 * HEAD_DIM), 1) < HEAD_DIM
    ys = []
    for p in range(heads // 2):
        xp = x[:, 128 * p : 128 * p + 128]
        pair = [
            nn((scores * span_weights(row, col, 2 * p + i, tokens)).astype(BF16), xp)
            for i in range(2)
        ]
        ys.append(jnp.where(first, pair[0], pair[1]))
    tails = by_lane(jnp.exp(col[tokens - 1 : tokens, :] - col), tokens, heads)
    end = tn((x.astype(F32) * tails).astype(BF16), b)
    return jnp.concatenate(ys, axis=1), end


def mix_backward(x, b, c, gate, out_grad, y, lead_grad, entering, row, col, heads):
    tokens = x.shape[0]
    sigma = jax.nn.sigmoid(gate)
    gb = (out_grad * (gate * sigma)).astype(BF16)
    d_gate = out_grad * y * sigma * (1.0 + gate * (1.0 - sigma))
    scores = nt(c, b)
    first = iota((tokens, 2 * HEAD_DIM), 1) < HEAD_DIM
    d_scores = jnp.zeros((tokens, tokens), F32)
    dxs = []
    for p in range(heads // 2):
        xp = x[:, 128 * p : 128 * p + 128]
        gp = gb[:, 128 * p : 128 * p + 128]
        pair = []
        for i in range(2):
            w = span_weights(row, col, 2 * p + i, tokens)
            mine = first if i == 0 else jnp.logical_not(first)
            d_scores = d_scores + w * nt(jnp.where(mine, gp, jnp.zeros_like(gp)), xp)
            pair.append(tn((scores * w).astype(BF16), gp))
        dxs.append(jnp.where(first, pair[0], pair[1]))
    ds = d_scores.astype(BF16)
    return jnp.concatenate(dxs, axis=1), tn(ds, c), nn(ds, b) + nn(lead_grad, entering), d_gate


MESH = pl.DeviceIdType.MESH
STEP = 16


def remote(src, dst, send, recv, device):
    return pltpu.make_async_remote_copy(
        src_ref=src, dst_ref=dst, send_sem=send, recv_sem=recv, device_id=device, device_id_type=MESH
    )


def moe_kernel(
    heads,
    ids,
    wts,
    ld,
    x_in,
    b_in,
    c_in,
    gate_in,
    mixed,
    cot,
    wg_hbm,
    wu_hbm,
    wd_hbm,
    op_hbm,
    dx_hbm,
    db_hbm,
    dc_hbm,
    dgate_hbm,
    proj_hbm,
    gg_hbm,
    gu_hbm,
    gd_hbm,
    dx_out,
    db_out,
    dc_out,
    dgate_out,
    proj_out,
    gm,
    op,
    y_ref,
    gated,
    state_send,
    state_in,
    enter_send,
    enter,
    back_send,
    back_in,
    leave_send,
    leave,
    features,
    mixed_q,
    cot_q,
    cot_own,
    wg,
    wu,
    wd,
    slot_ref,
    weight_ref,
    hot,
    sendbuf,
    rows,
    act,
    dgate,
    dup,
    part,
    part_in,
    q1,
    y1,
    q2,
    y2,
    fin,
    ret,
    sums,
    gg,
    gu,
    gd,
    local,
    a_send,
    a_recv,
    yr_send,
    n_recv,
    ys_send,
    pa_send,
    pa_recv,
    pn_send,
    pn_recv,
    d_send,
    d_recv,
    s1_send,
    s1_recv,
    s2_send,
    s2_recv,
    c_send,
    c_recv,
    g_send,
    g_recv,
    e_send,
    e_recv,
    f_send,
    f_recv,
    b_send,
    b_recv,
    l_send,
    l_recv,
    p_send,
    p_recv,
    q_send,
    q_recv,
    r_send,
    r_recv,
):
    z, x, t = lax.axis_index("sp_0"), lax.axis_index("sp_1"), lax.axis_index("tp")
    s = 4 * z + x
    y, core = t // 2, t % 2
    quarter = t % 4
    beside = (quarter + 2) % 4
    partner_q = quarter + 1 - 2 * core
    partner_beside = (partner_q + 2) % 4
    up, down, partner = (z, x, (t + 2) % 8), (z, x, (t + 6) % 8), (z, x, t + 1 - 2 * core)
    tokens, width = mixed.shape
    experts, _, _, cap, chunk = sendbuf.shape
    share = 2 * chunk
    own = width // 8

    loads = [
        pltpu.make_async_copy(mixed.at[:, pl.ds(quarter * share, share)], mixed_q, local.at[0]),
        pltpu.make_async_copy(cot.at[:, pl.ds(quarter * share, share)], cot_q, local.at[1]),
        pltpu.make_async_copy(cot.at[:, pl.ds(t * own, own)], cot_own, local.at[2]),
        pltpu.make_async_copy(wg_hbm, wg, local.at[3]),
        pltpu.make_async_copy(wu_hbm, wu, local.at[4]),
        pltpu.make_async_copy(wd_hbm, wd, local.at[5]),
        pltpu.make_async_copy(op_hbm, op, local.at[9]),
    ]
    for load in loads:
        load.start()

    barrier = pltpu.get_barrier_semaphore()

    def peer(k):
        to_z, to_x = (z + k % 4) % 4, (x + k % 4 + k // 4) % 4
        return 4 * to_z + to_x, (to_z, to_x, t)

    def greet(k, carry):
        pl.semaphore_signal(barrier, inc=1, device_id=peer(k)[1], device_id_type=MESH)
        return carry

    lax.fori_loop(1, experts, greet, 0)
    for device in (up, down, partner):
        pl.semaphore_signal(barrier, inc=1, device_id=device, device_id_type=MESH)

    slot_ref[...] = slots(ids[...], experts)
    weight_ref[...] = weight_rows(ids[...], wts[...], experts)
    row, col = decays(ld[...])
    inner, last = mix_local(x_in[...], b_in[...], c_in[...], row, col, heads)
    y_ref[...] = inner
    totals = jnp.broadcast_to(row[:, tokens - 1 : tokens], (8, STATE))
    state_send[:, :STEP, :] = last.reshape(experts, STEP, STATE)
    state_send[:, STEP:, :] = jnp.broadcast_to(totals[None], (experts, 8, STATE))
    state_in[s] = state_send[s]

    others = pl.ds(0, experts - 1)

    def every(action):
        def step(k, carry):
            action(k)
            return carry

        lax.fori_loop(1, experts, step, 0)

    def over_sp(source_ref, target_ref, send, recv):
        def copy(k):
            j, device = peer(k)
            return remote(source_ref.at[j], target_ref.at[s], send, recv, device)

        return (
            lambda: every(lambda k: copy(k).start()),
            lambda: remote(source_ref.at[others], target_ref.at[others], send, recv, up).wait_recv(),
            lambda: remote(source_ref.at[others], target_ref.at[others], send, recv, up).wait_send(),
        )

    def gated_to(k):
        return remote(gated.at[s], gated.at[s], q_send, q_recv, peer(k)[1])

    def gated_all():
        return remote(gated.at[others], gated.at[others], q_send, q_recv, up)

    gates = (
        lambda: every(lambda k: gated_to(k).start()),
        lambda: gated_all().wait_recv(),
        lambda: gated_all().wait_send(),
    )
    states = over_sp(state_send, state_in, e_send, e_recv)
    enters = over_sp(enter_send, enter, f_send, f_recv)
    backs = over_sp(back_send, back_in, b_send, b_recv)
    leaves = over_sp(leave_send, leave, l_send, l_recv)

    loads[0].wait()
    loads[1].wait()
    pl.semaphore_wait(barrier, experts - 1 + 3)
    states[0]()

    def to_expert(e, h):
        return remote(
            sendbuf.at[e, h], rows.at[quarter, s, h], a_send, a_recv.at[s, h], (e // 4, e % 4, t)
        )

    def build(g, carry):
        place = iota((cap, tokens), 0)
        ones, ws = [], []
        for j in range(4):
            e = peer(4 * g + j)[0]
            mine = place == slot_ref[pl.ds(e, 1), :]
            one = mine.astype(BF16)
            hot[e] = one
            ones.append(one)
            w = jnp.where(mine, weight_ref[pl.ds(e, 1), :], 0.0)
            ws.append(jnp.sum(w, axis=1, keepdims=True))
        one = jnp.concatenate(ones, axis=0)
        w = jnp.concatenate(ws, axis=0)
        plain = nn(one, mixed_q[...]).astype(BF16)
        scaled = (nn(one, cot_q[...]) * w).astype(BF16)
        for j in range(4):
            e = peer(4 * g + j)[0]
            for h in range(2):
                part_rows, f = slice(j * cap, (j + 1) * cap), slice(h * chunk, (h + 1) * chunk)
                sendbuf[e, h, 0] = plain[part_rows, f]
                sendbuf[e, h, 1] = scaled[part_rows, f]
        for h in range(2):
            for j in range(4):
                e = peer(4 * g + j)[0]
                if j > 0:
                    to_expert(e, h).start()
                else:

                    @pl.when(g > 0)
                    def _():
                        to_expert(e, h).start()

        return carry

    lax.fori_loop(0, 4, build, 0)
    rows[quarter, s] = sendbuf[s]
    for load in loads[2:]:
        load.wait()

    def factor(src):
        return jnp.exp(state_in[src, pl.ds(STEP + s // 4, 1), :])

    def scan_forward():
        states[1]()
        held = jnp.zeros((STEP, STATE), F32)
        for src in range(experts):
            enter_send[src] = held.astype(BF16)
            held = factor(src) * held + state_in[src, :STEP, :]
        enter[s] = enter_send[s]
        enters[0]()

    def scan_back():
        backs[1]()
        held = jnp.zeros((STEP, STATE), F32)
        for src in reversed(range(experts)):
            leave_send[src] = held.astype(BF16)
            held = factor(src) * held + back_in[src].astype(F32)
        leave[s] = leave_send[s]
        leaves[0]()

    def finish_forward():
        enters[1]()
        _, col = decays(ld[...])
        leads = by_lane(jnp.exp(col), tokens, heads)
        entering = enter[...].reshape(x_in.shape[1], STATE)
        whole = y_ref[...] + leads * nt(c_in[...], entering)
        g = gate_in[...].astype(F32)
        y_ref[...] = whole
        gated[s] = (whole * (g * jax.nn.sigmoid(g))).astype(BF16)
        gates[0]()

    def source(g, j):
        return 4 * ((z + 4 - j) % 4) + (x + 8 - j - g) % 4

    def arrived(src, h):
        return remote(
            sendbuf.at[src, h], rows.at[quarter, src, h], a_send, a_recv.at[src, h], up
        )

    def rows_up(src, h, q):
        ref = rows.at[q, src, h, 0]
        return remote(ref, ref, yr_send, n_recv.at[src, h], up)

    def scaled_down(src, h, q):
        ref = rows.at[q, src, h, 1]
        return remote(ref, ref, ys_send, n_recv.at[src, h], down)

    def across(src, h, q, g):
        ref = rows.at[q, src, h]
        return remote(ref, ref, pa_send, pa_recv.at[g], partner)

    def across_beside(src, h, q, g):
        ref = rows.at[q, src, h]
        return remote(ref, ref, pn_send, pn_recv.at[g], partner)

    def unit(u):
        g, h, j = u // 8, u // 4 % 2, u % 4
        return source(g, j), h

    def forward_own(u):
        src, h = unit(u)

        @pl.when(src != s)
        def _():
            arrived(src, h).wait_recv()

        rows_up(src, h, quarter).start()
        scaled_down(src, h, quarter).start()
        across(src, h, quarter, u // 8).start()

    def forward_beside(u):
        src, h = unit(u)
        ref = rows.at[beside, src, h]
        remote(ref, ref, yr_send, n_recv.at[src, h], up).wait_recv()
        across_beside(src, h, beside, u // 8).start()

    def halves_across(g, f):
        return remote(
            part.at[g, 1 - core, f], part_in.at[g, f], d_send, d_recv.at[g, f], partner
        )

    def multiply(g, q):
        sources = [source(g, j) for j in range(4)]

        @pl.when(q == 0)
        def _():
            four = rows.at[partner_q, pl.ds(0, 4)]
            remote(four, four, pa_send, pa_recv.at[g], partner).wait_recv()
            remote(four, four, pn_send, pn_recv.at[g], partner).wait_recv()
            sums[...] = jnp.zeros_like(sums)

        for h in range(2):
            r = jnp.concatenate([rows[q, src, h, 0] for src in sources], axis=0)
            sc = jnp.concatenate([rows[q, src, h, 1] for src in sources], axis=0)
            f = pl.ds(pl.multiple_of(q * share + h * chunk, chunk), chunk)
            sums[0] += nn(r, wg[f, :])
            sums[1] += nn(r, wu[f, :])
            sums[2] += nt(sc, wd[:, f])

    def activate(g):
        sources = [source(g, j) for j in range(4)]
        gate_pre, up_pre, d_hidden = sums[0], sums[1], sums[2]
        sigma = jax.nn.sigmoid(gate_pre)
        silu = gate_pre * sigma
        dg = (d_hidden * up_pre * sigma * (1.0 + gate_pre * (1.0 - sigma))).astype(BF16)
        du = (d_hidden * silu).astype(BF16)
        hidden = (silu * up_pre).astype(BF16)
        for j, src in enumerate(sources):
            part_rows = slice(j * cap, (j + 1) * cap)
            act[src] = hidden[part_rows]
            dgate[src] = dg[part_rows]
            dup[src] = du[part_rows]

    def back(g, k):
        sources = [source(g, j) for j in range(4)]
        dg = jnp.concatenate([dgate[src] for src in sources], axis=0)
        du = jnp.concatenate([dup[src] for src in sources], axis=0)
        f = (y + 2 + 3 * k) % 4
        for m in range(2):
            cols = pl.ds(pl.multiple_of(f * share + m * own, own), own)
            part[g, m, f] = (nt(dg, wg[cols, :]) + nt(du, wu[cols, :])).astype(BF16)
        halves_across(g, f).start()

    def both(g, f):
        return part[g, core, f].astype(F32) + part_in[g, f].astype(F32)

    half = 2 * cap

    def first_step(g, way):
        return remote(
            q1.at[g, way], y1.at[g, way], s1_send, s1_recv.at[g, way], (up, down)[way]
        )

    def second_step(g, way):
        return remote(
            q2.at[g, way], y2.at[g, way], s2_send, s2_recv.at[g, way], (up, down)[way]
        )

    def sum_far(g):
        halves_across(g, (y + 2) % 4).wait_recv()
        far = both(g, (y + 2) % 4)
        q1[g, 0] = far[:half].astype(BF16)
        q1[g, 1] = far[half:].astype(BF16)
        first_step(g, 0).start()
        first_step(g, 1).start()

    def sum_near(g):
        first_step(g, 0).wait_recv()
        halves_across(g, (y + 1) % 4).wait_recv()
        above = both(g, (y + 1) % 4)
        q2[g, 0, :half] = (above[:half] + y1[g, 0].astype(F32)).astype(BF16)
        q2[g, 0, half:] = above[half:].astype(BF16)
        second_step(g, 0).start()
        first_step(g, 1).wait_recv()
        halves_across(g, (y + 3) % 4).wait_recv()
        below = both(g, (y + 3) % 4)
        q2[g, 1, :half] = below[:half].astype(BF16)
        q2[g, 1, half:] = (below[half:] + y1[g, 1].astype(F32)).astype(BF16)
        second_step(g, 1).start()

    def to_owner(g, src):
        return remote(
            fin.at[src], ret.at[s], c_send, c_recv, (src // 4, src % 4, t)
        )

    def sum_own(g):
        second_step(g, 0).wait_recv()
        second_step(g, 1).wait_recv()
        halves_across(g, y).wait_recv()
        total = (both(g, y) + y2[g, 0].astype(F32) + y2[g, 1].astype(F32)).astype(BF16)
        for j in range(4):
            fin[source(g, j)] = total[j * cap : (j + 1) * cap]
        for j in range(4):
            src = source(g, j)
            if j > 0:
                to_owner(g, src).start()
            else:

                @pl.when(g > 0)
                def _():
                    to_owner(g, src).start()

                @pl.when(g == 0)
                def _():
                    ret[s] = fin[s]

    def grad_rows(target, which):
        for k in range(8):
            r = rows[k // 2, :, k % 2, 0].reshape(experts * cap, chunk)
            target[k * chunk : (k + 1) * chunk, :] = tn(
                r, which[...].reshape(experts * cap, -1)
            ).astype(BF16)

    def grad_down():
        hidden = act[...].reshape(experts * cap, -1)
        for k in range(8):
            sc = rows[k // 2, :, k % 2, 1].reshape(experts * cap, chunk)
            gd[:, k * chunk : (k + 1) * chunk] = tn(hidden, sc).astype(BF16)

    stores = [
        pltpu.make_async_copy(gg, gg_hbm, local.at[6]),
        pltpu.make_async_copy(gu, gu_hbm, local.at[7]),
        pltpu.make_async_copy(gd, gd_hbm, local.at[8]),
        pltpu.make_async_copy(dgate_out, dgate_hbm, local.at[10]),
        pltpu.make_async_copy(dc_out, dc_hbm, local.at[11]),
        pltpu.make_async_copy(proj_out, proj_hbm, local.at[12]),
        pltpu.make_async_copy(dx_out, dx_hbm, local.at[13]),
        pltpu.make_async_copy(db_out, db_hbm, local.at[14]),
    ]

    def turn(u, carry):
        @pl.when(u < 32)
        def _():
            forward_own(u)

        v = u - 5

        @pl.when((v >= 0) & (v < 32))
        def _():
            forward_beside(v)

        m = u - 14
        g, k = (m + 64) // 8 - 8, (m + 64) % 8
        active = (m >= 0) & (m < 32)

        @pl.when(active & (k < 4))
        def _():
            multiply(g, k)

        @pl.when(active & (k == 3))
        def _():
            activate(g)

        @pl.when(active & (k >= 4))
        def _():
            back(g, k - 4)

        @pl.when(active & (k == 5))
        def _():
            sum_far(g)

        for late, task in ((11, sum_near), (17, sum_own)):
            w = m - late

            @pl.when((w >= 0) & (w < 32) & ((w + 64) % 8 == 0))
            def _():
                task((w + 64) // 8 - 8)

        @pl.when(u == 20)
        def _():
            scan_forward()

        @pl.when(u == 33)
        def _():
            finish_forward()

        return carry

    lax.fori_loop(0, 14 + 24 + 17 + 1, turn, 0)

    grad_rows(gg, dgate)
    stores[0].start()
    grad_rows(gu, dup)
    stores[1].start()
    grad_down()
    stores[2].start()

    for ref, send in (
        (sendbuf.at[others], a_send),
        (rows.at[0, :, :, 0], yr_send),
        (rows.at[0, :, :, 1], ys_send),
        (rows.at[0], pa_send),
        (rows.at[0], pn_send),
        (part.at[:, 0], d_send),
        (q1, s1_send),
        (q2, s2_send),
        (fin.at[others], c_send),
    ):
        remote(ref, ref, send, c_recv, up).wait_send()
    for exchange in (states, enters):
        exchange[2]()

    remote(fin.at[others], ret.at[others], c_send, c_recv, up).wait_recv()
    places = experts * cap
    picked = tn(hot[...].reshape(places, tokens), ret[...].reshape(places, own))
    gm[t] = (cot_own[...].astype(F32) + picked).astype(BF16)

    low, high = pl.ds(0, tokens // 2), pl.ds(tokens // 2, tokens // 2)
    below, above, far = (t + 6) % 8, (t + 2) % 8, (t + 4) % 8
    mate = t + 1 - 2 * core
    m_below, m_above, m_far = (mate + 6) % 8, (mate + 2) % 8, (mate + 4) % 8

    def gather(k, src, device, part_rows=None):
        ref = gm.at[src] if part_rows is None else gm.at[src, part_rows]
        return remote(ref, ref, g_send.at[k], g_recv.at[k], device)

    columns = gated.shape[2]
    my_half = pl.ds(core * (tokens // 2), tokens // 2)
    mate_half = pl.ds((1 - core) * (tokens // 2), tokens // 2)

    def to_features(i, k):
        return remote(
            gm.at[i // 2, my_half, k * columns : (k + 1) * columns],
            features.at[s, my_half],
            p_send,
            p_recv,
            (i // 4, i % 4, t),
        )

    def share_half(half_rows):
        ref = features.at[:, half_rows]
        return remote(ref, ref, r_send, r_recv, partner)

    def send_rows(j):
        for k in range(2):
            i = 2 * j + k

            @pl.when(i != s)
            def _():
                to_features(i, k).start()

            @pl.when(i == s)
            def _():
                features[s, my_half] = gm[j, my_half, k * columns : (k + 1) * columns]

    def project(j):
        return nn(gm[j], op[pl.ds(j * own, own), :])

    def features_all():
        ref = features.at[others, my_half]
        return remote(ref, ref, p_send, p_recv, up)

    def multiply_features(src, total):
        return total + tn(features[src], gated[src])

    moves = (
        (1, t, up, low),
        (2, t, up, high),
        (3, t, down, high),
        (4, t, down, low),
        (0, t, partner, None),
        (5, below, up, low),
        (6, above, down, high),
        (7, below, partner, None),
        (8, above, partner, None),
        (9, far, partner, None),
    )

    def start(k):
        gather(*[m for m in moves if m[0] == k][0]).start()

    for k in (1, 3, 2, 4, 0):
        start(k)
    out_grad = project(t)
    send_rows(t)
    gather(0, mate, partner).wait_recv()
    out_grad = out_grad + project(mate)
    send_rows(mate)
    gather(1, below, up, low).wait_recv()
    start(5)
    gather(3, above, down, high).wait_recv()
    start(6)
    gather(2, below, up, high).wait_recv()
    start(7)
    gather(4, above, down, low).wait_recv()
    start(8)
    out_grad = out_grad + project(above)
    send_rows(above)
    out_grad = out_grad + project(below)
    send_rows(below)
    gather(8, m_above, partner).wait_recv()
    out_grad = out_grad + project(m_above)
    send_rows(m_above)
    gather(7, m_below, partner).wait_recv()
    out_grad = out_grad + project(m_below)
    send_rows(m_below)
    gather(5, far, up, low).wait_recv()
    gather(6, far, down, high).wait_recv()
    start(9)
    out_grad = out_grad + project(far)
    gather(9, m_far, partner).wait_recv()
    out_grad = out_grad + project(m_far)

    row, col = decays(ld[...])
    leads = by_lane(jnp.exp(col), tokens, heads)
    gate = gate_in[...].astype(F32)
    lead_grad = (out_grad * (gate * jax.nn.sigmoid(gate)) * leads).astype(BF16)
    back_send[...] = tn(lead_grad, c_in[...]).astype(BF16).reshape(experts, STEP, STATE)
    back_in[s] = back_send[s]
    backs[0]()
    for j in (far, m_far):
        send_rows(j)
    backward = mix_backward(
        x_in[...], b_in[...], c_in[...], gate, out_grad, y_ref[...], lead_grad,
        enter[...].reshape(x_in.shape[1], STATE), row, col, heads
    )
    dgate_out[...] = backward[3].astype(BF16)
    dc_out[...] = backward[2].astype(BF16)
    stores[3].start()
    stores[4].start()
    scan_back()
    tails = by_lane(jnp.exp(col[tokens - 1 : tokens, :] - col), tokens, heads)
    tail_values = (x_in[...].astype(F32) * tails).astype(BF16)
    features_all().wait_recv()
    share_half(my_half).start()
    gates[1]()
    share_half(mate_half).wait_recv()
    proj_out[...] = lax.fori_loop(
        0, experts, multiply_features, jnp.zeros(proj_out.shape, F32)
    )
    stores[5].start()
    features_all().wait_send()
    share_half(my_half).wait_send()
    gates[2]()
    backs[2]()
    for move in moves:
        gather(*move).wait_send()
    for store in stores[:6]:
        store.wait()

    leaves[1]()
    leaving = leave[...].reshape(x_in.shape[1], STATE)
    dx_out[...] = (backward[0] + tails * nt(b_in[...], leaving)).astype(BF16)
    stores[6].start()
    db_out[...] = (backward[1] + nn(tail_values, leaving)).astype(BF16)
    stores[7].start()

    leaves[2]()
    stores[6].wait()
    stores[7].wait()


def whole(ids, wts, ld, x, b, c, gate, mixed, cot, wg, wu, wd, op, experts, cap, heads):
    tokens, width = mixed.shape
    hidden = wg.shape[1]
    channels = x.shape[1]
    share, own = width // 4, width // 8
    vmem = pl.BlockSpec(memory_space=pltpu.VMEM)
    hbm = pl.BlockSpec(memory_space=pl.ANY)
    dma = pltpu.SemaphoreType.DMA

    def kernel(*refs):
        moe_kernel(heads, *refs)

    def buf(*shape, dtype=BF16):
        return pltpu.VMEM(shape, dtype)

    n = 4 * cap
    return pl.pallas_call(
        kernel,
        out_shape=[
            jax.ShapeDtypeStruct(x.shape, BF16),
            jax.ShapeDtypeStruct(b.shape, BF16),
            jax.ShapeDtypeStruct(c.shape, BF16),
            jax.ShapeDtypeStruct(gate.shape, BF16),
            jax.ShapeDtypeStruct((width // experts, channels), F32),
            jax.ShapeDtypeStruct(wg.shape, BF16),
            jax.ShapeDtypeStruct(wu.shape, BF16),
            jax.ShapeDtypeStruct(wd.shape, BF16),
        ],
        in_specs=[vmem] * 7 + [hbm] * 6,
        out_specs=[hbm] * 8,
        scratch_shapes=[
            buf(*x.shape),
            buf(*b.shape),
            buf(*c.shape),
            buf(*gate.shape),
            buf(width // experts, channels, dtype=F32),
            buf(8, tokens, own),
            buf(*op.shape),
            buf(tokens, channels, dtype=F32),
            buf(experts, tokens, channels),
            buf(experts, STEP + 8, STATE, dtype=F32),
            buf(experts, STEP + 8, STATE, dtype=F32),
            buf(experts, STEP, STATE),
            buf(experts, STEP, STATE),
            buf(experts, STEP, STATE),
            buf(experts, STEP, STATE),
            buf(experts, STEP, STATE),
            buf(experts, STEP, STATE),
            buf(experts, tokens, width // experts),
            buf(tokens, share),
            buf(tokens, share),
            buf(tokens, own),
            buf(*wg.shape),
            buf(*wu.shape),
            buf(*wd.shape),
            buf(experts, tokens, dtype=jnp.int32),
            buf(experts, tokens, dtype=F32),
            buf(experts, cap, tokens),
            buf(experts, 2, 2, cap, own),
            buf(4, experts, 2, 2, cap, own),
            buf(experts, cap, hidden),
            buf(experts, cap, hidden),
            buf(experts, cap, hidden),
            buf(4, 2, 4, n, own),
            buf(4, 4, n, own),
            buf(4, 2, n // 2, own),
            buf(4, 2, n // 2, own),
            buf(4, 2, n, own),
            buf(4, 2, n, own),
            buf(experts, cap, own),
            buf(experts, cap, own),
            buf(3, n, hidden, dtype=F32),
            buf(*wg.shape),
            buf(*wu.shape),
            buf(*wd.shape),
            dma((15,)),
        ]
        + [dma(()), dma((experts, 2))] * 2
        + [dma(())]
        + [dma(()), dma((4,))] * 2
        + [dma(()), dma((4, 4))]
        + [dma(()), dma((4, 2))] * 2
        + [dma(())] * 2
        + [dma((10,))] * 2
        + [dma(())] * 14,
        compiler_params=pltpu.CompilerParams(
            collective_id=0, has_side_effects=True, vmem_limit_bytes=60 * 2**20
        ),
        name="whole",
    )(ids, wts, ld, x, b, c, gate, mixed, cot, wg, wu, wd, op)


def hand_out(arrays):
    pieces = []
    for k, a in enumerate(arrays):
        count = max(1, a.size * a.dtype.itemsize // 2**19)
        step = a.shape[0] // count
        pieces += [(k, pl.ds(m * step, step)) for m in range(count)]

    def kernel(*refs):
        n = len(arrays)
        ins, outs, held, (come, go) = refs[:n], refs[n : 2 * n], refs[2 * n : 3 * n], refs[3 * n :]
        fetch = [
            pltpu.make_async_copy(ins[k].at[at], held[k].at[at], come.at[m])
            for m, (k, at) in enumerate(pieces)
        ]
        store = [
            pltpu.make_async_copy(held[k].at[at], outs[k].at[at], go.at[m])
            for m, (k, at) in enumerate(pieces)
        ]
        for f in fetch:
            f.start()
        for f, g in zip(fetch, store):
            f.wait()
            g.start()
        for g in store:
            g.wait()

    hbm = pl.BlockSpec(memory_space=pl.ANY)
    return pl.pallas_call(
        kernel,
        out_shape=[jax.ShapeDtypeStruct(a.shape, a.dtype) for a in arrays],
        in_specs=[hbm] * len(arrays),
        out_specs=[hbm] * len(arrays),
        scratch_shapes=[pltpu.VMEM(a.shape, a.dtype) for a in arrays]
        + [pltpu.SemaphoreType.DMA((len(pieces),))] * 2,
        name="hand_out",
    )(*arrays)


def body(
    token_values,
    write_keys,
    read_keys,
    log_decay,
    out_gate,
    out_proj,
    mixed,
    cotangent,
    route_ids,
    route_weights,
    w_gate,
    w_up,
    w_down,
):
    experts = lax.axis_size(SP)
    outs = hand_out(whole(
        route_ids.T,
        route_weights.T,
        log_decay,
        token_values,
        write_keys,
        read_keys,
        out_gate,
        mixed,
        cotangent,
        w_gate[0],
        w_up[0],
        w_down[0],
        out_proj,
        experts,
        3 * mixed.shape[0] // experts,
        log_decay.shape[0],
    ))
    return (*outs[:5], *(g[None] for g in outs[5:]))


def solution(mesh):
    finer = Mesh(mesh.devices.reshape(4, 4, mesh.shape["tp"]), ("sp_0", "sp_1", "tp"))
    return jax.shard_map(
        body,
        mesh=finer,
        in_specs=(
            P(SP, "tp"),
            P(SP, "tp"),
            P(SP, "tp"),
            P("tp", SP),
            P(SP, "tp"),
            P(None, "tp"),
            P(SP, None),
            P(SP, None),
            P(SP, None),
            P(SP, None),
            P(SP, None, "tp"),
            P(SP, None, "tp"),
            P(SP, "tp", None),
        ),
        out_specs=(
            P(SP, "tp"),
            P(SP, "tp"),
            P(SP, "tp"),
            P(SP, "tp"),
            P(SP, "tp"),
            P(SP, None, "tp"),
            P(SP, None, "tp"),
            P(SP, "tp", None),
        ),
        check_vma=False,
    )
```

```python
import jax
import jax.numpy as jnp
from jax import lax
from jax.experimental import pallas as pl
from jax.experimental.pallas import tpu as pltpu
from jax.sharding import Mesh
from jax.sharding import PartitionSpec as P

HEAD_DIM = 64
STATE = 128
SP = ("sp_0", "sp_1")
F32 = jnp.float32
BF16 = jnp.bfloat16
highest = lax.Precision.HIGHEST


def nn(a, b):
    return lax.dot_general(a, b, (((1,), (0,)), ((), ())), preferred_element_type=F32)


def nt(a, b):
    return lax.dot_general(a, b, (((1,), (1,)), ((), ())), preferred_element_type=F32)


def tn(a, b):
    return lax.dot_general(a, b, (((0,), (0,)), ((), ())), preferred_element_type=F32)


def iota(shape, dim):
    return lax.broadcasted_iota(jnp.int32, shape, dim)


def slots(ids_t, experts):
    tokens = ids_t.shape[1]
    e = iota((experts, tokens), 0)
    member = (ids_t[0:1, :] == e) | (ids_t[1:2, :] == e)
    before = (iota((tokens, tokens), 0) < iota((tokens, tokens), 1)).astype(BF16)
    slot = nn(member.astype(BF16), before)
    return jnp.where(member, slot.astype(jnp.int32), -1)


def weight_rows(ids_t, w_t, experts):
    e = iota((experts, ids_t.shape[1]), 0)
    return jnp.where(ids_t[0:1, :] == e, w_t[0:1, :], 0.0) + jnp.where(
        ids_t[1:2, :] == e, w_t[1:2, :], 0.0
    )


def decays(ld):
    heads, tokens = ld.shape
    ld8 = jnp.concatenate([ld, jnp.zeros((8 - heads, tokens), F32)], axis=0)
    upto = (iota((tokens, tokens), 0) <= iota((tokens, tokens), 1)).astype(F32)
    row = lax.dot_general(
        ld8, upto, (((1,), (0,)), ((), ())), precision=highest, preferred_element_type=F32
    )
    col = lax.dot_general(
        upto, ld8, (((0,), (1,)), ((), ())), precision=highest, preferred_element_type=F32
    )
    return row, col


def by_lane(col, tokens, heads):
    lane = iota((tokens, 2 * HEAD_DIM), 1)
    return jnp.concatenate(
        [
            jnp.where(lane < HEAD_DIM, col[:, 2 * p : 2 * p + 1], col[:, 2 * p + 1 : 2 * p + 2])
            for p in range(heads // 2)
        ],
        axis=1,
    )


def span_weights(row, col, h, tokens):
    lower = iota((tokens, tokens), 0) >= iota((tokens, tokens), 1)
    return jnp.exp(jnp.where(lower, col[:, h : h + 1] - row[h : h + 1, :], -1e30))


def mix_local(x, b, c, row, col, heads):
    tokens = x.shape[0]
    scores = nt(c, b)
    first = iota((tokens, 2 * HEAD_DIM), 1) < HEAD_DIM
    ys = []
    for p in range(heads // 2):
        xp = x[:, 128 * p : 128 * p + 128]
        pair = [
            nn((scores * span_weights(row, col, 2 * p + i, tokens)).astype(BF16), xp)
            for i in range(2)
        ]
        ys.append(jnp.where(first, pair[0], pair[1]))
    tails = by_lane(jnp.exp(col[tokens - 1 : tokens, :] - col), tokens, heads)
    end = tn((x.astype(F32) * tails).astype(BF16), b)
    return jnp.concatenate(ys, axis=1), end


def mix_backward(x, b, c, gate, out_grad, y, lead_grad, entering, row, col, heads):
    tokens = x.shape[0]
    sigma = jax.nn.sigmoid(gate)
    gb = (out_grad * (gate * sigma)).astype(BF16)
    d_gate = out_grad * y * sigma * (1.0 + gate * (1.0 - sigma))
    scores = nt(c, b)
    first = iota((tokens, 2 * HEAD_DIM), 1) < HEAD_DIM
    d_scores = jnp.zeros((tokens, tokens), F32)
    dxs = []
    for p in range(heads // 2):
        xp = x[:, 128 * p : 128 * p + 128]
        gp = gb[:, 128 * p : 128 * p + 128]
        pair = []
        for i in range(2):
            w = span_weights(row, col, 2 * p + i, tokens)
            mine = first if i == 0 else jnp.logical_not(first)
            d_scores = d_scores + w * nt(jnp.where(mine, gp, jnp.zeros_like(gp)), xp)
            pair.append(tn((scores * w).astype(BF16), gp))
        dxs.append(jnp.where(first, pair[0], pair[1]))
    ds = d_scores.astype(BF16)
    return jnp.concatenate(dxs, axis=1), tn(ds, c), nn(ds, b) + nn(lead_grad, entering), d_gate


MESH = pl.DeviceIdType.MESH
STEP = 16


def remote(src, dst, send, recv, device):
    return pltpu.make_async_remote_copy(
        src_ref=src, dst_ref=dst, send_sem=send, recv_sem=recv, device_id=device, device_id_type=MESH
    )


def moe_kernel(
    heads,
    ids,
    wts,
    ld,
    x_in,
    b_in,
    c_in,
    gate_in,
    mixed,
    cot,
    wg_hbm,
    wu_hbm,
    wd_hbm,
    op_hbm,
    dx_hbm,
    db_hbm,
    dc_hbm,
    dgate_hbm,
    proj_hbm,
    gg_hbm,
    gu_hbm,
    gd_hbm,
    dx_out,
    db_out,
    dc_out,
    dgate_out,
    proj_out,
    gm,
    op,
    y_ref,
    gated,
    state_send,
    state_in,
    enter_send,
    enter,
    back_send,
    back_in,
    leave_send,
    leave,
    features,
    mixed_q,
    cot_q,
    cot_own,
    wg,
    wu,
    wd,
    slot_ref,
    weight_ref,
    hot,
    sendbuf,
    rows,
    act,
    dgate,
    dup,
    part,
    part_in,
    q1,
    y1,
    q2,
    y2,
    fin,
    ret,
    sums,
    gg,
    gu,
    gd,
    local,
    a_send,
    a_recv,
    yr_send,
    n_recv,
    ys_send,
    pa_send,
    pa_recv,
    pn_send,
    pn_recv,
    d_send,
    d_recv,
    s1_send,
    s1_recv,
    s2_send,
    s2_recv,
    c_send,
    c_recv,
    g_send,
    g_recv,
    e_send,
    e_recv,
    f_send,
    f_recv,
    b_send,
    b_recv,
    l_send,
    l_recv,
    p_send,
    p_recv,
    q_send,
    q_recv,
    r_send,
    r_recv,
):
    z, x, t = lax.axis_index("sp_0"), lax.axis_index("sp_1"), lax.axis_index("tp")
    s = 4 * z + x
    y, core = t // 2, t % 2
    quarter = t % 4
    beside = (quarter + 2) % 4
    partner_q = quarter + 1 - 2 * core
    partner_beside = (partner_q + 2) % 4
    up, down, partner = (z, x, (t + 2) % 8), (z, x, (t + 6) % 8), (z, x, t + 1 - 2 * core)
    tokens, width = mixed.shape
    experts, _, _, cap, chunk = sendbuf.shape
    share = 2 * chunk
    own = width // 8

    loads = [
        pltpu.make_async_copy(mixed.at[:, pl.ds(quarter * share, share)], mixed_q, local.at[0]),
        pltpu.make_async_copy(cot.at[:, pl.ds(quarter * share, share)], cot_q, local.at[1]),
        pltpu.make_async_copy(cot.at[:, pl.ds(t * own, own)], cot_own, local.at[2]),
        pltpu.make_async_copy(wg_hbm, wg, local.at[3]),
        pltpu.make_async_copy(wu_hbm, wu, local.at[4]),
        pltpu.make_async_copy(wd_hbm, wd, local.at[5]),
        pltpu.make_async_copy(op_hbm, op, local.at[9]),
    ]
    for load in loads:
        load.start()

    barrier = pltpu.get_barrier_semaphore()

    def peer(k):
        to_z, to_x = (z + k % 4) % 4, (x + k % 4 + k // 4) % 4
        return 4 * to_z + to_x, (to_z, to_x, t)

    def greet(k, carry):
        pl.semaphore_signal(barrier, inc=1, device_id=peer(k)[1], device_id_type=MESH)
        return carry

    lax.fori_loop(1, experts, greet, 0)
    for device in (up, down, partner):
        pl.semaphore_signal(barrier, inc=1, device_id=device, device_id_type=MESH)

    slot_ref[...] = slots(ids[...], experts)
    weight_ref[...] = weight_rows(ids[...], wts[...], experts)
    row, col = decays(ld[...])
    inner, last = mix_local(x_in[...], b_in[...], c_in[...], row, col, heads)
    y_ref[...] = inner
    totals = jnp.broadcast_to(row[:, tokens - 1 : tokens], (8, STATE))
    state_send[:, :STEP, :] = last.reshape(experts, STEP, STATE)
    state_send[:, STEP:, :] = jnp.broadcast_to(totals[None], (experts, 8, STATE))
    state_in[s] = state_send[s]

    others = pl.ds(0, experts - 1)

    def every(action):
        def step(k, carry):
            action(k)
            return carry

        lax.fori_loop(1, experts, step, 0)

    def over_sp(source_ref, target_ref, send, recv):
        def copy(k):
            j, device = peer(k)
            return remote(source_ref.at[j], target_ref.at[s], send, recv, device)

        return (
            lambda: every(lambda k: copy(k).start()),
            lambda: remote(source_ref.at[others], target_ref.at[others], send, recv, up).wait_recv(),
            lambda: remote(source_ref.at[others], target_ref.at[others], send, recv, up).wait_send(),
        )

    first_half, second_half = pl.ds(0, tokens // 2), pl.ds(tokens // 2, tokens // 2)

    def gated_one(k):
        ref, other = gated.at[z, x, first_half], gated.at[z, x, second_half]
        to_z, to_x = (z + k) % 4, (x + k) % 4
        return (
            remote(ref, ref, q_send.at[0], q_recv.at[0], (z, to_x, t)),
            remote(other, other, q_send.at[1], q_recv.at[1], (to_z, x, t)),
        )

    def gated_four(k):
        ref, other = gated.at[z, :, first_half], gated.at[:, x, second_half]
        to_z, to_x = (z + k) % 4, (x + k) % 4
        return (
            remote(ref, ref, q_send.at[2], q_recv.at[2], (to_z, x, t)),
            remote(other, other, q_send.at[3], q_recv.at[3], (z, to_x, t)),
        )

    def gated_came(k):
        three = pl.ds(0, 3)
        ref = gated.at[three, :, first_half] if k > 1 else gated.at[z, three, first_half]
        return remote(ref, ref, q_send.at[k], q_recv.at[k], up)

    def gated_start(step):
        for k in range(1, 4):
            for copy in step(k):
                copy.start()

    def gated_second():
        gated_came(0).wait_recv()
        gated_came(1).wait_recv()
        gated_start(gated_four)

    states = over_sp(state_send, state_in, e_send, e_recv)
    enters = over_sp(enter_send, enter, f_send, f_recv)
    backs = over_sp(back_send, back_in, b_send, b_recv)
    leaves = over_sp(leave_send, leave, l_send, l_recv)

    loads[0].wait()
    loads[1].wait()
    pl.semaphore_wait(barrier, experts - 1 + 3)
    states[0]()

    def to_expert(e, h):
        return remote(
            sendbuf.at[e, h], rows.at[quarter, s, h], a_send, a_recv.at[s, h], (e // 4, e % 4, t)
        )

    def build(g, carry):
        place = iota((cap, tokens), 0)
        ones, ws = [], []
        for j in range(4):
            e = peer(4 * g + j)[0]
            mine = place == slot_ref[pl.ds(e, 1), :]
            one = mine.astype(BF16)
            hot[e] = one
            ones.append(one)
            w = jnp.where(mine, weight_ref[pl.ds(e, 1), :], 0.0)
            ws.append(jnp.sum(w, axis=1, keepdims=True))
        one = jnp.concatenate(ones, axis=0)
        w = jnp.concatenate(ws, axis=0)
        plain = nn(one, mixed_q[...]).astype(BF16)
        scaled = (nn(one, cot_q[...]) * w).astype(BF16)
        for j in range(4):
            e = peer(4 * g + j)[0]
            for h in range(2):
                part_rows, f = slice(j * cap, (j + 1) * cap), slice(h * chunk, (h + 1) * chunk)
                sendbuf[e, h, 0] = plain[part_rows, f]
                sendbuf[e, h, 1] = scaled[part_rows, f]
        for h in range(2):
            for j in range(4):
                e = peer(4 * g + j)[0]
                if j > 0:
                    to_expert(e, h).start()
                else:

                    @pl.when(g > 0)
                    def _():
                        to_expert(e, h).start()

        return carry

    lax.fori_loop(0, 4, build, 0)
    rows[quarter, s] = sendbuf[s]
    for load in loads[2:]:
        load.wait()

    def factor(src):
        return jnp.exp(state_in[src, pl.ds(STEP + s // 4, 1), :])

    def scan_forward():
        states[1]()
        held = jnp.zeros((STEP, STATE), F32)
        for src in range(experts):
            enter_send[src] = held.astype(BF16)
            held = factor(src) * held + state_in[src, :STEP, :]
        enter[s] = enter_send[s]
        enters[0]()

    def scan_back():
        backs[1]()
        held = jnp.zeros((STEP, STATE), F32)
        for src in reversed(range(experts)):
            leave_send[src] = held.astype(BF16)
            held = factor(src) * held + back_in[src].astype(F32)
        leave[s] = leave_send[s]
        leaves[0]()

    def finish_forward():
        enters[1]()
        _, col = decays(ld[...])
        leads = by_lane(jnp.exp(col), tokens, heads)
        entering = enter[...].reshape(x_in.shape[1], STATE)
        whole = y_ref[...] + leads * nt(c_in[...], entering)
        g = gate_in[...].astype(F32)
        y_ref[...] = whole
        gated[z, x] = (whole * (g * jax.nn.sigmoid(g))).astype(BF16)
        gated_start(gated_one)

    def source(g, j):
        return 4 * ((z + 4 - j) % 4) + (x + 8 - j - g) % 4

    def arrived(src, h):
        return remote(
            sendbuf.at[src, h], rows.at[quarter, src, h], a_send, a_recv.at[src, h], up
        )

    def rows_up(src, h, q):
        ref = rows.at[q, src, h, 0]
        return remote(ref, ref, yr_send, n_recv.at[src, h], up)

    def scaled_down(src, h, q):
        ref = rows.at[q, src, h, 1]
        return remote(ref, ref, ys_send, n_recv.at[src, h], down)

    def across(src, h, q, g):
        ref = rows.at[q, src, h]
        return remote(ref, ref, pa_send, pa_recv.at[g], partner)

    def across_beside(src, h, q, g):
        ref = rows.at[q, src, h]
        return remote(ref, ref, pn_send, pn_recv.at[g], partner)

    def unit(u):
        g, h, j = u // 8, u // 4 % 2, u % 4
        return source(g, j), h

    def forward_own(u):
        src, h = unit(u)

        @pl.when(src != s)
        def _():
            arrived(src, h).wait_recv()

        rows_up(src, h, quarter).start()
        scaled_down(src, h, quarter).start()
        across(src, h, quarter, u // 8).start()

    def forward_beside(u):
        src, h = unit(u)
        ref = rows.at[beside, src, h]
        remote(ref, ref, yr_send, n_recv.at[src, h], up).wait_recv()
        across_beside(src, h, beside, u // 8).start()

    def halves_across(g, f):
        return remote(
            part.at[g, 1 - core, f], part_in.at[g, f], d_send, d_recv.at[g, f], partner
        )

    def multiply(g, q):
        sources = [source(g, j) for j in range(4)]

        @pl.when(q == 0)
        def _():
            four = rows.at[partner_q, pl.ds(0, 4)]
            remote(four, four, pa_send, pa_recv.at[g], partner).wait_recv()
            remote(four, four, pn_send, pn_recv.at[g], partner).wait_recv()
            sums[...] = jnp.zeros_like(sums)

        for h in range(2):
            r = jnp.concatenate([rows[q, src, h, 0] for src in sources], axis=0)
            sc = jnp.concatenate([rows[q, src, h, 1] for src in sources], axis=0)
            f = pl.ds(pl.multiple_of(q * share + h * chunk, chunk), chunk)
            sums[0] += nn(r, wg[f, :])
            sums[1] += nn(r, wu[f, :])
            sums[2] += nt(sc, wd[:, f])

    def activate(g):
        sources = [source(g, j) for j in range(4)]
        gate_pre, up_pre, d_hidden = sums[0], sums[1], sums[2]
        sigma = jax.nn.sigmoid(gate_pre)
        silu = gate_pre * sigma
        dg = (d_hidden * up_pre * sigma * (1.0 + gate_pre * (1.0 - sigma))).astype(BF16)
        du = (d_hidden * silu).astype(BF16)
        hidden = (silu * up_pre).astype(BF16)
        for j, src in enumerate(sources):
            part_rows = slice(j * cap, (j + 1) * cap)
            act[src] = hidden[part_rows]
            dgate[src] = dg[part_rows]
            dup[src] = du[part_rows]

    def back(g, k):
        sources = [source(g, j) for j in range(4)]
        dg = jnp.concatenate([dgate[src] for src in sources], axis=0)
        du = jnp.concatenate([dup[src] for src in sources], axis=0)
        f = (y + 2 + 3 * k) % 4
        for m in range(2):
            cols = pl.ds(pl.multiple_of(f * share + m * own, own), own)
            part[g, m, f] = (nt(dg, wg[cols, :]) + nt(du, wu[cols, :])).astype(BF16)
        halves_across(g, f).start()

    def both(g, f):
        return part[g, core, f].astype(F32) + part_in[g, f].astype(F32)

    half = 2 * cap

    def first_step(g, way):
        return remote(
            q1.at[g, way], y1.at[g, way], s1_send, s1_recv.at[g, way], (up, down)[way]
        )

    def second_step(g, way):
        return remote(
            q2.at[g, way], y2.at[g, way], s2_send, s2_recv.at[g, way], (up, down)[way]
        )

    def sum_far(g):
        halves_across(g, (y + 2) % 4).wait_recv()
        far = both(g, (y + 2) % 4)
        q1[g, 0] = far[:half].astype(BF16)
        q1[g, 1] = far[half:].astype(BF16)
        first_step(g, 0).start()
        first_step(g, 1).start()

    def sum_near(g):
        first_step(g, 0).wait_recv()
        halves_across(g, (y + 1) % 4).wait_recv()
        above = both(g, (y + 1) % 4)
        q2[g, 0, :half] = (above[:half] + y1[g, 0].astype(F32)).astype(BF16)
        q2[g, 0, half:] = above[half:].astype(BF16)
        second_step(g, 0).start()
        first_step(g, 1).wait_recv()
        halves_across(g, (y + 3) % 4).wait_recv()
        below = both(g, (y + 3) % 4)
        q2[g, 1, :half] = below[:half].astype(BF16)
        q2[g, 1, half:] = (below[half:] + y1[g, 1].astype(F32)).astype(BF16)
        second_step(g, 1).start()

    def to_owner(g, src):
        return remote(
            fin.at[src], ret.at[s], c_send, c_recv, (src // 4, src % 4, t)
        )

    def sum_own(g):
        second_step(g, 0).wait_recv()
        second_step(g, 1).wait_recv()
        halves_across(g, y).wait_recv()
        total = (both(g, y) + y2[g, 0].astype(F32) + y2[g, 1].astype(F32)).astype(BF16)
        for j in range(4):
            fin[source(g, j)] = total[j * cap : (j + 1) * cap]
        for j in range(4):
            src = source(g, j)
            if j > 0:
                to_owner(g, src).start()
            else:

                @pl.when(g > 0)
                def _():
                    to_owner(g, src).start()

                @pl.when(g == 0)
                def _():
                    ret[s] = fin[s]

    def grad_rows(target, which):
        for k in range(8):
            r = rows[k // 2, :, k % 2, 0].reshape(experts * cap, chunk)
            target[k * chunk : (k + 1) * chunk, :] = tn(
                r, which[...].reshape(experts * cap, -1)
            ).astype(BF16)

    def grad_down():
        hidden = act[...].reshape(experts * cap, -1)
        for k in range(8):
            sc = rows[k // 2, :, k % 2, 1].reshape(experts * cap, chunk)
            gd[:, k * chunk : (k + 1) * chunk] = tn(hidden, sc).astype(BF16)

    stores = [
        pltpu.make_async_copy(gg, gg_hbm, local.at[6]),
        pltpu.make_async_copy(gu, gu_hbm, local.at[7]),
        pltpu.make_async_copy(gd, gd_hbm, local.at[8]),
        pltpu.make_async_copy(dgate_out, dgate_hbm, local.at[10]),
        pltpu.make_async_copy(dc_out, dc_hbm, local.at[11]),
        pltpu.make_async_copy(proj_out, proj_hbm, local.at[12]),
        pltpu.make_async_copy(dx_out, dx_hbm, local.at[13]),
        pltpu.make_async_copy(db_out, db_hbm, local.at[14]),
    ]

    def turn(u, carry):
        @pl.when(u < 32)
        def _():
            forward_own(u)

        v = u - 5

        @pl.when((v >= 0) & (v < 32))
        def _():
            forward_beside(v)

        m = u - 14
        g, k = (m + 64) // 8 - 8, (m + 64) % 8
        active = (m >= 0) & (m < 32)

        @pl.when(active & (k < 4))
        def _():
            multiply(g, k)

        @pl.when(active & (k == 3))
        def _():
            activate(g)

        @pl.when(active & (k >= 4))
        def _():
            back(g, k - 4)

        @pl.when(active & (k == 5))
        def _():
            sum_far(g)

        for late, task in ((11, sum_near), (17, sum_own)):
            w = m - late

            @pl.when((w >= 0) & (w < 32) & ((w + 64) % 8 == 0))
            def _():
                task((w + 64) // 8 - 8)

        @pl.when(u == 20)
        def _():
            scan_forward()

        @pl.when(u == 33)
        def _():
            finish_forward()

        @pl.when(u == 38)
        def _():
            gated_second()

        return carry

    lax.fori_loop(0, 14 + 24 + 17 + 1, turn, 0)

    grad_rows(gg, dgate)
    stores[0].start()
    grad_rows(gu, dup)
    stores[1].start()
    grad_down()
    stores[2].start()

    for ref, send in (
        (sendbuf.at[others], a_send),
        (rows.at[0, :, :, 0], yr_send),
        (rows.at[0, :, :, 1], ys_send),
        (rows.at[0], pa_send),
        (rows.at[0], pn_send),
        (part.at[:, 0], d_send),
        (q1, s1_send),
        (q2, s2_send),
        (fin.at[others], c_send),
    ):
        remote(ref, ref, send, c_recv, up).wait_send()
    for exchange in (states, enters):
        exchange[2]()

    remote(fin.at[others], ret.at[others], c_send, c_recv, up).wait_recv()
    places = experts * cap
    picked = tn(hot[...].reshape(places, tokens), ret[...].reshape(places, own))
    gm[t] = (cot_own[...].astype(F32) + picked).astype(BF16)

    low, high = pl.ds(0, tokens // 2), pl.ds(tokens // 2, tokens // 2)
    below, above, far = (t + 6) % 8, (t + 2) % 8, (t + 4) % 8
    mate = t + 1 - 2 * core
    m_below, m_above, m_far = (mate + 6) % 8, (mate + 2) % 8, (mate + 4) % 8

    def gather(k, src, device, part_rows=None):
        ref = gm.at[src] if part_rows is None else gm.at[src, part_rows]
        return remote(ref, ref, g_send.at[k], g_recv.at[k], device)

    columns = gated.shape[3]
    half_size = tokens // 2
    my_half = pl.ds(pl.multiple_of(core * half_size, half_size), half_size)
    mate_half = pl.ds(pl.multiple_of((1 - core) * half_size, half_size), half_size)

    def to_features(i, k):
        return remote(
            gm.at[i // 2, my_half, k * columns : (k + 1) * columns],
            features.at[s, my_half],
            p_send,
            p_recv,
            (i // 4, i % 4, t),
        )

    def share_half(half_rows):
        ref = features.at[:, half_rows]
        return remote(ref, ref, r_send, r_recv, partner)

    def send_rows(j):
        for k in range(2):
            i = 2 * j + k

            @pl.when(i != s)
            def _():
                to_features(i, k).start()

            @pl.when(i == s)
            def _():
                features[s, my_half] = gm[j, my_half, k * columns : (k + 1) * columns]

    def project(j):
        return nn(gm[j], op[pl.ds(j * own, own), :])

    def features_all():
        ref = features.at[others, my_half]
        return remote(ref, ref, p_send, p_recv, up)

    def multiply_features(half_rows):
        long = (experts * tokens // 2, columns)
        return tn(features[:, half_rows].reshape(long), gated[:, :, half_rows].reshape(long))

    moves = (
        (1, t, up, low),
        (2, t, up, high),
        (3, t, down, high),
        (4, t, down, low),
        (0, t, partner, None),
        (5, below, up, low),
        (6, above, down, high),
        (7, below, partner, None),
        (8, above, partner, None),
        (9, far, partner, None),
    )

    def start(k):
        gather(*[m for m in moves if m[0] == k][0]).start()

    for k in (1, 3, 2, 4, 0):
        start(k)
    out_grad = project(t)
    send_rows(t)
    gather(0, mate, partner).wait_recv()
    out_grad = out_grad + project(mate)
    send_rows(mate)
    gather(1, below, up, low).wait_recv()
    start(5)
    gather(3, above, down, high).wait_recv()
    start(6)
    gather(2, below, up, high).wait_recv()
    start(7)
    gather(4, above, down, low).wait_recv()
    start(8)
    out_grad = out_grad + project(above)
    send_rows(above)
    out_grad = out_grad + project(below)
    send_rows(below)
    gather(8, m_above, partner).wait_recv()
    out_grad = out_grad + project(m_above)
    send_rows(m_above)
    gather(7, m_below, partner).wait_recv()
    out_grad = out_grad + project(m_below)
    send_rows(m_below)
    gather(5, far, up, low).wait_recv()
    gather(6, far, down, high).wait_recv()
    start(9)
    out_grad = out_grad + project(far)
    gather(9, m_far, partner).wait_recv()
    out_grad = out_grad + project(m_far)

    row, col = decays(ld[...])
    leads = by_lane(jnp.exp(col), tokens, heads)
    gate = gate_in[...].astype(F32)
    lead_grad = (out_grad * (gate * jax.nn.sigmoid(gate)) * leads).astype(BF16)
    back_send[...] = tn(lead_grad, c_in[...]).astype(BF16).reshape(experts, STEP, STATE)
    back_in[s] = back_send[s]
    backs[0]()
    for j in (far, m_far):
        send_rows(j)
    backward = mix_backward(
        x_in[...], b_in[...], c_in[...], gate, out_grad, y_ref[...], lead_grad,
        enter[...].reshape(x_in.shape[1], STATE), row, col, heads
    )
    dgate_out[...] = backward[3].astype(BF16)
    dc_out[...] = backward[2].astype(BF16)
    stores[3].start()
    stores[4].start()
    scan_back()
    tails = by_lane(jnp.exp(col[tokens - 1 : tokens, :] - col), tokens, heads)
    tail_values = (x_in[...].astype(F32) * tails).astype(BF16)
    features_all().wait_recv()
    share_half(my_half).start()
    gated_came(2).wait_recv()
    gated_came(3).wait_recv()
    proj_out[...] = multiply_features(my_half)
    share_half(mate_half).wait_recv()
    proj_out[...] += multiply_features(mate_half)
    stores[5].start()
    features_all().wait_send()
    share_half(my_half).wait_send()
    for k in range(4):
        gated_came(k).wait_send()
    backs[2]()
    for move in moves:
        gather(*move).wait_send()
    for store in stores[:6]:
        store.wait()

    leaves[1]()
    leaving = leave[...].reshape(x_in.shape[1], STATE)
    dx_out[...] = (backward[0] + tails * nt(b_in[...], leaving)).astype(BF16)
    stores[6].start()
    db_out[...] = (backward[1] + nn(tail_values, leaving)).astype(BF16)
    stores[7].start()

    leaves[2]()
    stores[6].wait()
    stores[7].wait()


def whole(ids, wts, ld, x, b, c, gate, mixed, cot, wg, wu, wd, op, experts, cap, heads):
    tokens, width = mixed.shape
    hidden = wg.shape[1]
    channels = x.shape[1]
    share, own = width // 4, width // 8
    vmem = pl.BlockSpec(memory_space=pltpu.VMEM)
    hbm = pl.BlockSpec(memory_space=pl.ANY)
    dma = pltpu.SemaphoreType.DMA

    def kernel(*refs):
        moe_kernel(heads, *refs)

    def buf(*shape, dtype=BF16):
        return pltpu.VMEM(shape, dtype)

    n = 4 * cap
    return pl.pallas_call(
        kernel,
        out_shape=[
            jax.ShapeDtypeStruct(x.shape, BF16),
            jax.ShapeDtypeStruct(b.shape, BF16),
            jax.ShapeDtypeStruct(c.shape, BF16),
            jax.ShapeDtypeStruct(gate.shape, BF16),
            jax.ShapeDtypeStruct((width // experts, channels), F32),
            jax.ShapeDtypeStruct(wg.shape, BF16),
            jax.ShapeDtypeStruct(wu.shape, BF16),
            jax.ShapeDtypeStruct(wd.shape, BF16),
        ],
        in_specs=[vmem] * 7 + [hbm] * 6,
        out_specs=[hbm] * 8,
        scratch_shapes=[
            buf(*x.shape),
            buf(*b.shape),
            buf(*c.shape),
            buf(*gate.shape),
            buf(width // experts, channels, dtype=F32),
            buf(8, tokens, own),
            buf(*op.shape),
            buf(tokens, channels, dtype=F32),
            buf(4, 4, tokens, channels),
            buf(experts, STEP + 8, STATE, dtype=F32),
            buf(experts, STEP + 8, STATE, dtype=F32),
            buf(experts, STEP, STATE),
            buf(experts, STEP, STATE),
            buf(experts, STEP, STATE),
            buf(experts, STEP, STATE),
            buf(experts, STEP, STATE),
            buf(experts, STEP, STATE),
            buf(experts, tokens, width // experts),
            buf(tokens, share),
            buf(tokens, share),
            buf(tokens, own),
            buf(*wg.shape),
            buf(*wu.shape),
            buf(*wd.shape),
            buf(experts, tokens, dtype=jnp.int32),
            buf(experts, tokens, dtype=F32),
            buf(experts, cap, tokens),
            buf(experts, 2, 2, cap, own),
            buf(4, experts, 2, 2, cap, own),
            buf(experts, cap, hidden),
            buf(experts, cap, hidden),
            buf(experts, cap, hidden),
            buf(4, 2, 4, n, own),
            buf(4, 4, n, own),
            buf(4, 2, n // 2, own),
            buf(4, 2, n // 2, own),
            buf(4, 2, n, own),
            buf(4, 2, n, own),
            buf(experts, cap, own),
            buf(experts, cap, own),
            buf(3, n, hidden, dtype=F32),
            buf(*wg.shape),
            buf(*wu.shape),
            buf(*wd.shape),
            dma((15,)),
        ]
        + [dma(()), dma((experts, 2))] * 2
        + [dma(())]
        + [dma(()), dma((4,))] * 2
        + [dma(()), dma((4, 4))]
        + [dma(()), dma((4, 2))] * 2
        + [dma(())] * 2
        + [dma((10,))] * 2
        + [dma(())] * 10
        + [dma((4,))] * 2
        + [dma(())] * 2,
        compiler_params=pltpu.CompilerParams(
            collective_id=0, has_side_effects=True, vmem_limit_bytes=60 * 2**20
        ),
        name="whole",
    )(ids, wts, ld, x, b, c, gate, mixed, cot, wg, wu, wd, op)


def hand_out(arrays):
    pieces = []
    for k, a in enumerate(arrays):
        count = max(1, a.size * a.dtype.itemsize // 2**19)
        step = a.shape[0] // count
        pieces += [(k, pl.ds(m * step, step)) for m in range(count)]

    def kernel(*refs):
        n = len(arrays)
        ins, outs, held, (come, go) = refs[:n], refs[n : 2 * n], refs[2 * n : 3 * n], refs[3 * n :]
        fetch = [
            pltpu.make_async_copy(ins[k].at[at], held[k].at[at], come.at[m])
            for m, (k, at) in enumerate(pieces)
        ]
        store = [
            pltpu.make_async_copy(held[k].at[at], outs[k].at[at], go.at[m])
            for m, (k, at) in enumerate(pieces)
        ]
        for f in fetch:
            f.start()
        for f, g in zip(fetch, store):
            f.wait()
            g.start()
        for g in store:
            g.wait()

    hbm = pl.BlockSpec(memory_space=pl.ANY)
    return pl.pallas_call(
        kernel,
        out_shape=[jax.ShapeDtypeStruct(a.shape, a.dtype) for a in arrays],
        in_specs=[hbm] * len(arrays),
        out_specs=[hbm] * len(arrays),
        scratch_shapes=[pltpu.VMEM(a.shape, a.dtype) for a in arrays]
        + [pltpu.SemaphoreType.DMA((len(pieces),))] * 2,
        name="hand_out",
    )(*arrays)


def body(
    token_values,
    write_keys,
    read_keys,
    log_decay,
    out_gate,
    out_proj,
    mixed,
    cotangent,
    route_ids,
    route_weights,
    w_gate,
    w_up,
    w_down,
):
    experts = lax.axis_size(SP)
    outs = hand_out(whole(
        route_ids.T,
        route_weights.T,
        log_decay,
        token_values,
        write_keys,
        read_keys,
        out_gate,
        mixed,
        cotangent,
        w_gate[0],
        w_up[0],
        w_down[0],
        out_proj,
        experts,
        3 * mixed.shape[0] // experts,
        log_decay.shape[0],
    ))
    return (*outs[:5], *(g[None] for g in outs[5:]))


def solution(mesh):
    finer = Mesh(mesh.devices.reshape(4, 4, mesh.shape["tp"]), ("sp_0", "sp_1", "tp"))
    return jax.shard_map(
        body,
        mesh=finer,
        in_specs=(
            P(SP, "tp"),
            P(SP, "tp"),
            P(SP, "tp"),
            P("tp", SP),
            P(SP, "tp"),
            P(None, "tp"),
            P(SP, None),
            P(SP, None),
            P(SP, None),
            P(SP, None),
            P(SP, None, "tp"),
            P(SP, None, "tp"),
            P(SP, "tp", None),
        ),
        out_specs=(
            P(SP, "tp"),
            P(SP, "tp"),
            P(SP, "tp"),
            P(SP, "tp"),
            P(SP, "tp"),
            P(SP, None, "tp"),
            P(SP, None, "tp"),
            P(SP, "tp", None),
        ),
        check_vma=False,
    )
```

```python
import jax
import jax.numpy as jnp
from jax import lax
from jax.experimental import pallas as pl
from jax.experimental.pallas import tpu as pltpu
from jax.sharding import Mesh
from jax.sharding import PartitionSpec as P

HEAD_DIM = 64
STATE = 128
SP = ("sp_0", "sp_1")
F32 = jnp.float32
BF16 = jnp.bfloat16
highest = lax.Precision.HIGHEST


def nn(a, b):
    return lax.dot_general(a, b, (((1,), (0,)), ((), ())), preferred_element_type=F32)


def nt(a, b):
    return lax.dot_general(a, b, (((1,), (1,)), ((), ())), preferred_element_type=F32)


def tn(a, b):
    return lax.dot_general(a, b, (((0,), (0,)), ((), ())), preferred_element_type=F32)


def iota(shape, dim):
    return lax.broadcasted_iota(jnp.int32, shape, dim)


def slots(ids_t, experts):
    tokens = ids_t.shape[1]
    e = iota((experts, tokens), 0)
    member = (ids_t[0:1, :] == e) | (ids_t[1:2, :] == e)
    before = (iota((tokens, tokens), 0) < iota((tokens, tokens), 1)).astype(BF16)
    slot = nn(member.astype(BF16), before)
    return jnp.where(member, slot.astype(jnp.int32), -1)


def weight_rows(ids_t, w_t, experts):
    e = iota((experts, ids_t.shape[1]), 0)
    return jnp.where(ids_t[0:1, :] == e, w_t[0:1, :], 0.0) + jnp.where(
        ids_t[1:2, :] == e, w_t[1:2, :], 0.0
    )


def decays(ld):
    heads, tokens = ld.shape
    ld8 = jnp.concatenate([ld, jnp.zeros((8 - heads, tokens), F32)], axis=0)
    upto = (iota((tokens, tokens), 0) <= iota((tokens, tokens), 1)).astype(F32)
    row = lax.dot_general(
        ld8, upto, (((1,), (0,)), ((), ())), precision=highest, preferred_element_type=F32
    )
    col = lax.dot_general(
        upto, ld8, (((0,), (1,)), ((), ())), precision=highest, preferred_element_type=F32
    )
    return row, col


def by_lane(col, tokens, heads):
    lane = iota((tokens, 2 * HEAD_DIM), 1)
    return jnp.concatenate(
        [
            jnp.where(lane < HEAD_DIM, col[:, 2 * p : 2 * p + 1], col[:, 2 * p + 1 : 2 * p + 2])
            for p in range(heads // 2)
        ],
        axis=1,
    )


def span_weights(row, col, h, tokens):
    lower = iota((tokens, tokens), 0) >= iota((tokens, tokens), 1)
    return jnp.exp(jnp.where(lower, col[:, h : h + 1] - row[h : h + 1, :], -1e30))


def mix_local(x, b, c, row, col, heads):
    tokens = x.shape[0]
    scores = nt(c, b)
    first = iota((tokens, 2 * HEAD_DIM), 1) < HEAD_DIM
    ys = []
    for p in range(heads // 2):
        xp = x[:, 128 * p : 128 * p + 128]
        pair = [
            nn((scores * span_weights(row, col, 2 * p + i, tokens)).astype(BF16), xp)
            for i in range(2)
        ]
        ys.append(jnp.where(first, pair[0], pair[1]))
    tails = by_lane(jnp.exp(col[tokens - 1 : tokens, :] - col), tokens, heads)
    end = tn((x.astype(F32) * tails).astype(BF16), b)
    return jnp.concatenate(ys, axis=1), end


def mix_backward(x, b, c, gate, out_grad, y, lead_grad, entering, row, col, heads):
    tokens = x.shape[0]
    sigma = jax.nn.sigmoid(gate)
    gb = (out_grad * (gate * sigma)).astype(BF16)
    d_gate = out_grad * y * sigma * (1.0 + gate * (1.0 - sigma))
    scores = nt(c, b)
    first = iota((tokens, 2 * HEAD_DIM), 1) < HEAD_DIM
    d_scores = jnp.zeros((tokens, tokens), F32)
    dxs = []
    for p in range(heads // 2):
        xp = x[:, 128 * p : 128 * p + 128]
        gp = gb[:, 128 * p : 128 * p + 128]
        pair = []
        for i in range(2):
            w = span_weights(row, col, 2 * p + i, tokens)
            mine = first if i == 0 else jnp.logical_not(first)
            d_scores = d_scores + w * nt(jnp.where(mine, gp, jnp.zeros_like(gp)), xp)
            pair.append(tn((scores * w).astype(BF16), gp))
        dxs.append(jnp.where(first, pair[0], pair[1]))
    ds = d_scores.astype(BF16)
    return jnp.concatenate(dxs, axis=1), tn(ds, c), nn(ds, b) + nn(lead_grad, entering), d_gate


MESH = pl.DeviceIdType.MESH
STEP = 16


def remote(src, dst, send, recv, device):
    return pltpu.make_async_remote_copy(
        src_ref=src, dst_ref=dst, send_sem=send, recv_sem=recv, device_id=device, device_id_type=MESH
    )


def moe_kernel(
    heads,
    ids,
    wts,
    ld,
    x_in,
    b_in,
    c_in,
    gate_in,
    mixed,
    cot,
    wg_hbm,
    wu_hbm,
    wd_hbm,
    op_hbm,
    dx_hbm,
    db_hbm,
    dc_hbm,
    dgate_hbm,
    proj_hbm,
    gg_hbm,
    gu_hbm,
    gd_hbm,
    dx_out,
    db_out,
    dc_out,
    dgate_out,
    proj_out,
    gm,
    op,
    y_ref,
    gated,
    state_send,
    state_in,
    enter_send,
    enter,
    back_send,
    back_in,
    leave_send,
    leave,
    features,
    mixed_q,
    cot_q,
    cot_own,
    wg,
    wu,
    wd,
    slot_ref,
    weight_ref,
    hot,
    sendbuf,
    rows,
    act,
    dgate,
    dup,
    part,
    part_in,
    q1,
    y1,
    q2,
    y2,
    fin,
    ret,
    sums,
    gg,
    gu,
    gd,
    local,
    a_send,
    a_recv,
    yr_send,
    n_recv,
    ys_send,
    pa_send,
    pa_recv,
    pn_send,
    pn_recv,
    d_send,
    d_recv,
    s1_send,
    s1_recv,
    s2_send,
    s2_recv,
    c_send,
    c_recv,
    g_send,
    g_recv,
    e_send,
    e_recv,
    f_send,
    f_recv,
    b_send,
    b_recv,
    l_send,
    l_recv,
    p_send,
    p_recv,
    q_send,
    q_recv,
    r_send,
    r_recv,
):
    z, x, t = lax.axis_index("sp_0"), lax.axis_index("sp_1"), lax.axis_index("tp")
    s = 4 * z + x
    y, core = t // 2, t % 2
    quarter = t % 4
    beside = (quarter + 2) % 4
    partner_q = quarter + 1 - 2 * core
    partner_beside = (partner_q + 2) % 4
    up, down, partner = (z, x, (t + 2) % 8), (z, x, (t + 6) % 8), (z, x, t + 1 - 2 * core)
    tokens, width = mixed.shape
    experts, _, _, cap, chunk = sendbuf.shape
    share = 2 * chunk
    own = width // 8

    loads = [
        pltpu.make_async_copy(mixed.at[:, pl.ds(quarter * share, share)], mixed_q, local.at[0]),
        pltpu.make_async_copy(cot.at[:, pl.ds(quarter * share, share)], cot_q, local.at[1]),
        pltpu.make_async_copy(cot.at[:, pl.ds(t * own, own)], cot_own, local.at[2]),
        pltpu.make_async_copy(wg_hbm, wg, local.at[3]),
        pltpu.make_async_copy(wu_hbm, wu, local.at[4]),
        pltpu.make_async_copy(wd_hbm, wd, local.at[5]),
        pltpu.make_async_copy(op_hbm, op, local.at[9]),
    ]
    for load in loads:
        load.start()

    barrier = pltpu.get_barrier_semaphore()

    def peer(k):
        to_z, to_x = (z + k % 4) % 4, (x + k % 4 + k // 4) % 4
        return 4 * to_z + to_x, (to_z, to_x, t)

    def greet(k, carry):
        pl.semaphore_signal(barrier, inc=1, device_id=peer(k)[1], device_id_type=MESH)
        return carry

    lax.fori_loop(1, experts, greet, 0)
    for device in (up, down, partner):
        pl.semaphore_signal(barrier, inc=1, device_id=device, device_id_type=MESH)

    slot_ref[...] = slots(ids[...], experts)
    weight_ref[...] = weight_rows(ids[...], wts[...], experts)
    row, col = decays(ld[...])
    inner, last = mix_local(x_in[...], b_in[...], c_in[...], row, col, heads)
    y_ref[...] = inner
    totals = jnp.broadcast_to(row[:, tokens - 1 : tokens], (8, STATE))
    state_send[:, :STEP, :] = last.reshape(experts, STEP, STATE)
    state_send[:, STEP:, :] = jnp.broadcast_to(totals[None], (experts, 8, STATE))
    state_in[s] = state_send[s]

    others = pl.ds(0, experts - 1)

    def every(action):
        def step(k, carry):
            action(k)
            return carry

        lax.fori_loop(1, experts, step, 0)

    def over_sp(source_ref, target_ref, send, recv):
        def copy(k):
            j, device = peer(k)
            return remote(source_ref.at[j], target_ref.at[s], send, recv, device)

        return (
            lambda: every(lambda k: copy(k).start()),
            lambda: remote(source_ref.at[others], target_ref.at[others], send, recv, up).wait_recv(),
            lambda: remote(source_ref.at[others], target_ref.at[others], send, recv, up).wait_send(),
        )

    first_half, second_half = pl.ds(0, tokens // 2), pl.ds(tokens // 2, tokens // 2)

    def gated_one(k):
        ref, other = gated.at[z, x, first_half], gated.at[z, x, second_half]
        to_z, to_x = (z + k) % 4, (x + k) % 4
        return (
            remote(ref, ref, q_send.at[0], q_recv.at[0], (z, to_x, t)),
            remote(other, other, q_send.at[1], q_recv.at[1], (to_z, x, t)),
        )

    def gated_four(k):
        ref, other = gated.at[z, :, first_half], gated.at[:, x, second_half]
        to_z, to_x = (z + k) % 4, (x + k) % 4
        return (
            remote(ref, ref, q_send.at[2], q_recv.at[2], (to_z, x, t)),
            remote(other, other, q_send.at[3], q_recv.at[3], (z, to_x, t)),
        )

    def gated_came(k):
        three = pl.ds(0, 3)
        ref = gated.at[three, :, first_half] if k > 1 else gated.at[z, three, first_half]
        return remote(ref, ref, q_send.at[k], q_recv.at[k], up)

    def gated_start(step):
        for k in range(1, 4):
            for copy in step(k):
                copy.start()

    def gated_second():
        gated_came(0).wait_recv()
        gated_came(1).wait_recv()
        gated_start(gated_four)

    states = over_sp(state_send, state_in, e_send, e_recv)
    enters = over_sp(enter_send, enter, f_send, f_recv)
    backs = over_sp(back_send, back_in, b_send, b_recv)
    leaves = over_sp(leave_send, leave, l_send, l_recv)

    loads[0].wait()
    loads[1].wait()
    pl.semaphore_wait(barrier, experts - 1 + 3)
    states[0]()

    def to_expert(e, h):
        return remote(
            sendbuf.at[e, h], rows.at[quarter, s, h], a_send, a_recv.at[s, h], (e // 4, e % 4, t)
        )

    def build(g, carry):
        place = iota((cap, tokens), 0)
        ones, ws = [], []
        for j in range(4):
            e = peer(4 * g + j)[0]
            mine = place == slot_ref[pl.ds(e, 1), :]
            one = mine.astype(BF16)
            hot[e] = one
            ones.append(one)
            w = jnp.where(mine, weight_ref[pl.ds(e, 1), :], 0.0)
            ws.append(jnp.sum(w, axis=1, keepdims=True))
        one = jnp.concatenate(ones, axis=0)
        w = jnp.concatenate(ws, axis=0)
        plain = nn(one, mixed_q[...]).astype(BF16)
        scaled = (nn(one, cot_q[...]) * w).astype(BF16)
        for j in range(4):
            e = peer(4 * g + j)[0]
            for h in range(2):
                part_rows, f = slice(j * cap, (j + 1) * cap), slice(h * chunk, (h + 1) * chunk)
                sendbuf[e, h, 0] = plain[part_rows, f]
                sendbuf[e, h, 1] = scaled[part_rows, f]
        for h in range(2):
            for j in range(4):
                e = peer(4 * g + j)[0]
                if j > 0:
                    to_expert(e, h).start()
                else:

                    @pl.when(g > 0)
                    def _():
                        to_expert(e, h).start()

        return carry

    lax.fori_loop(0, 4, build, 0)
    rows[quarter, s] = sendbuf[s]
    for load in loads[2:]:
        load.wait()

    def factor(src):
        return jnp.exp(state_in[src, pl.ds(STEP + s // 4, 1), :])

    def scan_forward():
        states[1]()
        held = jnp.zeros((STEP, STATE), F32)
        for src in range(experts):
            enter_send[src] = held.astype(BF16)
            held = factor(src) * held + state_in[src, :STEP, :]
        enter[s] = enter_send[s]
        enters[0]()

    def scan_back():
        backs[1]()
        held = jnp.zeros((STEP, STATE), F32)
        for src in reversed(range(experts)):
            leave_send[src] = held.astype(BF16)
            held = factor(src) * held + back_in[src].astype(F32)
        leave[s] = leave_send[s]
        leaves[0]()

    def finish_forward():
        enters[1]()
        _, col = decays(ld[...])
        leads = by_lane(jnp.exp(col), tokens, heads)
        entering = enter[...].reshape(x_in.shape[1], STATE)
        whole = y_ref[...] + leads * nt(c_in[...], entering)
        g = gate_in[...].astype(F32)
        y_ref[...] = whole
        gated[z, x] = (whole * (g * jax.nn.sigmoid(g))).astype(BF16)
        gated_start(gated_one)

    def source(g, j):
        return 4 * ((z + 4 - j) % 4) + (x + 8 - j - g) % 4

    def arrived(src, h):
        return remote(
            sendbuf.at[src, h], rows.at[quarter, src, h], a_send, a_recv.at[src, h], up
        )

    def rows_up(src, h, q):
        ref = rows.at[q, src, h, 0]
        return remote(ref, ref, yr_send, n_recv.at[src, h], up)

    def scaled_down(src, h, q):
        ref = rows.at[q, src, h, 1]
        return remote(ref, ref, ys_send, n_recv.at[src, h], down)

    def across(src, h, q, g):
        ref = rows.at[q, src, h]
        return remote(ref, ref, pa_send, pa_recv.at[g], partner)

    def across_beside(src, h, q, g):
        ref = rows.at[q, src, h]
        return remote(ref, ref, pn_send, pn_recv.at[g], partner)

    def unit(u):
        g, h, j = u // 8, u // 4 % 2, u % 4
        return source(g, j), h

    def forward_own(u):
        src, h = unit(u)

        @pl.when(src != s)
        def _():
            arrived(src, h).wait_recv()

        rows_up(src, h, quarter).start()
        scaled_down(src, h, quarter).start()
        across(src, h, quarter, u // 8).start()

    def forward_beside(u):
        src, h = unit(u)
        ref = rows.at[beside, src, h]
        remote(ref, ref, yr_send, n_recv.at[src, h], up).wait_recv()
        across_beside(src, h, beside, u // 8).start()

    def halves_across(g, f):
        return remote(
            part.at[g, 1 - core, f], part_in.at[g, f], d_send, d_recv.at[g, f], partner
        )

    def multiply(g, q):
        sources = [source(g, j) for j in range(4)]

        @pl.when(q == 0)
        def _():
            four = rows.at[partner_q, pl.ds(0, 4)]
            remote(four, four, pa_send, pa_recv.at[g], partner).wait_recv()
            remote(four, four, pn_send, pn_recv.at[g], partner).wait_recv()
            sums[...] = jnp.zeros_like(sums)

        for h in range(2):
            r = jnp.concatenate([rows[q, src, h, 0] for src in sources], axis=0)
            sc = jnp.concatenate([rows[q, src, h, 1] for src in sources], axis=0)
            f = pl.ds(pl.multiple_of(q * share + h * chunk, chunk), chunk)
            sums[0] += nn(r, wg[f, :])
            sums[1] += nn(r, wu[f, :])
            sums[2] += nt(sc, wd[:, f])

    def activate(g):
        sources = [source(g, j) for j in range(4)]
        gate_pre, up_pre, d_hidden = sums[0], sums[1], sums[2]
        sigma = jax.nn.sigmoid(gate_pre)
        silu = gate_pre * sigma
        dg = (d_hidden * up_pre * sigma * (1.0 + gate_pre * (1.0 - sigma))).astype(BF16)
        du = (d_hidden * silu).astype(BF16)
        hidden = (silu * up_pre).astype(BF16)
        for j, src in enumerate(sources):
            part_rows = slice(j * cap, (j + 1) * cap)
            act[src] = hidden[part_rows]
            dgate[src] = dg[part_rows]
            dup[src] = du[part_rows]

    def back(g, k):
        sources = [source(g, j) for j in range(4)]
        dg = jnp.concatenate([dgate[src] for src in sources], axis=0)
        du = jnp.concatenate([dup[src] for src in sources], axis=0)
        f = (y + 2 + 3 * k) % 4
        for m in range(2):
            cols = pl.ds(pl.multiple_of(f * share + m * own, own), own)
            part[g, m, f] = (nt(dg, wg[cols, :]) + nt(du, wu[cols, :])).astype(BF16)
        halves_across(g, f).start()

    def both(g, f):
        return part[g, core, f].astype(F32) + part_in[g, f].astype(F32)

    half = 2 * cap

    def first_step(g, way):
        return remote(
            q1.at[g, way], y1.at[g, way], s1_send, s1_recv.at[g, way], (up, down)[way]
        )

    def second_step(g, way):
        return remote(
            q2.at[g, way], y2.at[g, way], s2_send, s2_recv.at[g, way], (up, down)[way]
        )

    def sum_far(g):
        halves_across(g, (y + 2) % 4).wait_recv()
        far = both(g, (y + 2) % 4)
        q1[g, 0] = far[:half].astype(BF16)
        q1[g, 1] = far[half:].astype(BF16)
        first_step(g, 0).start()
        first_step(g, 1).start()

    def sum_near(g):
        first_step(g, 0).wait_recv()
        halves_across(g, (y + 1) % 4).wait_recv()
        above = both(g, (y + 1) % 4)
        q2[g, 0, :half] = (above[:half] + y1[g, 0].astype(F32)).astype(BF16)
        q2[g, 0, half:] = above[half:].astype(BF16)
        second_step(g, 0).start()
        first_step(g, 1).wait_recv()
        halves_across(g, (y + 3) % 4).wait_recv()
        below = both(g, (y + 3) % 4)
        q2[g, 1, :half] = below[:half].astype(BF16)
        q2[g, 1, half:] = (below[half:] + y1[g, 1].astype(F32)).astype(BF16)
        second_step(g, 1).start()

    def to_owner(g, src):
        return remote(
            fin.at[src], ret.at[s], c_send, c_recv, (src // 4, src % 4, t)
        )

    def sum_own(g):
        second_step(g, 0).wait_recv()
        second_step(g, 1).wait_recv()
        halves_across(g, y).wait_recv()
        total = (both(g, y) + y2[g, 0].astype(F32) + y2[g, 1].astype(F32)).astype(BF16)
        for j in range(4):
            fin[source(g, j)] = total[j * cap : (j + 1) * cap]
        for j in range(4):
            src = source(g, j)
            if j > 0:
                to_owner(g, src).start()
            else:

                @pl.when(g > 0)
                def _():
                    to_owner(g, src).start()

                @pl.when(g == 0)
                def _():
                    ret[s] = fin[s]

    def grad_rows(target, which):
        for k in range(8):
            r = rows[k // 2, :, k % 2, 0].reshape(experts * cap, chunk)
            target[k * chunk : (k + 1) * chunk, :] = tn(
                r, which[...].reshape(experts * cap, -1)
            ).astype(BF16)

    def grad_down():
        hidden = act[...].reshape(experts * cap, -1)
        for k in range(8):
            sc = rows[k // 2, :, k % 2, 1].reshape(experts * cap, chunk)
            gd[:, k * chunk : (k + 1) * chunk] = tn(hidden, sc).astype(BF16)

    stores = [
        pltpu.make_async_copy(gg, gg_hbm, local.at[6]),
        pltpu.make_async_copy(gu, gu_hbm, local.at[7]),
        pltpu.make_async_copy(gd, gd_hbm, local.at[8]),
        pltpu.make_async_copy(dgate_out, dgate_hbm, local.at[10]),
        pltpu.make_async_copy(dc_out, dc_hbm, local.at[11]),
        pltpu.make_async_copy(proj_out, proj_hbm, local.at[12]),
        pltpu.make_async_copy(dx_out, dx_hbm, local.at[13]),
        pltpu.make_async_copy(db_out, db_hbm, local.at[14]),
    ]

    def turn(u, carry):
        @pl.when(u < 32)
        def _():
            forward_own(u)

        v = u - 5

        @pl.when((v >= 0) & (v < 32))
        def _():
            forward_beside(v)

        m = u - 14
        g, k = (m + 64) // 8 - 8, (m + 64) % 8
        active = (m >= 0) & (m < 32)

        @pl.when(active & (k < 4))
        def _():
            multiply(g, k)

        @pl.when(active & (k == 3))
        def _():
            activate(g)

        @pl.when(active & (k >= 4))
        def _():
            back(g, k - 4)

        @pl.when(active & (k == 5))
        def _():
            sum_far(g)

        for late, task in ((11, sum_near), (17, sum_own)):
            w = m - late

            @pl.when((w >= 0) & (w < 32) & ((w + 64) % 8 == 0))
            def _():
                task((w + 64) // 8 - 8)

        @pl.when(u == 20)
        def _():
            scan_forward()

        @pl.when(u == 33)
        def _():
            finish_forward()

        @pl.when(u == 38)
        def _():
            gated_second()

        return carry

    lax.fori_loop(0, 14 + 24 + 17 + 1, turn, 0)

    grad_rows(gg, dgate)
    stores[0].start()
    grad_rows(gu, dup)
    stores[1].start()
    grad_down()
    stores[2].start()

    for ref, send in (
        (sendbuf.at[others], a_send),
        (rows.at[0, :, :, 0], yr_send),
        (rows.at[0, :, :, 1], ys_send),
        (rows.at[0], pa_send),
        (rows.at[0], pn_send),
        (part.at[:, 0], d_send),
        (q1, s1_send),
        (q2, s2_send),
        (fin.at[others], c_send),
    ):
        remote(ref, ref, send, c_recv, up).wait_send()
    for exchange in (states, enters):
        exchange[2]()

    remote(fin.at[others], ret.at[others], c_send, c_recv, up).wait_recv()
    low, high = pl.ds(0, tokens // 2), pl.ds(tokens // 2, tokens // 2)
    below, above, far = (t + 6) % 8, (t + 2) % 8, (t + 4) % 8
    mate = t + 1 - 2 * core
    m_below, m_above, m_far = (mate + 6) % 8, (mate + 2) % 8, (mate + 4) % 8

    def gather(k, src, device, part_rows=None):
        ref = gm.at[src] if part_rows is None else gm.at[src, part_rows]
        return remote(ref, ref, g_send.at[k], g_recv.at[k], device)

    columns = gated.shape[3]
    half_size = tokens // 2
    my_half = pl.ds(pl.multiple_of(core * half_size, half_size), half_size)
    mate_half = pl.ds(pl.multiple_of((1 - core) * half_size, half_size), half_size)

    def to_features(i, k):
        return remote(
            gm.at[i // 2, my_half, k * columns : (k + 1) * columns],
            features.at[s, my_half],
            p_send,
            p_recv,
            (i // 4, i % 4, t),
        )

    def share_half(half_rows):
        ref = features.at[:, half_rows]
        return remote(ref, ref, r_send, r_recv, partner)

    def send_rows(j):
        for k in range(2):
            i = 2 * j + k

            @pl.when(i != s)
            def _():
                to_features(i, k).start()

            @pl.when(i == s)
            def _():
                features[s, my_half] = gm[j, my_half, k * columns : (k + 1) * columns]

    def project(j):
        return nn(gm[j], op[pl.ds(j * own, own), :])

    def features_all():
        ref = features.at[others, my_half]
        return remote(ref, ref, p_send, p_recv, up)

    def multiply_features(half_rows):
        long = (experts * tokens // 2, columns)
        return tn(features[:, half_rows].reshape(long), gated[:, :, half_rows].reshape(long))

    moves = (
        (1, t, up, low),
        (2, t, up, high),
        (3, t, down, high),
        (4, t, down, low),
        (0, t, partner, None),
        (5, below, up, low),
        (6, above, down, high),
        (7, below, partner, None),
        (8, above, partner, None),
        (9, far, partner, None),
    )

    def start(k):
        gather(*[m for m in moves if m[0] == k][0]).start()

    def combine(at):
        there = hot[:, :, at].reshape(experts * cap, -1)
        picked = tn(there, ret[...].reshape(experts * cap, own))
        gm[t, at] = (cot_own[at].astype(F32) + picked).astype(BF16)

    combine(slice(0, tokens // 2))
    start(1)
    combine(slice(tokens // 2, tokens))
    for k in (3, 2, 4, 0):
        start(k)
    out_grad = project(t)
    send_rows(t)
    gather(0, mate, partner).wait_recv()
    out_grad = out_grad + project(mate)
    send_rows(mate)
    gather(1, below, up, low).wait_recv()
    start(5)
    gather(3, above, down, high).wait_recv()
    start(6)
    gather(2, below, up, high).wait_recv()
    start(7)
    gather(4, above, down, low).wait_recv()
    start(8)
    out_grad = out_grad + project(above)
    send_rows(above)
    out_grad = out_grad + project(below)
    send_rows(below)
    gather(8, m_above, partner).wait_recv()
    out_grad = out_grad + project(m_above)
    send_rows(m_above)
    gather(7, m_below, partner).wait_recv()
    out_grad = out_grad + project(m_below)
    send_rows(m_below)
    gather(5, far, up, low).wait_recv()
    gather(6, far, down, high).wait_recv()
    start(9)
    out_grad = out_grad + project(far)
    gather(9, m_far, partner).wait_recv()
    out_grad = out_grad + project(m_far)

    row, col = decays(ld[...])
    leads = by_lane(jnp.exp(col), tokens, heads)
    gate = gate_in[...].astype(F32)
    lead_grad = (out_grad * (gate * jax.nn.sigmoid(gate)) * leads).astype(BF16)
    back_send[...] = tn(lead_grad, c_in[...]).astype(BF16).reshape(experts, STEP, STATE)
    back_in[s] = back_send[s]
    backs[0]()
    for j in (far, m_far):
        send_rows(j)
    backward = mix_backward(
        x_in[...], b_in[...], c_in[...], gate, out_grad, y_ref[...], lead_grad,
        enter[...].reshape(x_in.shape[1], STATE), row, col, heads
    )
    dgate_out[...] = backward[3].astype(BF16)
    dc_out[...] = backward[2].astype(BF16)
    stores[3].start()
    stores[4].start()
    scan_back()
    tails = by_lane(jnp.exp(col[tokens - 1 : tokens, :] - col), tokens, heads)
    tail_values = (x_in[...].astype(F32) * tails).astype(BF16)
    features_all().wait_recv()
    share_half(my_half).start()
    gated_came(2).wait_recv()
    gated_came(3).wait_recv()
    proj_out[...] = multiply_features(my_half)
    share_half(mate_half).wait_recv()
    proj_out[...] += multiply_features(mate_half)
    stores[5].start()
    features_all().wait_send()
    share_half(my_half).wait_send()
    for k in range(4):
        gated_came(k).wait_send()
    backs[2]()
    for move in moves:
        gather(*move).wait_send()
    for store in stores[:6]:
        store.wait()

    leaves[1]()
    leaving = leave[...].reshape(x_in.shape[1], STATE)
    dx_out[...] = (backward[0] + tails * nt(b_in[...], leaving)).astype(BF16)
    stores[6].start()
    db_out[...] = (backward[1] + nn(tail_values, leaving)).astype(BF16)
    stores[7].start()

    leaves[2]()
    stores[6].wait()
    stores[7].wait()


def whole(ids, wts, ld, x, b, c, gate, mixed, cot, wg, wu, wd, op, experts, cap, heads):
    tokens, width = mixed.shape
    hidden = wg.shape[1]
    channels = x.shape[1]
    share, own = width // 4, width // 8
    vmem = pl.BlockSpec(memory_space=pltpu.VMEM)
    hbm = pl.BlockSpec(memory_space=pl.ANY)
    dma = pltpu.SemaphoreType.DMA

    def kernel(*refs):
        moe_kernel(heads, *refs)

    def buf(*shape, dtype=BF16):
        return pltpu.VMEM(shape, dtype)

    n = 4 * cap
    return pl.pallas_call(
        kernel,
        out_shape=[
            jax.ShapeDtypeStruct(x.shape, BF16),
            jax.ShapeDtypeStruct(b.shape, BF16),
            jax.ShapeDtypeStruct(c.shape, BF16),
            jax.ShapeDtypeStruct(gate.shape, BF16),
            jax.ShapeDtypeStruct((width // experts, channels), F32),
            jax.ShapeDtypeStruct(wg.shape, BF16),
            jax.ShapeDtypeStruct(wu.shape, BF16),
            jax.ShapeDtypeStruct(wd.shape, BF16),
        ],
        in_specs=[vmem] * 7 + [hbm] * 6,
        out_specs=[hbm] * 8,
        scratch_shapes=[
            buf(*x.shape),
            buf(*b.shape),
            buf(*c.shape),
            buf(*gate.shape),
            buf(width // experts, channels, dtype=F32),
            buf(8, tokens, own),
            buf(*op.shape),
            buf(tokens, channels, dtype=F32),
            buf(4, 4, tokens, channels),
            buf(experts, STEP + 8, STATE, dtype=F32),
            buf(experts, STEP + 8, STATE, dtype=F32),
            buf(experts, STEP, STATE),
            buf(experts, STEP, STATE),
            buf(experts, STEP, STATE),
            buf(experts, STEP, STATE),
            buf(experts, STEP, STATE),
            buf(experts, STEP, STATE),
            buf(experts, tokens, width // experts),
            buf(tokens, share),
            buf(tokens, share),
            buf(tokens, own),
            buf(*wg.shape),
            buf(*wu.shape),
            buf(*wd.shape),
            buf(experts, tokens, dtype=jnp.int32),
            buf(experts, tokens, dtype=F32),
            buf(experts, cap, tokens),
            buf(experts, 2, 2, cap, own),
            buf(4, experts, 2, 2, cap, own),
            buf(experts, cap, hidden),
            buf(experts, cap, hidden),
            buf(experts, cap, hidden),
            buf(4, 2, 4, n, own),
            buf(4, 4, n, own),
            buf(4, 2, n // 2, own),
            buf(4, 2, n // 2, own),
            buf(4, 2, n, own),
            buf(4, 2, n, own),
            buf(experts, cap, own),
            buf(experts, cap, own),
            buf(3, n, hidden, dtype=F32),
            buf(*wg.shape),
            buf(*wu.shape),
            buf(*wd.shape),
            dma((15,)),
        ]
        + [dma(()), dma((experts, 2))] * 2
        + [dma(())]
        + [dma(()), dma((4,))] * 2
        + [dma(()), dma((4, 4))]
        + [dma(()), dma((4, 2))] * 2
        + [dma(())] * 2
        + [dma((10,))] * 2
        + [dma(())] * 10
        + [dma((4,))] * 2
        + [dma(())] * 2,
        compiler_params=pltpu.CompilerParams(
            collective_id=0, has_side_effects=True, vmem_limit_bytes=60 * 2**20
        ),
        name="whole",
    )(ids, wts, ld, x, b, c, gate, mixed, cot, wg, wu, wd, op)


def hand_out(arrays):
    pieces = []
    for k, a in enumerate(arrays):
        count = max(1, a.size * a.dtype.itemsize // 2**20)
        step = a.shape[0] // count
        pieces += [(k, pl.ds(m * step, step)) for m in range(count)]

    def kernel(*refs):
        n = len(arrays)
        ins, outs, held, (come, go) = refs[:n], refs[n : 2 * n], refs[2 * n : 3 * n], refs[3 * n :]
        fetch = [
            pltpu.make_async_copy(ins[k].at[at], held[k].at[at], come.at[m])
            for m, (k, at) in enumerate(pieces)
        ]
        store = [
            pltpu.make_async_copy(held[k].at[at], outs[k].at[at], go.at[m])
            for m, (k, at) in enumerate(pieces)
        ]
        for f in fetch:
            f.start()
        for f, g in zip(fetch, store):
            f.wait()
            g.start()
        for g in store:
            g.wait()

    hbm = pl.BlockSpec(memory_space=pl.ANY)
    return pl.pallas_call(
        kernel,
        out_shape=[jax.ShapeDtypeStruct(a.shape, a.dtype) for a in arrays],
        in_specs=[hbm] * len(arrays),
        out_specs=[hbm] * len(arrays),
        scratch_shapes=[pltpu.VMEM(a.shape, a.dtype) for a in arrays]
        + [pltpu.SemaphoreType.DMA((len(pieces),))] * 2,
        name="hand_out",
    )(*arrays)


def body(
    token_values,
    write_keys,
    read_keys,
    log_decay,
    out_gate,
    out_proj,
    mixed,
    cotangent,
    route_ids,
    route_weights,
    w_gate,
    w_up,
    w_down,
):
    experts = lax.axis_size(SP)
    outs = hand_out(whole(
        route_ids.T,
        route_weights.T,
        log_decay,
        token_values,
        write_keys,
        read_keys,
        out_gate,
        mixed,
        cotangent,
        w_gate[0],
        w_up[0],
        w_down[0],
        out_proj,
        experts,
        3 * mixed.shape[0] // experts,
        log_decay.shape[0],
    ))
    return (*outs[:5], *(g[None] for g in outs[5:]))


def solution(mesh):
    finer = Mesh(mesh.devices.reshape(4, 4, mesh.shape["tp"]), ("sp_0", "sp_1", "tp"))
    return jax.shard_map(
        body,
        mesh=finer,
        in_specs=(
            P(SP, "tp"),
            P(SP, "tp"),
            P(SP, "tp"),
            P("tp", SP),
            P(SP, "tp"),
            P(None, "tp"),
            P(SP, None),
            P(SP, None),
            P(SP, None),
            P(SP, None),
            P(SP, None, "tp"),
            P(SP, None, "tp"),
            P(SP, "tp", None),
        ),
        out_specs=(
            P(SP, "tp"),
            P(SP, "tp"),
            P(SP, "tp"),
            P(SP, "tp"),
            P(SP, "tp"),
            P(SP, None, "tp"),
            P(SP, None, "tp"),
            P(SP, "tp", None),
        ),
        check_vma=False,
    )
```
